512 devices in a mesh: kv: 16 (over y, x), tp: 32 (over z, core).
Axes of the slice: x: 4, y: 4, z: 16, core: 2. Of those that a mesh axis runs over, the one named last changes fastest.
Arguments:
- residual: bfloat16 [512, 2048], P('tp', 'kv'), may hold values from -64 to 64
- prior_state: float32 [512, 16, 128, 128], P('tp', 'kv'), may hold values from -6 to 6
- w_query: bfloat16 [2048, 2048], P('tp', 'kv'), may hold values from -0.125 to 0.125
- w_forget: bfloat16 [2048, 2048], P('tp', 'kv'), may hold values from -0.125 to 0.125
- w_value: bfloat16 [2048, 2048], P('tp', 'kv'), may hold values from -0.125 to 0.125
- w_outgate: bfloat16 [2048, 2048], P('tp', 'kv'), may hold values from -0.125 to 0.125
- forget_floor: float32 [2048], P('kv'), may hold values from 0.05 to 0.9
- group_gain: float32 [2048], P('kv'), may hold values from 0.1 to 1.9
- w_mix_out: bfloat16 [2048, 2048], P('kv', 'tp'), may hold values from -0.397747564 to 0.397747564
- gain_mix_pre: float32 [2048], replicated, may hold values from 0.1 to 1.9
- gain_mix_post: float32 [2048], replicated, may hold values from 0.05 to 1.9
- gain_mlp_pre: float32 [2048], replicated, may hold values from 0.1 to 1.9
- gain_mlp_post: float32 [2048], replicated, may hold values from 0.1 to 1.9
- w_up: bfloat16 [2048, 8192], P('tp', 'kv'), may hold values from -0.125 to 0.125
- w_down: bfloat16 [8192, 2048], P('kv', 'tp'), may hold values from -0.198873782 to 0.198873782
Outputs:
- layer_out: bfloat16 [512, 2048], P('tp', 'kv')
- new_state: float32 [512, 16, 128, 128], P('tp', 'kv')
The draws below stay inside these ranges and needn't reach their ends.
All inputs are finite; a program needn't handle non-finite values.
Results may differ from the reference program's by a relative error of at most 0.015.
Values may be sent and summed in bfloat16 or wider, within the bound.
No kernel may reach another device: no remote copies, remote signals or barrier semaphores. Data moves between devices by JAX's collectives and lax.ppermute only.
A program may use at most 64 MiB of HBM per device.

```python
import jax
import jax.numpy as jnp
from jax import lax

D = 2048
HEADS = 16
HEAD_DIM = 128
FF = 8192
BATCH = 512


def ramp_scale(length, ratio_top):
    return jnp.exp(jnp.log(ratio_top) * jnp.arange(length, dtype=jnp.float32) / (length - 1))


def ramped_matrix(key, key_offset, row_count, col_count, fan_scale):
    base_key = jax.random.fold_in(key, key_offset)
    values = jnp.clip(jax.random.normal(base_key, (row_count, col_count), jnp.float32), -6.0, 6.0)
    return values * fan_scale * ramp_scale(col_count, 3.0)[None, :]


def draw_residual(key, part):
    base_key = jax.random.fold_in(jax.random.fold_in(key, 5), 0)
    values = jnp.clip(jax.random.normal(base_key, (BATCH, D), jnp.float32), -6.0, 6.0)
    return (0.5 * values * ramp_scale(D, 3.0)[None, :]).astype(jnp.bfloat16)


def draw_w_mix_out(key, part):
    rows_total = HEADS * HEAD_DIM
    return ramped_matrix(key, 23, rows_total, D, rows_total ** (-0.5)).astype(jnp.bfloat16)


def draw_w_down(key, part):
    return ramped_matrix(key, 29, FF, D, FF ** (-0.5)).astype(jnp.bfloat16)


def draw_gain_mix_post(key, part):
    base_key = jax.random.fold_in(key, 41)
    position = jnp.arange(D, dtype=jnp.float32) / (D - 1)
    factor = jax.random.uniform(base_key, (D,), jnp.float32, 0.55, 1.0)
    return (0.1 + 1.8 * position) * factor


def block_scale(rng, shape, pieces, smallest, top_value):
    loudness = 1.0
    for dim, blocks in pieces:
        steps = jax.random.uniform(jax.random.fold_in(jax.random.fold_in(rng, 6), dim), (blocks,), jnp.float32, smallest / len(pieces), top_value / len(pieces))
        loudness = loudness * jnp.repeat(jnp.exp(steps), shape[dim] // blocks).reshape((-1,) + (1,) * (len(shape) - 1 - dim))
    return loudness


def scatter_about(own_key, shape, scale, limit, pieces=(), kind=jnp.bfloat16):
    entries = jax.random.normal(own_key, shape, jnp.float32) * scale
    if len(pieces) > 0:
        entries = block_scale(own_key, shape, pieces, -0.22, 0.18) * entries
    return jnp.clip(entries, min=-limit, max=limit).astype(kind)


def setup_inputs(seed: int = 0) -> dict:
    keys = jax.random.split(jax.random.key(seed), 16)
    return {
        "residual": draw_residual(jax.random.fold_in(keys[15], 71), 0),
        "prior_state": scatter_about(keys[1], (BATCH, HEADS, HEAD_DIM, HEAD_DIM), 1.0, 6.0, ((0, 32), (1, 16)), jnp.float32),
        "w_query": scatter_about(keys[2], (D, HEADS * HEAD_DIM), D ** -0.5, 0.125, ((0, 32), (1, 16))),
        "w_forget": scatter_about(keys[3], (D, HEADS * HEAD_DIM), D ** -0.5, 0.125, ((0, 32), (1, 16))),
        "w_value": scatter_about(keys[4], (D, HEADS * HEAD_DIM), D ** -0.5, 0.125, ((0, 32), (1, 16))),
        "w_outgate": scatter_about(keys[5], (D, HEADS * HEAD_DIM), D ** -0.5, 0.125, ((0, 32), (1, 16))),
        "forget_floor": jnp.clip(0.05 + 0.84999998 * jax.random.uniform(keys[6], (HEADS * HEAD_DIM,), jnp.float32) ** block_scale(keys[6], (HEADS * HEAD_DIM,), ((0, 16),), -0.2, 0.2), 0.05, 0.9),
        "group_gain": jnp.clip(1.0 + 0.18 * jax.random.normal(keys[7], (HEADS * HEAD_DIM,), jnp.float32), 0.1, 1.9),
        "w_mix_out": draw_w_mix_out(jax.random.fold_in(keys[15], 71), 0),
        "gain_mix_pre": jnp.clip(1.0 + 0.18 * jax.random.normal(keys[9], (D,), jnp.float32), 0.1, 1.9),
        "gain_mix_post": draw_gain_mix_post(jax.random.fold_in(keys[15], 71), 0),
        "gain_mlp_pre": jnp.clip(1.0 + 0.18 * jax.random.normal(keys[11], (D,), jnp.float32), 0.1, 1.9),
        "gain_mlp_post": jnp.clip(1.0 + 0.18 * jax.random.normal(keys[12], (D,), jnp.float32), 0.1, 1.9),
        "w_up": scatter_about(keys[13], (D, FF), D ** -0.5, 0.125, ((0, 32), (1, 16))),
        "w_down": draw_w_down(jax.random.fold_in(keys[15], 71), 0),
    }


epsilon = 1e-06

def inverse_norm(values):
    return lax.rsqrt(lax.optimization_barrier(jnp.mean(values * values, axis=-1, keepdims=True)) + epsilon)

def reference(residual, prior_state, w_query, w_forget, w_value, w_outgate, forget_floor, group_gain, w_mix_out, gain_mix_pre, gain_mix_post, gain_mlp_pre, gain_mlp_post, w_up, w_down):
    stream = residual.astype(jnp.float32)
    normed = (stream * inverse_norm(stream) * gain_mix_pre).astype(jnp.bfloat16)
    query_pre = jnp.dot(normed, w_query, preferred_element_type=jnp.float32).astype(jnp.bfloat16)
    forget_pre = jnp.dot(normed, w_forget, preferred_element_type=jnp.float32).astype(jnp.bfloat16)
    value_pre = jnp.dot(normed, w_value, preferred_element_type=jnp.float32).astype(jnp.bfloat16)
    gate_pre = jnp.dot(normed, w_outgate, preferred_element_type=jnp.float32).astype(jnp.bfloat16)
    batch_rows = residual.shape[0]
    head_shape = (batch_rows, HEADS, HEAD_DIM)
    query_act = jax.nn.silu(query_pre.astype(jnp.float32)).reshape(head_shape)
    lower_bound = forget_floor.reshape(HEADS, HEAD_DIM)
    forget = lower_bound + (1.0 - lower_bound) * jax.nn.sigmoid(forget_pre.astype(jnp.float32).reshape(head_shape))
    values_in = value_pre.astype(jnp.float32).reshape(head_shape)
    new_state = forget[..., None] * prior_state + (1.0 - forget)[..., None] * values_in[:, :, None, :]
    readout = jnp.einsum('bhk,bhkv->bhv', query_act, new_state, precision=lax.Precision.HIGHEST)
    gate_act = jax.nn.sigmoid(gate_pre.astype(jnp.float32).reshape(head_shape))
    gated_out = (readout * inverse_norm(readout) * group_gain.reshape(HEADS, HEAD_DIM) * gate_act).astype(jnp.bfloat16)
    mixed_sum = jnp.dot(gated_out.reshape(batch_rows, HEADS * HEAD_DIM), w_mix_out, preferred_element_type=jnp.float32)
    after_mix = (stream + mixed_sum * inverse_norm(mixed_sum) * gain_mix_post).astype(jnp.bfloat16)
    after_wide = after_mix.astype(jnp.float32)
    hidden_in = (after_wide * inverse_norm(after_wide) * gain_mlp_pre).astype(jnp.bfloat16)
    up_sum = jnp.dot(hidden_in, w_up, preferred_element_type=jnp.float32)
    squared = jnp.square(jax.nn.relu(up_sum)).astype(jnp.bfloat16)
    channel = jnp.dot(squared, w_down, preferred_element_type=jnp.float32)
    layer_out = (after_wide + channel * gain_mlp_post).astype(jnp.bfloat16)
    return (layer_out, new_state)
```

```python
import jax
import jax.numpy as jnp
from jax import lax
from jax.sharding import Mesh
from jax.sharding import PartitionSpec as P

HEAD_DIM = 128
KV = ("y", "x")
TP = ("z", "c")

epsilon = 1e-06


def inverse_norm(values):
    return lax.rsqrt(jnp.mean(values * values, axis=-1, keepdims=True) + epsilon)


def exchange(blocks, axes):
    return lax.all_to_all(blocks, axes, 0, 0, tiled=True)


def from_everyone(value, axes):
    devices = lax.axis_size(axes)
    return exchange(jnp.broadcast_to(value[None], (devices, *value.shape)), axes)


def shards(
    residual,
    prior_state,
    w_query,
    w_forget,
    w_value,
    w_outgate,
    forget_floor,
    group_gain,
    w_mix_out,
    gain_mix_pre,
    gain_mix_post,
    gain_mlp_pre,
    gain_mlp_post,
    w_up,
    w_down,
):
    batch_rows, own_cols = residual.shape
    groups = lax.axis_size(KV)
    full_width = groups * own_cols
    place = lax.axis_index(KV)
    head_cols = w_query.shape[1]
    hidden = w_up.shape[1]

    own_weights = jnp.concatenate(
        (w_query, w_forget, w_value, w_outgate, w_mix_out.T, w_up, w_down.T), axis=1
    )
    weights = lax.all_gather(own_weights, TP, axis=0, tiled=True)
    at = 4 * head_cols
    w_in = weights[:, :at]
    w_mix = weights[:, at : at + w_mix_out.shape[0]]
    at += w_mix_out.shape[0]
    w_up_all = weights[:, at : at + hidden]
    w_down_all = weights[:, at + hidden :]

    stream = from_everyone(residual, KV).astype(jnp.float32)
    scale = lax.rsqrt(
        jnp.sum(stream * stream, axis=(0, 2), keepdims=True) / full_width + epsilon
    )
    normed = (stream * scale * gain_mix_pre.reshape(groups, 1, own_cols)).astype(jnp.bfloat16)
    normed = normed.transpose(1, 0, 2).reshape(batch_rows, full_width)
    pre = jnp.dot(normed, w_in, preferred_element_type=jnp.float32).astype(jnp.bfloat16)
    query_pre, forget_pre, value_pre, gate_pre = (
        p.astype(jnp.float32) for p in jnp.split(pre, 4, axis=1)
    )
    query = jax.nn.silu(query_pre)
    forget = forget_floor + (1.0 - forget_floor) * jax.nn.sigmoid(forget_pre)
    new_state = (
        forget[:, :, None] * prior_state[:, 0]
        + (1.0 - forget)[:, :, None] * value_pre[:, None, :]
    )
    readout = jnp.einsum("bk,bkv->bv", query, new_state, precision=lax.Precision.HIGHEST)
    gated = (
        readout * inverse_norm(readout) * group_gain * jax.nn.sigmoid(gate_pre)
    ).astype(jnp.bfloat16)
    mixed_part = lax.dot_general(
        gated, w_mix, (((1,), (1,)), ((), ())), preferred_element_type=jnp.float32
    )
    mixed = exchange(
        mixed_part.astype(jnp.bfloat16).reshape(batch_rows, groups, own_cols), KV
    )
    mixed = jnp.sum(mixed.astype(jnp.float32), axis=0)
    mix_scale = lax.rsqrt(jnp.sum(mixed * mixed) / full_width + epsilon)
    own_row = lax.dynamic_index_in_dim(stream, place, 1, keepdims=False)
    after_row = (
        own_row + mixed * mix_scale * gain_mix_post.reshape(groups, own_cols)
    ).astype(jnp.bfloat16)
    after = from_everyone(after_row, KV).astype(jnp.float32)
    after_scale = lax.rsqrt(
        jnp.sum(after * after, axis=(1, 2), keepdims=True) / full_width + epsilon
    )
    hidden_in = (after * after_scale * gain_mlp_pre.reshape(groups, own_cols)).astype(
        jnp.bfloat16
    )
    up_sum = jnp.dot(
        hidden_in.reshape(batch_rows, full_width), w_up_all, preferred_element_type=jnp.float32
    )
    squared = jnp.square(jax.nn.relu(up_sum)).astype(jnp.bfloat16)
    channel_part = lax.dot_general(
        squared, w_down_all, (((1,), (1,)), ((), ())), preferred_element_type=jnp.float32
    )
    channel = exchange(
        channel_part.astype(jnp.bfloat16)
        .reshape(batch_rows, groups, own_cols)
        .transpose(1, 0, 2),
        KV,
    )
    channel = jnp.sum(channel.astype(jnp.float32), axis=0)
    out_gain = lax.dynamic_index_in_dim(
        gain_mlp_post.reshape(groups, own_cols), place, 0, keepdims=True
    )
    after_own = lax.dynamic_index_in_dim(after, place, 1, keepdims=False)
    layer_out = (after_own + channel * out_gain).astype(jnp.bfloat16)
    return layer_out, new_state[:, None]


def solution(mesh):
    grid = Mesh(mesh.devices.reshape(4, 4, 16, 2), (*KV, *TP))
    return jax.shard_map(
        shards,
        mesh=grid,
        in_specs=(
            P(TP, KV),
            P(TP, KV, None, None),
            P(TP, KV),
            P(TP, KV),
            P(TP, KV),
            P(TP, KV),
            P(KV),
            P(KV),
            P(KV, TP),
            P(),
            P(),
            P(),
            P(),
            P(TP, KV),
            P(KV, TP),
        ),
        out_specs=(P(TP, KV), P(TP, KV, None, None)),
        check_vma=False,
    )
```

```python
import jax
import jax.numpy as jnp
from jax import lax
from jax.experimental import pallas as pl
from jax.experimental.pallas import tpu as pltpu
from jax.sharding import Mesh
from jax.sharding import PartitionSpec as P


HEAD_DIM = 128
KV = ("y", "x")
TP = ("za", "zb", "c")
FOUR = 4

epsilon = 1e-06


def exchange(blocks, axes):
    return lax.all_to_all(blocks, axes, 0, 0, tiled=True)


def pack_body(
    residual, wq, wf, wv, wg, mix, up, down, first_ref, mlp_ref, spread_ref, sems
):
    cols = wq.shape[1]
    rows = wq.shape[0]
    part = first_ref.shape[0] - rows
    hidden = up.shape[1]
    copies = [
        (up, mlp_ref.at[:, :hidden]),
        (down, mlp_ref.at[:, hidden:]),
    ]
    for k, w in enumerate((wq, wf, wv, wg)):
        copies.append((w, first_ref.at[:rows, k * cols : (k + 1) * cols]))
    for k in range(FOUR):
        copies.append(
            (
                mix.at[k * part : (k + 1) * part],
                first_ref.at[rows:, k * cols : (k + 1) * cols],
            )
        )
    started = [
        pltpu.make_async_copy(src, dst, sems.at[k]) for k, (src, dst) in enumerate(copies)
    ]
    for copy in started:
        copy.start()
    spread_ref[...] = jnp.broadcast_to(residual[...][None], spread_ref.shape)
    for copy in started:
        copy.wait()


def pack(residual, wq, wf, wv, wg, mix, up, down, groups):
    rows, cols = wq.shape
    part = mix.shape[0] // FOUR
    anywhere = pl.BlockSpec(memory_space=pl.ANY)
    vmem = pl.BlockSpec(memory_space=pltpu.VMEM)
    return pl.pallas_call(
        pack_body,
        out_shape=(
            jax.ShapeDtypeStruct((rows + part, 4 * cols), wq.dtype),
            jax.ShapeDtypeStruct((rows, up.shape[1] + down.shape[1]), wq.dtype),
            jax.ShapeDtypeStruct((groups, *residual.shape), residual.dtype),
        ),
        in_specs=[vmem] + [anywhere] * 7,
        out_specs=(anywhere, anywhere, vmem),
        scratch_shapes=[pltpu.SemaphoreType.DMA((10,))],
        name="pack",
    )(residual, wq, wf, wv, wg, mix, up, down)


def project_body(x_ref, w_ref, out_ref):
    za = lax.axis_index("za")
    rows = w_ref.shape[2] // 5 * 4
    total = None
    for r in range(FOUR):
        f = lax.rem(za + r, FOUR)
        x = jnp.concatenate([x_ref[k, f] for k in range(FOUR)], axis=0)
        w = jnp.concatenate([w_ref[c, r, :rows] for c in range(2)], axis=0)
        term = jnp.dot(x, w, preferred_element_type=jnp.float32)
        total = term if total is None else total + term
    height = x_ref.shape[2]
    for k in range(FOUR):
        out_ref[k] = total[k * height : (k + 1) * height].astype(out_ref.dtype)


def project(x, w):
    return pl.pallas_call(
        project_body,
        out_shape=jax.ShapeDtypeStruct((FOUR, x.shape[2], w.shape[3]), jnp.bfloat16),
        name="project",
    )(x, w)


def recur_body(part_ref, prior_ref, floor_ref, gain_ref, state_ref, out_ref, read_ref):
    pre = part_ref[0].astype(jnp.float32)
    for k in range(1, FOUR):
        pre = pre + part_ref[k].astype(jnp.float32)
    pre = pre.astype(jnp.bfloat16).astype(jnp.float32)
    width = prior_ref.shape[1]
    query = jax.nn.silu(pre[:, :width])
    floor = floor_ref[...]
    forget = floor + (1.0 - floor) * jax.nn.sigmoid(pre[:, width : 2 * width])
    value = pre[:, 2 * width : 3 * width]
    gate = jax.nn.sigmoid(pre[:, 3 * width :])
    forget_t = forget.T
    query_t = query.T
    for b in range(prior_ref.shape[0]):
        keep = forget_t[:, b : b + 1]
        state = keep * prior_ref[b] + (1.0 - keep) * value[b : b + 1]
        state_ref[b] = state
        read_ref[b : b + 1] = jnp.sum(query_t[:, b : b + 1] * state, axis=0, keepdims=True)
    read = read_ref[...]
    scale = lax.rsqrt(jnp.mean(read * read, axis=-1, keepdims=True) + epsilon)
    out_ref[...] = (read * scale * gain_ref[...] * gate).astype(out_ref.dtype)


def recur(part, prior, floor, gain):
    rows, width, _ = prior.shape
    return pl.pallas_call(
        recur_body,
        out_shape=(
            jax.ShapeDtypeStruct(prior.shape, jnp.float32),
            jax.ShapeDtypeStruct((rows, width), jnp.bfloat16),
        ),
        scratch_shapes=[pltpu.VMEM((rows, width), jnp.float32)],
        name="recur",
    )(part, prior, floor, gain)


def mix_body(gated_ref, w_ref, out_ref, order_ref):
    height, width = gated_ref.shape[1:]
    for k in range(FOUR):
        order_ref[pl.ds(k, height, stride=FOUR)] = gated_ref[k].astype(jnp.float32)
    left = order_ref[...].astype(jnp.bfloat16)
    rows = w_ref.shape[2] // 5 * 4
    for r in range(FOUR):
        right = jnp.concatenate(
            [
                w_ref[c, r, rows:, k * width : (k + 1) * width]
                for c in range(2)
                for k in range(FOUR)
            ],
            axis=0,
        )
        out_ref[pl.ds(r, FOUR * height, stride=FOUR)] = lax.dot_general(
            left, right, (((1,), (1,)), ((), ())), preferred_element_type=jnp.float32
        )


def mix_out(gated, w):
    height, width = gated.shape[1:]
    return pl.pallas_call(
        mix_body,
        out_shape=jax.ShapeDtypeStruct((FOUR * FOUR * height, width), jnp.float32),
        scratch_shapes=[pltpu.VMEM((FOUR * height, width), jnp.float32)],
        name="mix_out",
    )(gated, w)


def row_body(sums_ref, stream_ref, gain_ref, out_ref, mixed_ref):
    za = lax.axis_index("za")
    place = lax.axis_index("y") * lax.axis_size("x") + lax.axis_index("x")
    groups = gain_ref.shape[0]
    total = sums_ref[:groups]
    for k in range(1, groups):
        total = total + sums_ref[k * groups : (k + 1) * groups]
    scale = lax.rsqrt(jnp.sum(total * total) / gain_ref.size + epsilon)
    for zb in range(FOUR):
        for r in range(FOUR):
            k = zb * FOUR + r
            mixed_ref[pl.ds(lax.rem(za + r, FOUR) * FOUR + zb, 1)] = total[k : k + 1]
    row = stream_ref[:, pl.ds(place, 1), :].reshape(gain_ref.shape)
    after = (row + mixed_ref[...] * scale * gain_ref[...]).astype(out_ref.dtype)
    out_ref[...] = jnp.broadcast_to(after[None], out_ref.shape)


def row_update(sums, stream, gain):
    groups, width = gain.shape
    return pl.pallas_call(
        row_body,
        out_shape=jax.ShapeDtypeStruct((groups, groups, width), jnp.bfloat16),
        scratch_shapes=[pltpu.VMEM((groups, width), jnp.float32)],
        name="row_update",
    )(sums, stream, gain)


def shards(
    residual,
    prior_state,
    w_query,
    w_forget,
    w_value,
    w_outgate,
    forget_floor,
    group_gain,
    w_mix_out,
    gain_mix_pre,
    gain_mix_post,
    gain_mlp_pre,
    gain_mlp_post,
    w_up,
    w_down,
):
    batch_rows, own_cols = residual.shape
    groups = lax.axis_size(KV)
    full_width = groups * own_cols
    place = lax.axis_index(KV)
    hidden = w_up.shape[1]

    first, mlp, spread = pack(
        residual, w_query, w_forget, w_value, w_outgate, w_mix_out.T, w_up, w_down.T, groups
    )
    mlp_weights = lax.all_gather(mlp, TP, axis=0, tiled=True)
    weights = jnp.stack(
        [first]
        + [
            lax.ppermute(first, "za", [((k + r) % FOUR, k) for k in range(FOUR)])
            for r in range(1, FOUR)
        ]
    )
    weights = lax.all_gather(weights, "c", axis=0)

    stream = exchange(spread, KV).astype(jnp.float32)
    scale = lax.rsqrt(
        jnp.sum(stream * stream, axis=(0, 2), keepdims=True) / full_width + epsilon
    )
    normed = (stream * scale * gain_mix_pre.reshape(groups, 1, own_cols)).astype(jnp.bfloat16)
    normed = normed.reshape(FOUR, FOUR, batch_rows, own_cols).transpose(1, 0, 2, 3)
    part = exchange(project(exchange(normed, "zb"), weights), "zb")
    new_state, gated = recur(
        part, prior_state[:, 0], forget_floor[None], group_gain[None]
    )
    gated = exchange(jnp.broadcast_to(gated[None], (FOUR, *gated.shape)), "zb")
    mixed_part = mix_out(gated, weights).reshape(groups * FOUR, FOUR, own_cols)
    mixed = exchange(mixed_part, (*KV, "zb")).reshape(-1, own_cols)
    after_row = row_update(mixed, stream, gain_mix_post.reshape(groups, own_cols))
    after = exchange(after_row, KV).astype(jnp.float32)
    after_scale = lax.rsqrt(
        jnp.sum(after * after, axis=(1, 2), keepdims=True) / full_width + epsilon
    )
    hidden_in = (after * after_scale * gain_mlp_pre.reshape(groups, own_cols)).astype(
        jnp.bfloat16
    )
    up_sum = jnp.dot(
        hidden_in.reshape(batch_rows, full_width),
        mlp_weights[:, :hidden],
        preferred_element_type=jnp.float32,
    )
    squared = jnp.square(jax.nn.relu(up_sum)).astype(jnp.bfloat16)
    channel_part = lax.dot_general(
        squared,
        mlp_weights[:, hidden:],
        (((1,), (1,)), ((), ())),
        preferred_element_type=jnp.float32,
    )
    channel = exchange(
        channel_part.astype(jnp.bfloat16)
        .reshape(batch_rows, groups, own_cols)
        .transpose(1, 0, 2),
        KV,
    )
    channel = jnp.sum(channel.astype(jnp.float32), axis=0)
    out_gain = lax.dynamic_index_in_dim(
        gain_mlp_post.reshape(groups, own_cols), place, 0, keepdims=True
    )
    after_own = lax.dynamic_index_in_dim(after, place, 1, keepdims=False)
    layer_out = (after_own + channel * out_gain).astype(jnp.bfloat16)
    return layer_out, new_state[:, None]


def solution(mesh):
    grid = Mesh(mesh.devices.reshape(4, 4, FOUR, FOUR, 2), (*KV, *TP))
    return jax.shard_map(
        shards,
        mesh=grid,
        in_specs=(
            P(TP, KV),
            P(TP, KV, None, None),
            P(TP, KV),
            P(TP, KV),
            P(TP, KV),
            P(TP, KV),
            P(KV),
            P(KV),
            P(KV, TP),
            P(),
            P(),
            P(),
            P(),
            P(TP, KV),
            P(KV, TP),
        ),
        out_specs=(P(TP, KV), P(TP, KV, None, None)),
        check_vma=False,
    )
```

```python
import jax
import jax.numpy as jnp
from jax import lax
from jax.experimental import pallas as pl
from jax.experimental.pallas import tpu as pltpu
from jax.sharding import Mesh
from jax.sharding import PartitionSpec as P

KV = ("y", "x")
TP = ("zh", "zo", "c")
HALVES = 2
CHIPS = 8
CORES = 2
EARLY = 48

epsilon = 1e-06


def exchange(blocks, axes):
    return lax.all_to_all(blocks, axes, 0, 0, tiled=True)


def pack_body(
    residual, wq, wf, wv, wg, mix, up, down, early_ref, late_ref, mlp_ref, spread_ref, sems
):
    rows, cols = wq.shape
    rest = rows - EARLY
    part = mix.shape[0] // 4
    hidden = up.shape[1]
    copies = [
        (up, mlp_ref.at[:, :hidden]),
        (down, mlp_ref.at[:, hidden:]),
    ]
    for k, w in enumerate((wq, wf, wv, wg)):
        at = slice(k * cols, (k + 1) * cols)
        copies.append((w.at[:EARLY], early_ref.at[:, at]))
        copies.append((w.at[EARLY:], late_ref.at[:rest, at]))
        copies.append((mix.at[k * part : (k + 1) * part], late_ref.at[rest:, at]))
    started = [
        pltpu.make_async_copy(src, dst, sems.at[k]) for k, (src, dst) in enumerate(copies)
    ]
    for copy in started:
        copy.start()
    spread_ref[...] = jnp.broadcast_to(residual[...][None], spread_ref.shape)
    for copy in started:
        copy.wait()


def pack(residual, wq, wf, wv, wg, mix, up, down, peers):
    rows, cols = wq.shape
    late = rows - EARLY + mix.shape[0] // 4
    anywhere = pl.BlockSpec(memory_space=pl.ANY)
    vmem = pl.BlockSpec(memory_space=pltpu.VMEM)
    return pl.pallas_call(
        pack_body,
        out_shape=(
            jax.ShapeDtypeStruct((EARLY, 4 * cols), wq.dtype),
            jax.ShapeDtypeStruct((late, 4 * cols), wq.dtype),
            jax.ShapeDtypeStruct((rows, up.shape[1] + down.shape[1]), wq.dtype),
            jax.ShapeDtypeStruct((peers, *residual.shape), residual.dtype),
        ),
        in_specs=[vmem] + [anywhere] * 7,
        out_specs=(vmem, vmem, vmem, vmem),
        scratch_shapes=[pltpu.SemaphoreType.DMA((14,))],
        name="pack",
    )(residual, wq, wf, wv, wg, mix, up, down)


def project_body(x_ref, gain_ref, early_ref, late_ref, own_ref, send_ref):
    zo = lax.axis_index("zo")
    groups, _, height, width = x_ref.shape
    rest = late_ref.shape[2] // 2
    squares = [None] * HALVES
    for f in range(groups):
        for h in range(HALVES):
            x = x_ref[f, h].astype(jnp.float32)
            squares[h] = x * x if f == 0 else squares[h] + x * x
    scale = [
        lax.rsqrt(jnp.sum(s, axis=-1, keepdims=True) / (groups * width) + epsilon)
        for s in squares
    ]
    total = None
    for k in range(CHIPS):
        f = HALVES * k + zo
        gain = gain_ref[pl.ds(f, 1)]
        x = jnp.concatenate(
            [
                (x_ref[f, h].astype(jnp.float32) * scale[h] * gain).astype(jnp.bfloat16)
                for h in range(HALVES)
            ],
            axis=0,
        )
        w = jnp.concatenate(
            [
                piece
                for c in range(CORES)
                for piece in (early_ref[k, c], late_ref[k, c, :rest])
            ],
            axis=0,
        )
        term = jnp.dot(x, w, preferred_element_type=jnp.float32)
        total = term if total is None else total + term
    mine = jnp.where(zo == 0, total[:height], total[height:])
    other = jnp.where(zo == 0, total[height:], total[:height])
    own_ref[...] = mine
    send_ref[...] = other.astype(send_ref.dtype)


def project(x, gain, early, late):
    height = x.shape[2]
    cols = early.shape[3]
    return pl.pallas_call(
        project_body,
        out_shape=(
            jax.ShapeDtypeStruct((height, cols), jnp.float32),
            jax.ShapeDtypeStruct((height, cols), jnp.bfloat16),
        ),
        name="project",
    )(x, gain, early, late)


def recur_body(
    own_ref, part_ref, prior_ref, floor_ref, gain_ref, state_ref, out_ref, read_ref
):
    zo = lax.axis_index("zo")
    pre = own_ref[...] + part_ref[1 - zo].astype(jnp.float32)
    pre = pre.astype(jnp.bfloat16).astype(jnp.float32)
    width = prior_ref.shape[1]
    query = jax.nn.silu(pre[:, :width])
    floor = floor_ref[...]
    forget = floor + (1.0 - floor) * jax.nn.sigmoid(pre[:, width : 2 * width])
    value = pre[:, 2 * width : 3 * width]
    gate = jax.nn.sigmoid(pre[:, 3 * width :])
    forget_t = forget.T
    query_t = query.T
    for b in range(prior_ref.shape[0]):
        keep = forget_t[:, b : b + 1]
        state = keep * prior_ref[b] + (1.0 - keep) * value[b : b + 1]
        state_ref[b] = state
        read_ref[b : b + 1] = jnp.sum(query_t[:, b : b + 1] * state, axis=0, keepdims=True)
    read = read_ref[...]
    scale = lax.rsqrt(jnp.mean(read * read, axis=-1, keepdims=True) + epsilon)
    out_ref[...] = (read * scale * gain_ref[...] * gate).astype(out_ref.dtype)


def recur(own, part, prior, floor, gain):
    rows, width, _ = prior.shape
    return pl.pallas_call(
        recur_body,
        out_shape=(
            jax.ShapeDtypeStruct(prior.shape, jnp.float32),
            jax.ShapeDtypeStruct((rows, width), jnp.bfloat16),
        ),
        scratch_shapes=[pltpu.VMEM((rows, width), jnp.float32)],
        name="recur",
    )(own, part, prior, floor, gain)


def mix_body(gated_ref, late_ref, out_ref, order_ref):
    height, width = gated_ref.shape[1:]
    rest = late_ref.shape[2] // 2
    for h in range(HALVES):
        order_ref[pl.ds(h, height, stride=HALVES)] = gated_ref[h].astype(jnp.float32)
    left = order_ref[...].astype(jnp.bfloat16)
    for k in range(CHIPS):
        right = jnp.concatenate(
            [
                late_ref[k, c, rest:, j * width : (j + 1) * width]
                for c in range(CORES)
                for j in range(4)
            ],
            axis=0,
        )
        out_ref[pl.ds(k, HALVES * height, stride=CHIPS)] = lax.dot_general(
            left, right, (((1,), (1,)), ((), ())), preferred_element_type=jnp.float32
        )


def mix_out(gated, late):
    height, width = gated.shape[1:]
    return pl.pallas_call(
        mix_body,
        out_shape=jax.ShapeDtypeStruct((CHIPS * HALVES * height, width), jnp.float32),
        scratch_shapes=[pltpu.VMEM((HALVES * height, width), jnp.float32)],
        name="mix_out",
    )(gated, late)


def row_body(sums_ref, x_ref, gain_ref, out_ref, mixed_ref):
    zo = lax.axis_index("zo")
    place = lax.axis_index("y") * lax.axis_size("x") + lax.axis_index("x")
    groups, width = gain_ref.shape
    for h in range(HALVES):
        total = sums_ref[0, h]
        for k in range(1, groups):
            total = total + sums_ref[k, h]
        mixed_ref[pl.ds(h, CHIPS, stride=HALVES)] = total
    mixed = mixed_ref[...]
    scale = lax.rsqrt(jnp.sum(mixed * mixed) / gain_ref.size + epsilon)
    stream = x_ref[:, zo].astype(jnp.float32)
    at = lax.broadcasted_iota(jnp.int32, stream.shape, 1) == place
    row = jnp.sum(jnp.where(at, stream, 0.0), axis=1)
    after = (row + mixed * scale * gain_ref[...]).astype(out_ref.dtype)
    out_ref[...] = jnp.broadcast_to(after[None], out_ref.shape)


def row_update(sums, x, gain):
    groups, width = gain.shape
    return pl.pallas_call(
        row_body,
        out_shape=jax.ShapeDtypeStruct((groups, groups, width), jnp.bfloat16),
        scratch_shapes=[pltpu.VMEM((groups, width), jnp.float32)],
        name="row_update",
    )(sums, x, gain)


def shards(
    residual,
    prior_state,
    w_query,
    w_forget,
    w_value,
    w_outgate,
    forget_floor,
    group_gain,
    w_mix_out,
    gain_mix_pre,
    gain_mix_post,
    gain_mlp_pre,
    gain_mlp_post,
    w_up,
    w_down,
):
    batch_rows, own_cols = residual.shape
    groups = lax.axis_size(KV)
    full_width = groups * own_cols
    place = lax.axis_index(KV)
    hidden = w_up.shape[1]

    early, late, mlp, spread = pack(
        residual,
        w_query,
        w_forget,
        w_value,
        w_outgate,
        w_mix_out.T,
        w_up,
        w_down.T,
        groups * HALVES,
    )
    mlp_weights = lax.all_gather(mlp, TP, axis=0, tiled=True)
    stream = exchange(spread, (*KV, "zo")).reshape(groups, HALVES, batch_rows, own_cols)
    early = lax.all_gather(early, ("zh", "c"), axis=0).reshape(CHIPS, CORES, *early.shape)
    late = lax.all_gather(late, ("zh", "c"), axis=0).reshape(CHIPS, CORES, *late.shape)
    own, send = project(stream, gain_mix_pre.reshape(groups, own_cols), early, late)
    part = lax.all_gather(send, "zo", axis=0)
    new_state, gated = recur(
        own, part, prior_state[:, 0], forget_floor[None], group_gain[None]
    )
    gated = lax.all_gather(gated, "zo", axis=0)
    mixed_part = mix_out(gated, late).reshape(groups * HALVES, CHIPS, own_cols)
    mixed = exchange(mixed_part, (*KV, "zo")).reshape(groups, HALVES, CHIPS, own_cols)
    after_row = row_update(mixed, stream, gain_mix_post.reshape(groups, own_cols))
    after = exchange(after_row, KV).astype(jnp.float32)
    after_scale = lax.rsqrt(
        jnp.sum(after * after, axis=(1, 2), keepdims=True) / full_width + epsilon
    )
    hidden_in = (after * after_scale * gain_mlp_pre.reshape(groups, own_cols)).astype(
        jnp.bfloat16
    )
    up_sum = jnp.dot(
        hidden_in.reshape(batch_rows, full_width),
        mlp_weights[:, :hidden],
        preferred_element_type=jnp.float32,
    )
    squared = jnp.square(jax.nn.relu(up_sum)).astype(jnp.bfloat16)
    channel_part = lax.dot_general(
        squared,
        mlp_weights[:, hidden:],
        (((1,), (1,)), ((), ())),
        preferred_element_type=jnp.float32,
    )
    channel = exchange(
        channel_part.astype(jnp.bfloat16)
        .reshape(batch_rows, groups, own_cols)
        .transpose(1, 0, 2),
        KV,
    )
    channel = jnp.sum(channel.astype(jnp.float32), axis=0)
    out_gain = lax.dynamic_index_in_dim(
        gain_mlp_post.reshape(groups, own_cols), place, 0, keepdims=True
    )
    after_own = lax.dynamic_index_in_dim(after, place, 1, keepdims=False)
    layer_out = (after_own + channel * out_gain).astype(jnp.bfloat16)
    return layer_out, new_state[:, None]


def solution(mesh):
    grid = Mesh(mesh.devices.reshape(4, 4, CHIPS, HALVES, CORES), (*KV, *TP))
    return jax.shard_map(
        shards,
        mesh=grid,
        in_specs=(
            P(TP, KV),
            P(TP, KV, None, None),
            P(TP, KV),
            P(TP, KV),
            P(TP, KV),
            P(TP, KV),
            P(KV),
            P(KV),
            P(KV, TP),
            P(),
            P(),
            P(),
            P(),
            P(TP, KV),
            P(KV, TP),
        ),
        out_specs=(P(TP, KV), P(TP, KV, None, None)),
        check_vma=False,
    )
```

```python
import jax
import jax.numpy as jnp
from jax import lax
from jax.experimental import pallas as pl
from jax.experimental.pallas import tpu as pltpu
from jax.sharding import Mesh
from jax.sharding import PartitionSpec as P

KV = ("y", "x")
TP = ("zh", "zo", "c")
HALVES = 2
CHIPS = 8
CORES = 2
EARLY = 48

epsilon = 1e-06


def exchange(blocks, axes):
    return lax.all_to_all(blocks, axes, 0, 0, tiled=True)


def near(value):
    return pltpu.with_memory_space_constraint(value, pltpu.VMEM)


def run_copies(copies, sems):
    started = [
        pltpu.make_async_copy(src, dst, sems.at[k]) for k, (src, dst) in enumerate(copies)
    ]
    for copy in started:
        copy.start()
    return started


def pack_long_body(up, down, mix, out_ref, sems):
    hidden = up.shape[1]
    copies = [
        (up, out_ref.at[:, :hidden]),
        (down, out_ref.at[:, hidden : 2 * hidden]),
        (mix, out_ref.at[:, 2 * hidden :]),
    ]
    for copy in run_copies(copies, sems):
        copy.wait()


def pack_long(up, down, mix):
    anywhere = pl.BlockSpec(memory_space=pl.ANY)
    rows = up.shape[0]
    return pl.pallas_call(
        pack_long_body,
        out_shape=jax.ShapeDtypeStruct(
            (rows, up.shape[1] + down.shape[1] + mix.shape[1]), up.dtype
        ),
        in_specs=[anywhere] * 3,
        out_specs=pl.BlockSpec(memory_space=pltpu.VMEM),
        scratch_shapes=[pltpu.SemaphoreType.DMA((3,))],
        name="pack_long",
    )(up, down, mix)


def pack_body(residual, wq, wf, wv, wg, early_ref, late_ref, spread_ref, sems):
    cols = wq.shape[1]
    copies = []
    for k, w in enumerate((wq, wf, wv, wg)):
        at = slice(k * cols, (k + 1) * cols)
        copies.append((w.at[:EARLY], early_ref.at[:, at]))
        copies.append((w.at[EARLY:], late_ref.at[:, at]))
    started = run_copies(copies, sems)
    spread_ref[...] = jnp.broadcast_to(residual[...][None], spread_ref.shape)
    for copy in started:
        copy.wait()


def pack(residual, wq, wf, wv, wg, peers):
    rows, cols = wq.shape
    anywhere = pl.BlockSpec(memory_space=pl.ANY)
    vmem = pl.BlockSpec(memory_space=pltpu.VMEM)
    return pl.pallas_call(
        pack_body,
        out_shape=(
            pltpu.VMEM((EARLY, 4 * cols), wq.dtype),
            pltpu.VMEM((rows - EARLY, 4 * cols), wq.dtype),
            pltpu.VMEM((peers, *residual.shape), residual.dtype),
        ),
        in_specs=[vmem] + [anywhere] * 4,
        out_specs=(vmem, vmem, vmem),
        scratch_shapes=[pltpu.SemaphoreType.DMA((8,))],
        name="pack",
    )(residual, wq, wf, wv, wg)


def project_body(x_ref, gain_ref, early_ref, late_ref, own_ref, send_ref):
    zo = lax.axis_index("zo")
    groups, _, height, width = x_ref.shape
    squares = [None] * HALVES
    for f in range(groups):
        for h in range(HALVES):
            x = x_ref[f, h].astype(jnp.float32)
            squares[h] = x * x if f == 0 else squares[h] + x * x
    scale = [
        lax.rsqrt(jnp.sum(s, axis=-1, keepdims=True) / (groups * width) + epsilon)
        for s in squares
    ]
    total = None
    for k in range(CHIPS):
        f = HALVES * k + zo
        gain = gain_ref[pl.ds(f, 1)]
        x = jnp.concatenate(
            [
                (x_ref[f, h].astype(jnp.float32) * scale[h] * gain).astype(jnp.bfloat16)
                for h in range(HALVES)
            ],
            axis=0,
        )
        w = jnp.concatenate(
            [
                piece
                for c in range(CORES)
                for piece in (early_ref[k, c], late_ref[k, c])
            ],
            axis=0,
        )
        term = jnp.dot(x, w, preferred_element_type=jnp.float32)
        total = term if total is None else total + term
    mine = jnp.where(zo == 0, total[:height], total[height:])
    other = jnp.where(zo == 0, total[height:], total[:height])
    own_ref[...] = mine
    send_ref[...] = other.astype(send_ref.dtype)


def project(x, gain, early, late):
    height = x.shape[2]
    cols = early.shape[3]
    return pl.pallas_call(
        project_body,
        out_shape=(
            pltpu.VMEM((height, cols), jnp.float32),
            pltpu.VMEM((height, cols), jnp.bfloat16),
        ),
        name="project",
    )(near(x), gain, near(early), near(late))


def recur_body(
    own_ref, part_ref, prior_ref, floor_ref, gain_ref, state_ref, out_ref, read_ref
):
    zo = lax.axis_index("zo")
    pre = own_ref[...] + part_ref[1 - zo].astype(jnp.float32)
    pre = pre.astype(jnp.bfloat16).astype(jnp.float32)
    width = prior_ref.shape[1]
    query = jax.nn.silu(pre[:, :width])
    floor = floor_ref[...]
    forget = floor + (1.0 - floor) * jax.nn.sigmoid(pre[:, width : 2 * width])
    value = pre[:, 2 * width : 3 * width]
    gate = jax.nn.sigmoid(pre[:, 3 * width :])
    forget_t = forget.T
    query_t = query.T
    for b in range(prior_ref.shape[0]):
        keep = forget_t[:, b : b + 1]
        state = keep * prior_ref[b] + (1.0 - keep) * value[b : b + 1]
        state_ref[b] = state
        read_ref[b : b + 1] = jnp.sum(query_t[:, b : b + 1] * state, axis=0, keepdims=True)
    read = read_ref[...]
    scale = lax.rsqrt(jnp.mean(read * read, axis=-1, keepdims=True) + epsilon)
    out_ref[...] = (read * scale * gain_ref[...] * gate).astype(out_ref.dtype)


def recur(own, part, prior, floor, gain):
    rows, width, _ = prior.shape
    return pl.pallas_call(
        recur_body,
        out_shape=(
            jax.ShapeDtypeStruct(prior.shape, jnp.float32),
            pltpu.VMEM((rows, width), jnp.bfloat16),
        ),
        scratch_shapes=[pltpu.VMEM((rows, width), jnp.float32)],
        name="recur",
    )(near(own), near(part), near(prior), floor, gain)


def mix_body(gated_ref, long_ref, out_ref, w_ref, sem):
    peers, groups, _, width = out_ref.shape
    copy = pltpu.make_async_copy(long_ref.at[:, long_ref.shape[1] - width :], w_ref, sem)
    copy.start()
    copy.wait()
    for f in range(groups):
        part = lax.dot_general(
            gated_ref[...],
            w_ref[f * width : (f + 1) * width],
            (((1,), (1,)), ((), ())),
            preferred_element_type=jnp.float32,
        ).astype(out_ref.dtype)
        for peer in range(peers):
            out_ref[peer, f] = part


def mix_out(gated, weights, groups):
    rows, width = gated.shape
    return pl.pallas_call(
        mix_body,
        out_shape=pltpu.VMEM((groups, groups, rows, width), jnp.bfloat16),
        in_specs=[
            pl.BlockSpec(memory_space=pltpu.VMEM),
            pl.BlockSpec(memory_space=pl.ANY),
        ],
        scratch_shapes=[
            pltpu.VMEM((weights.shape[0], width), jnp.bfloat16),
            pltpu.SemaphoreType.DMA(()),
        ],
        name="mix_out",
    )(near(gated), weights)


def mlp_body(
    parts_ref,
    x_ref,
    post_ref,
    pre_ref,
    long_ref,
    out_ref,
    own_ref,
    after_ref,
    up_ref,
    down_ref,
    sems,
):
    zo = lax.axis_index("zo")
    place = lax.axis_index("y") * lax.axis_size("x") + lax.axis_index("x")
    groups, width = pre_ref.shape
    full = groups * width
    units = up_ref.shape[1]
    copies = run_copies(
        [
            (long_ref.at[:, :units], up_ref),
            (long_ref.at[:, units : 2 * units], down_ref),
        ],
        sems,
    )
    squares = None
    mixed = []
    for f in range(groups):
        total = parts_ref[0, f].astype(jnp.float32)
        for k in range(1, groups):
            total = total + parts_ref[k, f].astype(jnp.float32)
        mixed.append(total)
        squares = total * total if f == 0 else squares + total * total
    scale = lax.rsqrt(jnp.sum(squares, axis=-1, keepdims=True) / full + epsilon)
    for f in range(groups):
        x = x_ref[f, zo].astype(jnp.float32)
        after = x + mixed[f] * scale * post_ref[f : f + 1]
        after = after.astype(jnp.bfloat16).astype(jnp.float32)
        after_ref[f] = after
        squares = after * after if f == 0 else squares + after * after
    scale = lax.rsqrt(jnp.sum(squares, axis=-1, keepdims=True) / full + epsilon)
    hidden = jnp.concatenate(
        [
            (after_ref[f] * scale * pre_ref[f : f + 1]).astype(jnp.bfloat16)
            for f in range(groups)
        ],
        axis=1,
    )
    copies[0].wait()
    up = jnp.dot(hidden, up_ref[...], preferred_element_type=jnp.float32)
    squared = jnp.square(jnp.maximum(up, 0.0)).astype(jnp.bfloat16)
    copies[1].wait()
    channel = lax.dot_general(
        squared, down_ref[...], (((1,), (1,)), ((), ())), preferred_element_type=jnp.float32
    )
    for f in range(groups):
        out_ref[f] = channel[:, f * width : (f + 1) * width].astype(out_ref.dtype)
    own_ref[...] = after_ref[place]


def mlp(parts, x, post, pre, weights, hidden):
    groups, _, rows, width = parts.shape
    vmem = pl.BlockSpec(memory_space=pltpu.VMEM)
    return pl.pallas_call(
        mlp_body,
        out_shape=(
            pltpu.VMEM((groups, rows, width), jnp.bfloat16),
            pltpu.VMEM((rows, width), jnp.float32),
        ),
        in_specs=[vmem] * 4 + [pl.BlockSpec(memory_space=pl.ANY)],
        scratch_shapes=[
            pltpu.VMEM((groups, rows, width), jnp.float32),
            pltpu.VMEM((weights.shape[0], hidden), jnp.bfloat16),
            pltpu.VMEM((weights.shape[0], hidden), jnp.bfloat16),
            pltpu.SemaphoreType.DMA((2,)),
        ],
        name="mlp",
    )(near(parts), near(x), post, pre, weights)


def shards(
    residual,
    prior_state,
    w_query,
    w_forget,
    w_value,
    w_outgate,
    forget_floor,
    group_gain,
    w_mix_out,
    gain_mix_pre,
    gain_mix_post,
    gain_mlp_pre,
    gain_mlp_post,
    w_up,
    w_down,
):
    batch_rows, own_cols = residual.shape
    groups = lax.axis_size(KV)
    place = lax.axis_index(KV)
    hidden = w_up.shape[1]

    long = lax.all_gather(
        pack_long(w_up, w_down.T, w_mix_out.T), TP, axis=0, tiled=True
    )
    early, late, spread = pack(
        residual, w_query, w_forget, w_value, w_outgate, groups * HALVES
    )
    stream = exchange(spread, (*KV, "zo")).reshape(groups, HALVES, batch_rows, own_cols)
    early = lax.all_gather(early, ("zh", "c"), axis=0).reshape(CHIPS, CORES, *early.shape)
    late = lax.all_gather(late, ("zh", "c"), axis=0).reshape(CHIPS, CORES, *late.shape)
    own, send = project(stream, gain_mix_pre.reshape(groups, own_cols), early, late)
    part = lax.all_gather(send, "zo", axis=0)
    new_state, gated = recur(
        own, part, prior_state[:, 0], forget_floor[None], group_gain[None]
    )
    mixed = exchange(mix_out(gated, long, groups), KV)
    channel_part, after_own = mlp(
        mixed,
        stream,
        gain_mix_post.reshape(groups, own_cols),
        gain_mlp_pre.reshape(groups, own_cols),
        long,
        hidden,
    )
    channel = jnp.sum(exchange(channel_part, KV).astype(jnp.float32), axis=0)
    out_gain = lax.dynamic_index_in_dim(
        gain_mlp_post.reshape(groups, own_cols), place, 0, keepdims=True
    )
    layer_out = (after_own + channel * out_gain).astype(jnp.bfloat16)
    return layer_out, new_state[:, None]


def solution(mesh):
    grid = Mesh(mesh.devices.reshape(4, 4, CHIPS, HALVES, CORES), (*KV, *TP))
    return jax.shard_map(
        shards,
        mesh=grid,
        in_specs=(
            P(TP, KV),
            P(TP, KV, None, None),
            P(TP, KV),
            P(TP, KV),
            P(TP, KV),
            P(TP, KV),
            P(KV),
            P(KV),
            P(KV, TP),
            P(),
            P(),
            P(),
            P(),
            P(TP, KV),
            P(KV, TP),
        ),
        out_specs=(P(TP, KV), P(TP, KV, None, None)),
        check_vma=False,
    )
```

```python
import jax
import jax.numpy as jnp
from jax import lax
from jax.experimental import pallas as pl
from jax.experimental.pallas import tpu as pltpu
from jax.sharding import Mesh
from jax.sharding import PartitionSpec as P

KV = ("y", "x")
TP = ("zh", "zo", "c")
HALVES = 2
CHIPS = 8
CORES = 2
EARLY = 48

epsilon = 1e-06


def exchange(blocks, axes):
    return lax.all_to_all(blocks, axes, 0, 0, tiled=True)


def near(value):
    return pltpu.with_memory_space_constraint(value, pltpu.VMEM)


def run_copies(copies, sems):
    started = [
        pltpu.make_async_copy(src, dst, sems.at[k]) for k, (src, dst) in enumerate(copies)
    ]
    for copy in started:
        copy.start()
    return started


def pack_long_body(up, down, out_ref, sems):
    hidden = up.shape[1]
    copies = [
        (up, out_ref.at[:, :hidden]),
        (down, out_ref.at[:, hidden:]),
    ]
    for copy in run_copies(copies, sems):
        copy.wait()


def pack_long(up, down):
    anywhere = pl.BlockSpec(memory_space=pl.ANY)
    rows = up.shape[0]
    return pl.pallas_call(
        pack_long_body,
        out_shape=jax.ShapeDtypeStruct((rows, up.shape[1] + down.shape[1]), up.dtype),
        in_specs=[anywhere] * 2,
        out_specs=pl.BlockSpec(memory_space=pltpu.VMEM),
        scratch_shapes=[pltpu.SemaphoreType.DMA((2,))],
        name="pack_long",
    )(up, down)


def pack_body(residual, wq, wf, wv, wg, mix, early_ref, late_ref, spread_ref, sems):
    rows, cols = wq.shape
    rest = rows - EARLY
    part = mix.shape[0] // 4
    copies = []
    for k, w in enumerate((wq, wf, wv, wg)):
        at = slice(k * cols, (k + 1) * cols)
        copies.append((w.at[:EARLY], early_ref.at[:, at]))
        copies.append((w.at[EARLY:], late_ref.at[:rest, at]))
        copies.append((mix.at[k * part : (k + 1) * part], late_ref.at[rest:, at]))
    started = run_copies(copies, sems)
    spread_ref[...] = jnp.broadcast_to(residual[...][None], spread_ref.shape)
    for copy in started:
        copy.wait()


def pack(residual, wq, wf, wv, wg, mix, peers):
    rows, cols = wq.shape
    late = rows - EARLY + mix.shape[0] // 4
    anywhere = pl.BlockSpec(memory_space=pl.ANY)
    vmem = pl.BlockSpec(memory_space=pltpu.VMEM)
    return pl.pallas_call(
        pack_body,
        out_shape=(
            pltpu.VMEM((EARLY, 4 * cols), wq.dtype),
            pltpu.VMEM((late, 4 * cols), wq.dtype),
            pltpu.VMEM((peers, *residual.shape), residual.dtype),
        ),
        in_specs=[vmem] + [anywhere] * 5,
        out_specs=(vmem, vmem, vmem),
        scratch_shapes=[pltpu.SemaphoreType.DMA((12,))],
        name="pack",
    )(residual, wq, wf, wv, wg, mix)


def project_body(x_ref, gain_ref, early_ref, late_ref, own_ref, send_ref):
    zo = lax.axis_index("zo")
    groups, _, height, width = x_ref.shape
    rest = late_ref.shape[2] // 2
    squares = [None] * HALVES
    for f in range(groups):
        for h in range(HALVES):
            x = x_ref[f, h].astype(jnp.float32)
            squares[h] = x * x if f == 0 else squares[h] + x * x
    scale = [
        lax.rsqrt(jnp.sum(s, axis=-1, keepdims=True) / (groups * width) + epsilon)
        for s in squares
    ]
    total = None
    for k in range(CHIPS):
        f = HALVES * k + zo
        gain = gain_ref[pl.ds(f, 1)]
        x = jnp.concatenate(
            [
                (x_ref[f, h].astype(jnp.float32) * scale[h] * gain).astype(jnp.bfloat16)
                for h in range(HALVES)
            ],
            axis=0,
        )
        w = jnp.concatenate(
            [
                piece
                for c in range(CORES)
                for piece in (early_ref[k, c], late_ref[k, c, :rest])
            ],
            axis=0,
        )
        term = jnp.dot(x, w, preferred_element_type=jnp.float32)
        total = term if total is None else total + term
    mine = jnp.where(zo == 0, total[:height], total[height:])
    other = jnp.where(zo == 0, total[height:], total[:height])
    own_ref[...] = mine
    send_ref[...] = other.astype(send_ref.dtype)


def project(x, gain, early, late):
    height = x.shape[2]
    cols = early.shape[3]
    return pl.pallas_call(
        project_body,
        out_shape=(
            pltpu.VMEM((height, cols), jnp.float32),
            pltpu.VMEM((height, cols), jnp.bfloat16),
        ),
        name="project",
    )(near(x), gain, near(early), near(late))


def recur_body(
    own_ref, part_ref, prior_ref, floor_ref, gain_ref, state_ref, out_ref, read_ref
):
    zo = lax.axis_index("zo")
    pre = own_ref[...] + part_ref[1 - zo].astype(jnp.float32)
    pre = pre.astype(jnp.bfloat16).astype(jnp.float32)
    width = prior_ref.shape[1]
    query = jax.nn.silu(pre[:, :width])
    floor = floor_ref[...]
    forget = floor + (1.0 - floor) * jax.nn.sigmoid(pre[:, width : 2 * width])
    value = pre[:, 2 * width : 3 * width]
    gate = jax.nn.sigmoid(pre[:, 3 * width :])
    forget_t = forget.T
    query_t = query.T
    for b in range(prior_ref.shape[0]):
        keep = forget_t[:, b : b + 1]
        state = keep * prior_ref[b] + (1.0 - keep) * value[b : b + 1]
        state_ref[b] = state
        read_ref[b : b + 1] = jnp.sum(query_t[:, b : b + 1] * state, axis=0, keepdims=True)
    read = read_ref[...]
    scale = lax.rsqrt(jnp.mean(read * read, axis=-1, keepdims=True) + epsilon)
    out_ref[...] = (read * scale * gain_ref[...] * gate).astype(out_ref.dtype)


def recur(own, part, prior, floor, gain):
    rows, width, _ = prior.shape
    return pl.pallas_call(
        recur_body,
        out_shape=(
            jax.ShapeDtypeStruct(prior.shape, jnp.float32),
            pltpu.VMEM((rows, width), jnp.bfloat16),
        ),
        scratch_shapes=[pltpu.VMEM((rows, width), jnp.float32)],
        name="recur",
    )(near(own), near(part), near(prior), floor, gain)


def mix_body(gated_ref, late_ref, out_ref, order_ref):
    height, width = gated_ref.shape[1:]
    rest = late_ref.shape[2] // 2
    for h in range(HALVES):
        order_ref[pl.ds(h, height, stride=HALVES)] = gated_ref[h].astype(jnp.float32)
    left = order_ref[...].astype(jnp.bfloat16)
    for k in range(CHIPS):
        right = jnp.concatenate(
            [
                late_ref[k, c, rest:, j * width : (j + 1) * width]
                for c in range(CORES)
                for j in range(4)
            ],
            axis=0,
        )
        out_ref[pl.ds(k, HALVES * height, stride=CHIPS)] = lax.dot_general(
            left, right, (((1,), (1,)), ((), ())), preferred_element_type=jnp.float32
        )


def mix_out(gated, late):
    height, width = gated.shape[1:]
    return pl.pallas_call(
        mix_body,
        out_shape=pltpu.VMEM((CHIPS * HALVES * height, width), jnp.float32),
        scratch_shapes=[pltpu.VMEM((HALVES * height, width), jnp.float32)],
        name="mix_out",
    )(near(gated), near(late))


def row_body(sums_ref, x_ref, gain_ref, out_ref, mixed_ref):
    zo = lax.axis_index("zo")
    place = lax.axis_index("y") * lax.axis_size("x") + lax.axis_index("x")
    groups, width = gain_ref.shape
    for h in range(HALVES):
        total = sums_ref[0, h]
        for k in range(1, groups):
            total = total + sums_ref[k, h]
        mixed_ref[pl.ds(h, CHIPS, stride=HALVES)] = total
    mixed = mixed_ref[...]
    scale = lax.rsqrt(jnp.sum(mixed * mixed) / gain_ref.size + epsilon)
    stream = x_ref[:, zo].astype(jnp.float32)
    at = lax.broadcasted_iota(jnp.int32, stream.shape, 1) == place
    row = jnp.sum(jnp.where(at, stream, 0.0), axis=1)
    after = (row + mixed * scale * gain_ref[...]).astype(out_ref.dtype)
    out_ref[...] = jnp.broadcast_to(after[None], out_ref.shape)


def row_update(sums, x, gain):
    groups, width = gain.shape
    return pl.pallas_call(
        row_body,
        out_shape=pltpu.VMEM((groups, groups, width), jnp.bfloat16),
        scratch_shapes=[pltpu.VMEM((groups, width), jnp.float32)],
        name="row_update",
    )(near(sums), near(x), gain)


def mlp_body(
    row_ref,
    pre_ref,
    post_ref,
    long_ref,
    out_ref,
    own_ref,
    gain_ref,
    after_ref,
    up_ref,
    down_ref,
    sems,
):
    place = lax.axis_index("y") * lax.axis_size("x") + lax.axis_index("x")
    groups, width = pre_ref.shape
    height = row_ref.shape[0]
    units = up_ref.shape[1]
    copies = run_copies(
        [(long_ref.at[:, :units], up_ref), (long_ref.at[:, units:], down_ref)], sems
    )
    for row in range(height):
        after_ref[row * groups : (row + 1) * groups] = row_ref[row].astype(jnp.float32)
    after = [after_ref[pl.ds(f, height, stride=groups)] for f in range(groups)]
    squares = after[0] * after[0]
    for f in range(1, groups):
        squares = squares + after[f] * after[f]
    scale = lax.rsqrt(
        jnp.sum(squares, axis=-1, keepdims=True) / (groups * width) + epsilon
    )
    hidden = jnp.concatenate(
        [
            (after[f] * scale * pre_ref[f : f + 1]).astype(jnp.bfloat16)
            for f in range(groups)
        ],
        axis=1,
    )
    own_ref[...] = after_ref[pl.ds(place, height, stride=groups)]
    gain_ref[...] = post_ref[pl.ds(place, 1)]
    copies[0].wait()
    up = jnp.dot(hidden, up_ref[...], preferred_element_type=jnp.float32)
    squared = jnp.square(jnp.maximum(up, 0.0)).astype(jnp.bfloat16)
    copies[1].wait()
    channel = lax.dot_general(
        squared, down_ref[...], (((1,), (1,)), ((), ())), preferred_element_type=jnp.float32
    )
    for f in range(groups):
        out_ref[f] = channel[:, f * width : (f + 1) * width].astype(out_ref.dtype)


def mlp(after, pre, post, weights, hidden):
    rows, groups, width = after.shape
    vmem = pl.BlockSpec(memory_space=pltpu.VMEM)
    return pl.pallas_call(
        mlp_body,
        out_shape=(
            pltpu.VMEM((groups, rows, width), jnp.bfloat16),
            pltpu.VMEM((rows, width), jnp.float32),
            pltpu.VMEM((1, width), jnp.float32),
        ),
        in_specs=[vmem] * 3 + [pl.BlockSpec(memory_space=pl.ANY)],
        scratch_shapes=[
            pltpu.VMEM((rows * groups, width), jnp.float32),
            pltpu.VMEM((weights.shape[0], hidden), jnp.bfloat16),
            pltpu.VMEM((weights.shape[0], hidden), jnp.bfloat16),
            pltpu.SemaphoreType.DMA((2,)),
        ],
        name="mlp",
    )(near(after), pre, post, weights)


def shards(
    residual,
    prior_state,
    w_query,
    w_forget,
    w_value,
    w_outgate,
    forget_floor,
    group_gain,
    w_mix_out,
    gain_mix_pre,
    gain_mix_post,
    gain_mlp_pre,
    gain_mlp_post,
    w_up,
    w_down,
):
    batch_rows, own_cols = residual.shape
    groups = lax.axis_size(KV)
    hidden = w_up.shape[1]

    long = lax.all_gather(pack_long(w_up, w_down.T), TP, axis=0, tiled=True)
    early, late, spread = pack(
        residual, w_query, w_forget, w_value, w_outgate, w_mix_out.T, groups * HALVES
    )
    stream = exchange(spread, (*KV, "zo")).reshape(groups, HALVES, batch_rows, own_cols)
    early = lax.all_gather(early, ("zh", "c"), axis=0).reshape(CHIPS, CORES, *early.shape)
    late = lax.all_gather(late, ("zh", "c"), axis=0).reshape(CHIPS, CORES, *late.shape)
    own, send = project(stream, gain_mix_pre.reshape(groups, own_cols), early, late)
    part = lax.all_gather(send, "zo", axis=0)
    new_state, gated = recur(
        own, part, prior_state[:, 0], forget_floor[None], group_gain[None]
    )
    gated = lax.all_gather(gated, "zo", axis=0)
    mixed_part = mix_out(gated, late).reshape(groups * HALVES, CHIPS, own_cols)
    mixed = exchange(mixed_part, (*KV, "zo")).reshape(groups, HALVES, CHIPS, own_cols)
    after_row = row_update(mixed, stream, gain_mix_post.reshape(groups, own_cols))
    channel_part, after_own, out_gain = mlp(
        exchange(after_row, KV),
        gain_mlp_pre.reshape(groups, own_cols),
        gain_mlp_post.reshape(groups, own_cols),
        long,
        hidden,
    )
    channel = jnp.sum(exchange(channel_part, KV).astype(jnp.float32), axis=0)
    layer_out = (after_own + channel * out_gain).astype(jnp.bfloat16)
    return layer_out, new_state[:, None]


def solution(mesh):
    grid = Mesh(mesh.devices.reshape(4, 4, CHIPS, HALVES, CORES), (*KV, *TP))
    return jax.shard_map(
        shards,
        mesh=grid,
        in_specs=(
            P(TP, KV),
            P(TP, KV, None, None),
            P(TP, KV),
            P(TP, KV),
            P(TP, KV),
            P(TP, KV),
            P(KV),
            P(KV),
            P(KV, TP),
            P(),
            P(),
            P(),
            P(),
            P(TP, KV),
            P(KV, TP),
        ),
        out_specs=(P(TP, KV), P(TP, KV, None, None)),
        check_vma=False,
    )
```

```python
import jax
import jax.numpy as jnp
from jax import lax
from jax.experimental import pallas as pl
from jax.experimental.pallas import tpu as pltpu
from jax.sharding import Mesh
from jax.sharding import PartitionSpec as P

KV = ("y", "x")
TP = ("zh", "zo", "c")
HALVES = 2
CHIPS = 8
CORES = 2
EARLY = 56

epsilon = 1e-06


def exchange(blocks, axes):
    return lax.all_to_all(blocks, axes, 0, 0, tiled=True)


def near(value):
    return pltpu.with_memory_space_constraint(value, pltpu.VMEM)


def run_copies(copies, sems):
    started = [
        pltpu.make_async_copy(src, dst, sems.at[k]) for k, (src, dst) in enumerate(copies)
    ]
    for copy in started:
        copy.start()
    return started


def pack_body(
    residual,
    wq,
    wf,
    wv,
    wg,
    mix,
    up,
    down,
    long_ref,
    early_ref,
    late_ref,
    spread_ref,
    stage_ref,
    sems,
):
    rows, cols = wq.shape
    rest = rows - EARLY
    part = mix.shape[0] // 4
    hidden = up.shape[1]
    copies = [(up, long_ref.at[:, :hidden]), (down, long_ref.at[:, hidden:])]
    for k, w in enumerate((wq, wf, wv, wg)):
        at = slice(k * cols, (k + 1) * cols)
        copies.append((w.at[:EARLY], early_ref.at[:, at]))
        copies.append((w.at[EARLY:], stage_ref.at[:rest, at]))
        copies.append((mix.at[k * part : (k + 1) * part], stage_ref.at[rest:, at]))
    started = run_copies(copies, sems)
    spread_ref[...] = jnp.broadcast_to(residual[...][None], spread_ref.shape)
    for copy in started:
        copy.wait()
    late_ref[...] = jnp.broadcast_to(stage_ref[...][None], late_ref.shape)


def pack(residual, wq, wf, wv, wg, mix, up, down, peers, sharers):
    rows, cols = wq.shape
    late = rows - EARLY + mix.shape[0] // 4
    anywhere = pl.BlockSpec(memory_space=pl.ANY)
    vmem = pl.BlockSpec(memory_space=pltpu.VMEM)
    return pl.pallas_call(
        pack_body,
        out_shape=(
            jax.ShapeDtypeStruct((rows, up.shape[1] + down.shape[1]), up.dtype),
            pltpu.VMEM((EARLY, 4 * cols), wq.dtype),
            pltpu.VMEM((sharers, late, 4 * cols), wq.dtype),
            pltpu.VMEM((peers, *residual.shape), residual.dtype),
        ),
        in_specs=[vmem] + [anywhere] * 7,
        out_specs=(vmem,) * 4,
        scratch_shapes=[
            pltpu.VMEM((late, 4 * cols), wq.dtype),
            pltpu.SemaphoreType.DMA((14,)),
        ],
        name="pack",
    )(residual, wq, wf, wv, wg, mix, up, down)


def project_body(x_ref, gain_ref, early_ref, late_ref, own_ref, send_ref):
    zo = lax.axis_index("zo")
    groups, _, height, width = x_ref.shape
    rest = late_ref.shape[2] - width // 8
    squares = [None] * HALVES
    for f in range(groups):
        for h in range(HALVES):
            x = x_ref[f, h].astype(jnp.float32)
            squares[h] = x * x if f == 0 else squares[h] + x * x
    scale = [
        lax.rsqrt(jnp.sum(s, axis=-1, keepdims=True) / (groups * width) + epsilon)
        for s in squares
    ]
    total = None
    for k in range(CHIPS):
        f = HALVES * k + zo
        gain = gain_ref[pl.ds(f, 1)]
        x = jnp.concatenate(
            [
                (x_ref[f, h].astype(jnp.float32) * scale[h] * gain).astype(jnp.bfloat16)
                for h in range(HALVES)
            ],
            axis=0,
        )
        w = jnp.concatenate(
            [
                piece
                for c in range(CORES)
                for piece in (early_ref[k, c], late_ref[k, c, :rest])
            ],
            axis=0,
        )
        term = jnp.dot(x, w, preferred_element_type=jnp.float32)
        total = term if total is None else total + term
    mine = jnp.where(zo == 0, total[:height], total[height:])
    other = jnp.where(zo == 0, total[height:], total[:height])
    own_ref[...] = mine
    send_ref[...] = other.astype(send_ref.dtype)


def project(x, gain, early, late):
    height = x.shape[2]
    cols = early.shape[3]
    return pl.pallas_call(
        project_body,
        out_shape=(
            pltpu.VMEM((height, cols), jnp.float32),
            pltpu.VMEM((height, cols), jnp.bfloat16),
        ),
        name="project",
    )(near(x), gain, near(early), near(late))


def recur_body(
    own_ref, part_ref, prior_ref, floor_ref, gain_ref, state_ref, out_ref, read_ref
):
    zo = lax.axis_index("zo")
    pre = own_ref[...] + part_ref[1 - zo].astype(jnp.float32)
    pre = pre.astype(jnp.bfloat16).astype(jnp.float32)
    width = prior_ref.shape[1]
    query = jax.nn.silu(pre[:, :width])
    floor = floor_ref[...]
    forget = floor + (1.0 - floor) * jax.nn.sigmoid(pre[:, width : 2 * width])
    value = pre[:, 2 * width : 3 * width]
    gate = jax.nn.sigmoid(pre[:, 3 * width :])
    forget_t = forget.T
    query_t = query.T
    for b in range(prior_ref.shape[0]):
        keep = forget_t[:, b : b + 1]
        state = keep * prior_ref[b] + (1.0 - keep) * value[b : b + 1]
        state_ref[b] = state
        read_ref[b : b + 1] = jnp.sum(query_t[:, b : b + 1] * state, axis=0, keepdims=True)
    read = read_ref[...]
    scale = lax.rsqrt(jnp.mean(read * read, axis=-1, keepdims=True) + epsilon)
    out_ref[...] = (read * scale * gain_ref[...] * gate).astype(out_ref.dtype)


def recur(own, part, prior, floor, gain):
    rows, width, _ = prior.shape
    return pl.pallas_call(
        recur_body,
        out_shape=(
            jax.ShapeDtypeStruct(prior.shape, jnp.float32),
            pltpu.VMEM((rows, width), jnp.bfloat16),
        ),
        scratch_shapes=[pltpu.VMEM((rows, width), jnp.float32)],
        name="recur",
    )(near(own), near(part), near(prior), floor, gain)


def mix_body(gated_ref, late_ref, out_ref, order_ref):
    height, width = gated_ref.shape[1:]
    rest = late_ref.shape[2] - width // 8
    for h in range(HALVES):
        order_ref[pl.ds(h, height, stride=HALVES)] = gated_ref[h].astype(jnp.float32)
    left = order_ref[...].astype(jnp.bfloat16)
    for k in range(CHIPS):
        right = jnp.concatenate(
            [
                late_ref[k, c, rest:, j * width : (j + 1) * width]
                for c in range(CORES)
                for j in range(4)
            ],
            axis=0,
        )
        out_ref[pl.ds(k, HALVES * height, stride=CHIPS)] = lax.dot_general(
            left, right, (((1,), (1,)), ((), ())), preferred_element_type=jnp.float32
        )


def mix_out(gated, late):
    height, width = gated.shape[1:]
    return pl.pallas_call(
        mix_body,
        out_shape=pltpu.VMEM((CHIPS * HALVES * height, width), jnp.float32),
        scratch_shapes=[pltpu.VMEM((HALVES * height, width), jnp.float32)],
        name="mix_out",
    )(near(gated), near(late))


def row_body(sums_ref, x_ref, gain_ref, out_ref, mixed_ref):
    zo = lax.axis_index("zo")
    place = lax.axis_index("y") * lax.axis_size("x") + lax.axis_index("x")
    groups, width = gain_ref.shape
    for h in range(HALVES):
        total = sums_ref[0, h]
        for k in range(1, groups):
            total = total + sums_ref[k, h]
        mixed_ref[pl.ds(h, CHIPS, stride=HALVES)] = total
    mixed = mixed_ref[...]
    scale = lax.rsqrt(jnp.sum(mixed * mixed) / gain_ref.size + epsilon)
    stream = x_ref[:, zo].astype(jnp.float32)
    at = lax.broadcasted_iota(jnp.int32, stream.shape, 1) == place
    row = jnp.sum(jnp.where(at, stream, 0.0), axis=1)
    after = (row + mixed * scale * gain_ref[...]).astype(out_ref.dtype)
    out_ref[...] = jnp.broadcast_to(after[None], out_ref.shape)


def row_update(sums, x, gain):
    groups, width = gain.shape
    return pl.pallas_call(
        row_body,
        out_shape=pltpu.VMEM((groups, groups, width), jnp.bfloat16),
        scratch_shapes=[pltpu.VMEM((groups, width), jnp.float32)],
        name="row_update",
    )(near(sums), near(x), gain)


def mlp_body(
    row_ref,
    pre_ref,
    post_ref,
    long_ref,
    out_ref,
    own_ref,
    gain_ref,
    after_ref,
    up_ref,
    down_ref,
    sems,
):
    place = lax.axis_index("y") * lax.axis_size("x") + lax.axis_index("x")
    groups, width = pre_ref.shape
    height = row_ref.shape[0]
    units = up_ref.shape[1]
    copies = run_copies(
        [(long_ref.at[:, :units], up_ref), (long_ref.at[:, units:], down_ref)], sems
    )
    for row in range(height):
        after_ref[row * groups : (row + 1) * groups] = row_ref[row].astype(jnp.float32)
    after = [after_ref[pl.ds(f, height, stride=groups)] for f in range(groups)]
    squares = after[0] * after[0]
    for f in range(1, groups):
        squares = squares + after[f] * after[f]
    scale = lax.rsqrt(
        jnp.sum(squares, axis=-1, keepdims=True) / (groups * width) + epsilon
    )
    hidden = jnp.concatenate(
        [
            (after[f] * scale * pre_ref[f : f + 1]).astype(jnp.bfloat16)
            for f in range(groups)
        ],
        axis=1,
    )
    own_ref[...] = after_ref[pl.ds(place, height, stride=groups)]
    gain_ref[...] = post_ref[pl.ds(place, 1)]
    copies[0].wait()
    up = jnp.dot(hidden, up_ref[...], preferred_element_type=jnp.float32)
    squared = jnp.square(jnp.maximum(up, 0.0)).astype(jnp.bfloat16)
    copies[1].wait()
    channel = lax.dot_general(
        squared, down_ref[...], (((1,), (1,)), ((), ())), preferred_element_type=jnp.float32
    )
    for f in range(groups):
        out_ref[f] = channel[:, f * width : (f + 1) * width].astype(out_ref.dtype)


def mlp(after, pre, post, weights, hidden):
    rows, groups, width = after.shape
    vmem = pl.BlockSpec(memory_space=pltpu.VMEM)
    return pl.pallas_call(
        mlp_body,
        out_shape=(
            pltpu.VMEM((groups, rows, width), jnp.bfloat16),
            pltpu.VMEM((rows, width), jnp.float32),
            pltpu.VMEM((1, width), jnp.float32),
        ),
        in_specs=[vmem] * 3 + [pl.BlockSpec(memory_space=pl.ANY)],
        scratch_shapes=[
            pltpu.VMEM((rows * groups, width), jnp.float32),
            pltpu.VMEM((weights.shape[0], hidden), jnp.bfloat16),
            pltpu.VMEM((weights.shape[0], hidden), jnp.bfloat16),
            pltpu.SemaphoreType.DMA((2,)),
        ],
        name="mlp",
    )(near(after), pre, post, weights)


def shards(
    residual,
    prior_state,
    w_query,
    w_forget,
    w_value,
    w_outgate,
    forget_floor,
    group_gain,
    w_mix_out,
    gain_mix_pre,
    gain_mix_post,
    gain_mlp_pre,
    gain_mlp_post,
    w_up,
    w_down,
):
    batch_rows, own_cols = residual.shape
    groups = lax.axis_size(KV)
    hidden = w_up.shape[1]

    long, early, late, spread = pack(
        residual,
        w_query,
        w_forget,
        w_value,
        w_outgate,
        w_mix_out.T,
        w_up,
        w_down.T,
        groups * HALVES,
        CHIPS * CORES,
    )
    long = lax.all_gather(long, TP, axis=0, tiled=True)
    stream = exchange(spread, (*KV, "zo")).reshape(groups, HALVES, batch_rows, own_cols)
    late = exchange(late, ("zh", "c")).reshape(CHIPS, CORES, *late.shape[1:])
    early = lax.all_gather(early, ("zh", "c"), axis=0).reshape(CHIPS, CORES, *early.shape)
    own, send = project(stream, gain_mix_pre.reshape(groups, own_cols), early, late)
    part = lax.all_gather(send, "zo", axis=0)
    new_state, gated = recur(
        own, part, prior_state[:, 0], forget_floor[None], group_gain[None]
    )
    gated = lax.all_gather(gated, "zo", axis=0)
    mixed_part = mix_out(gated, late).reshape(groups * HALVES, CHIPS, own_cols)
    mixed = exchange(mixed_part, (*KV, "zo")).reshape(groups, HALVES, CHIPS, own_cols)
    after_row = row_update(mixed, stream, gain_mix_post.reshape(groups, own_cols))
    channel_part, after_own, out_gain = mlp(
        exchange(after_row, KV),
        gain_mlp_pre.reshape(groups, own_cols),
        gain_mlp_post.reshape(groups, own_cols),
        long,
        hidden,
    )
    channel = jnp.sum(exchange(channel_part, KV).astype(jnp.float32), axis=0)
    layer_out = (after_own + channel * out_gain).astype(jnp.bfloat16)
    return layer_out, new_state[:, None]


def solution(mesh):
    grid = Mesh(mesh.devices.reshape(4, 4, CHIPS, HALVES, CORES), (*KV, *TP))
    return jax.shard_map(
        shards,
        mesh=grid,
        in_specs=(
            P(TP, KV),
            P(TP, KV, None, None),
            P(TP, KV),
            P(TP, KV),
            P(TP, KV),
            P(TP, KV),
            P(KV),
            P(KV),
            P(KV, TP),
            P(),
            P(),
            P(),
            P(),
            P(TP, KV),
            P(KV, TP),
        ),
        out_specs=(P(TP, KV), P(TP, KV, None, None)),
        check_vma=False,
    )
```

```python
import jax
import jax.numpy as jnp
from jax import lax
from jax.experimental import pallas as pl
from jax.experimental.pallas import tpu as pltpu
from jax.sharding import Mesh
from jax.sharding import PartitionSpec as P

KV = ("y", "x")
TP = ("za", "zb", "c")
PARTS = 4
CHIPS = 4
CORES = 2

epsilon = 1e-06


def exchange(blocks, axes):
    return lax.all_to_all(blocks, axes, 0, 0, tiled=True)


def near(value):
    return pltpu.with_memory_space_constraint(value, pltpu.VMEM)


def run_copies(copies, sems):
    started = [
        pltpu.make_async_copy(src, dst, sems.at[k]) for k, (src, dst) in enumerate(copies)
    ]
    for copy in started:
        copy.start()
    return started


def pack_body(
    residual, wq, wf, wv, wg, mix, up, down, long_ref, short_ref, spread_ref, sems
):
    rows, cols = wq.shape
    part = mix.shape[0] // 4
    hidden = up.shape[1]
    copies = [(up, long_ref.at[:, :hidden]), (down, long_ref.at[:, hidden:])]
    for k, w in enumerate((wq, wf, wv, wg)):
        at = slice(k * cols, (k + 1) * cols)
        copies.append((w, short_ref.at[:rows, at]))
        copies.append((mix.at[k * part : (k + 1) * part], short_ref.at[rows:, at]))
    started = run_copies(copies, sems)
    spread_ref[...] = jnp.broadcast_to(residual[...][None], spread_ref.shape)
    for copy in started:
        copy.wait()


def pack(residual, wq, wf, wv, wg, mix, up, down, peers):
    rows, cols = wq.shape
    anywhere = pl.BlockSpec(memory_space=pl.ANY)
    vmem = pl.BlockSpec(memory_space=pltpu.VMEM)
    return pl.pallas_call(
        pack_body,
        out_shape=(
            jax.ShapeDtypeStruct((rows, up.shape[1] + down.shape[1]), up.dtype),
            pltpu.VMEM((rows + mix.shape[0] // 4, 4 * cols), wq.dtype),
            pltpu.VMEM((peers, *residual.shape), residual.dtype),
        ),
        in_specs=[vmem] + [anywhere] * 7,
        out_specs=(vmem,) * 3,
        scratch_shapes=[pltpu.SemaphoreType.DMA((10,))],
        name="pack",
    )(residual, wq, wf, wv, wg, mix, up, down)


def project_body(x_ref, gain_ref, short_ref, out_ref):
    zb = lax.axis_index("zb")
    groups, _, height, width = x_ref.shape
    rows = width // CORES
    squares = [None] * PARTS
    for f in range(groups):
        for h in range(PARTS):
            x = x_ref[f, h].astype(jnp.float32)
            squares[h] = x * x if f == 0 else squares[h] + x * x
    scale = [
        lax.rsqrt(jnp.sum(s, axis=-1, keepdims=True) / (groups * width) + epsilon)
        for s in squares
    ]
    total = None
    for k in range(CHIPS):
        f = PARTS * k + zb
        gain = gain_ref[pl.ds(f, 1)]
        x = jnp.concatenate(
            [
                (x_ref[f, h].astype(jnp.float32) * scale[h] * gain).astype(jnp.bfloat16)
                for h in range(PARTS)
            ],
            axis=0,
        )
        w = jnp.concatenate([short_ref[k, c, :rows] for c in range(CORES)], axis=0)
        term = jnp.dot(x, w, preferred_element_type=jnp.float32)
        total = term if total is None else total + term
    for h in range(PARTS):
        out_ref[h] = total[h * height : (h + 1) * height].astype(out_ref.dtype)


def project(x, gain, short):
    return pl.pallas_call(
        project_body,
        out_shape=pltpu.VMEM((PARTS, x.shape[2], short.shape[3]), jnp.bfloat16),
        name="project",
    )(near(x), gain, near(short))


def recur_body(part_ref, prior_ref, floor_ref, gain_ref, state_ref, out_ref, read_ref):
    pre = part_ref[0].astype(jnp.float32)
    for k in range(1, PARTS):
        pre = pre + part_ref[k].astype(jnp.float32)
    pre = pre.astype(jnp.bfloat16).astype(jnp.float32)
    width = prior_ref.shape[1]
    query = jax.nn.silu(pre[:, :width])
    floor = floor_ref[...]
    forget = floor + (1.0 - floor) * jax.nn.sigmoid(pre[:, width : 2 * width])
    value = pre[:, 2 * width : 3 * width]
    gate = jax.nn.sigmoid(pre[:, 3 * width :])
    forget_t = forget.T
    query_t = query.T
    for b in range(prior_ref.shape[0]):
        keep = forget_t[:, b : b + 1]
        state = keep * prior_ref[b] + (1.0 - keep) * value[b : b + 1]
        state_ref[b] = state
        read_ref[b : b + 1] = jnp.sum(query_t[:, b : b + 1] * state, axis=0, keepdims=True)
    read = read_ref[...]
    scale = lax.rsqrt(jnp.mean(read * read, axis=-1, keepdims=True) + epsilon)
    gated = (read * scale * gain_ref[...] * gate).astype(out_ref.dtype)
    out_ref[...] = jnp.broadcast_to(gated[None], out_ref.shape)


def recur(part, prior, floor, gain):
    rows, width, _ = prior.shape
    return pl.pallas_call(
        recur_body,
        out_shape=(
            jax.ShapeDtypeStruct(prior.shape, jnp.float32),
            pltpu.VMEM((PARTS, rows, width), jnp.bfloat16),
        ),
        scratch_shapes=[pltpu.VMEM((rows, width), jnp.float32)],
        name="recur",
    )(near(part), near(prior), floor, gain)


def mix_body(gated_ref, short_ref, out_ref, order_ref):
    height, width = gated_ref.shape[1:]
    rows = width // CORES
    for h in range(PARTS):
        order_ref[pl.ds(h, height, stride=PARTS)] = gated_ref[h].astype(jnp.float32)
    left = order_ref[...].astype(jnp.bfloat16)
    for k in range(CHIPS):
        right = jnp.concatenate(
            [
                short_ref[k, c, rows:, j * width : (j + 1) * width]
                for c in range(CORES)
                for j in range(4)
            ],
            axis=0,
        )
        out_ref[pl.ds(k, PARTS * height, stride=CHIPS)] = lax.dot_general(
            left, right, (((1,), (1,)), ((), ())), preferred_element_type=jnp.float32
        )


def mix_out(gated, short):
    height, width = gated.shape[1:]
    return pl.pallas_call(
        mix_body,
        out_shape=pltpu.VMEM((CHIPS * PARTS * height, width), jnp.float32),
        scratch_shapes=[pltpu.VMEM((PARTS * height, width), jnp.float32)],
        name="mix_out",
    )(near(gated), near(short))


def row_body(sums_ref, x_ref, gain_ref, out_ref, mixed_ref):
    zb = lax.axis_index("zb")
    place = lax.axis_index("y") * lax.axis_size("x") + lax.axis_index("x")
    groups, width = gain_ref.shape
    total = sums_ref[:groups]
    for k in range(1, groups):
        total = total + sums_ref[k * groups : (k + 1) * groups]
    for h in range(PARTS):
        mixed_ref[pl.ds(h, CHIPS, stride=PARTS)] = total[h * CHIPS : (h + 1) * CHIPS]
    mixed = mixed_ref[...]
    scale = lax.rsqrt(jnp.sum(mixed * mixed) / gain_ref.size + epsilon)
    stream = x_ref[:, zb].astype(jnp.float32)
    at = lax.broadcasted_iota(jnp.int32, stream.shape, 1) == place
    row = jnp.sum(jnp.where(at, stream, 0.0), axis=1)
    after = (row + mixed * scale * gain_ref[...]).astype(out_ref.dtype)
    out_ref[...] = jnp.broadcast_to(after[None], out_ref.shape)


def row_update(sums, x, gain):
    groups, width = gain.shape
    return pl.pallas_call(
        row_body,
        out_shape=pltpu.VMEM((groups, groups, width), jnp.bfloat16),
        scratch_shapes=[pltpu.VMEM((groups, width), jnp.float32)],
        name="row_update",
    )(near(sums), near(x), gain)


def mlp_body(
    row_ref,
    pre_ref,
    post_ref,
    long_ref,
    out_ref,
    own_ref,
    gain_ref,
    after_ref,
    up_ref,
    down_ref,
    sems,
):
    place = lax.axis_index("y") * lax.axis_size("x") + lax.axis_index("x")
    groups, width = pre_ref.shape
    height = row_ref.shape[0]
    units = up_ref.shape[1]
    copies = run_copies(
        [(long_ref.at[:, :units], up_ref), (long_ref.at[:, units:], down_ref)], sems
    )
    for row in range(height):
        after_ref[row * groups : (row + 1) * groups] = row_ref[row].astype(jnp.float32)
    after = [after_ref[pl.ds(f, height, stride=groups)] for f in range(groups)]
    squares = after[0] * after[0]
    for f in range(1, groups):
        squares = squares + after[f] * after[f]
    scale = lax.rsqrt(
        jnp.sum(squares, axis=-1, keepdims=True) / (groups * width) + epsilon
    )
    hidden = jnp.concatenate(
        [
            (after[f] * scale * pre_ref[f : f + 1]).astype(jnp.bfloat16)
            for f in range(groups)
        ],
        axis=1,
    )
    own_ref[...] = after_ref[pl.ds(place, height, stride=groups)]
    gain_ref[...] = post_ref[pl.ds(place, 1)]
    copies[0].wait()
    up = jnp.dot(hidden, up_ref[...], preferred_element_type=jnp.float32)
    squared = jnp.square(jnp.maximum(up, 0.0)).astype(jnp.bfloat16)
    copies[1].wait()
    channel = lax.dot_general(
        squared, down_ref[...], (((1,), (1,)), ((), ())), preferred_element_type=jnp.float32
    )
    for f in range(groups):
        out_ref[f] = channel[:, f * width : (f + 1) * width].astype(out_ref.dtype)


def mlp(after, pre, post, weights, hidden):
    rows, groups, width = after.shape
    vmem = pl.BlockSpec(memory_space=pltpu.VMEM)
    return pl.pallas_call(
        mlp_body,
        out_shape=(
            pltpu.VMEM((groups, rows, width), jnp.bfloat16),
            pltpu.VMEM((rows, width), jnp.float32),
            pltpu.VMEM((1, width), jnp.float32),
        ),
        in_specs=[vmem] * 3 + [pl.BlockSpec(memory_space=pl.ANY)],
        scratch_shapes=[
            pltpu.VMEM((rows * groups, width), jnp.float32),
            pltpu.VMEM((weights.shape[0], hidden), jnp.bfloat16),
            pltpu.VMEM((weights.shape[0], hidden), jnp.bfloat16),
            pltpu.SemaphoreType.DMA((2,)),
        ],
        name="mlp",
    )(near(after), pre, post, weights)


def shards(
    residual,
    prior_state,
    w_query,
    w_forget,
    w_value,
    w_outgate,
    forget_floor,
    group_gain,
    w_mix_out,
    gain_mix_pre,
    gain_mix_post,
    gain_mlp_pre,
    gain_mlp_post,
    w_up,
    w_down,
):
    batch_rows, own_cols = residual.shape
    groups = lax.axis_size(KV)
    hidden = w_up.shape[1]

    long, short, spread = pack(
        residual,
        w_query,
        w_forget,
        w_value,
        w_outgate,
        w_mix_out.T,
        w_up,
        w_down.T,
        groups * PARTS,
    )
    long = lax.all_gather(long, TP, axis=0, tiled=True)
    stream = exchange(spread, (*KV, "zb")).reshape(groups, PARTS, batch_rows, own_cols)
    short = lax.all_gather(short, ("za", "c"), axis=0).reshape(CHIPS, CORES, *short.shape)
    part = exchange(project(stream, gain_mix_pre.reshape(groups, own_cols), short), "zb")
    new_state, gated = recur(
        part, prior_state[:, 0], forget_floor[None], group_gain[None]
    )
    mixed_part = mix_out(exchange(gated, "zb"), short)
    mixed = exchange(mixed_part.reshape(groups * PARTS, CHIPS, own_cols), (*KV, "zb"))
    after_row = row_update(
        mixed.reshape(-1, own_cols), stream, gain_mix_post.reshape(groups, own_cols)
    )
    channel_part, after_own, out_gain = mlp(
        exchange(after_row, KV),
        gain_mlp_pre.reshape(groups, own_cols),
        gain_mlp_post.reshape(groups, own_cols),
        long,
        hidden,
    )
    channel = jnp.sum(exchange(channel_part, KV).astype(jnp.float32), axis=0)
    layer_out = (after_own + channel * out_gain).astype(jnp.bfloat16)
    return layer_out, new_state[:, None]


def solution(mesh):
    grid = Mesh(mesh.devices.reshape(4, 4, CHIPS, PARTS, CORES), (*KV, *TP))
    return jax.shard_map(
        shards,
        mesh=grid,
        in_specs=(
            P(TP, KV),
            P(TP, KV, None, None),
            P(TP, KV),
            P(TP, KV),
            P(TP, KV),
            P(TP, KV),
            P(KV),
            P(KV),
            P(KV, TP),
            P(),
            P(),
            P(),
            P(),
            P(TP, KV),
            P(KV, TP),
        ),
        out_specs=(P(TP, KV), P(TP, KV, None, None)),
        check_vma=False,
    )
```

```python
import jax
import jax.numpy as jnp
from jax import lax
from jax.experimental import pallas as pl
from jax.experimental.pallas import tpu as pltpu
from jax.sharding import Mesh
from jax.sharding import PartitionSpec as P

KV = ("y", "x")
TP = ("za", "zb", "c")
PARTS = 4
CHIPS = 4
CORES = 2
SLAB = 4
PIECES = 4

epsilon = 1e-06


def exchange(blocks, axes):
    return lax.all_to_all(blocks, axes, 0, 0, tiled=True)


def near(value):
    return pltpu.with_memory_space_constraint(value, pltpu.VMEM)


def run_copies(copies, sems):
    started = [
        pltpu.make_async_copy(src, dst, sems.at[k]) for k, (src, dst) in enumerate(copies)
    ]
    for copy in started:
        copy.start()
    return started


def pack_body(
    residual, wq, wf, wv, wg, mix, up, down, long_ref, short_ref, spread_ref, sems
):
    rows, cols = wq.shape
    part = mix.shape[0] // 4
    hidden = up.shape[1]
    copies = [(up, long_ref.at[:, :hidden]), (down, long_ref.at[:, hidden:])]
    for k, w in enumerate((wq, wf, wv, wg)):
        at = slice(k * cols, (k + 1) * cols)
        copies.append((w, short_ref.at[:rows, at]))
        copies.append((mix.at[k * part : (k + 1) * part], short_ref.at[rows:, at]))
    started = run_copies(copies, sems)
    spread_ref[...] = jnp.broadcast_to(residual[...][None], spread_ref.shape)
    for copy in started:
        copy.wait()


def pack(residual, wq, wf, wv, wg, mix, up, down, peers):
    rows, cols = wq.shape
    anywhere = pl.BlockSpec(memory_space=pl.ANY)
    vmem = pl.BlockSpec(memory_space=pltpu.VMEM)
    return pl.pallas_call(
        pack_body,
        out_shape=(
            jax.ShapeDtypeStruct((rows, up.shape[1] + down.shape[1]), up.dtype),
            pltpu.VMEM((rows + mix.shape[0] // 4, 4 * cols), wq.dtype),
            pltpu.VMEM((peers, *residual.shape), residual.dtype),
        ),
        in_specs=[vmem] + [anywhere] * 7,
        out_specs=(vmem,) * 3,
        scratch_shapes=[pltpu.SemaphoreType.DMA((10,))],
        name="pack",
    )(residual, wq, wf, wv, wg, mix, up, down)


def project_body(x_ref, gain_ref, short_ref, out_ref):
    zb = lax.axis_index("zb")
    groups, _, height, width = x_ref.shape
    rows = width // CORES
    squares = [None] * PARTS
    for f in range(groups):
        for h in range(PARTS):
            x = x_ref[f, h].astype(jnp.float32)
            squares[h] = x * x if f == 0 else squares[h] + x * x
    scale = [
        lax.rsqrt(jnp.sum(s, axis=-1, keepdims=True) / (groups * width) + epsilon)
        for s in squares
    ]
    total = None
    for k in range(CHIPS):
        f = PARTS * k + zb
        gain = gain_ref[pl.ds(f, 1)]
        x = jnp.concatenate(
            [
                (x_ref[f, h].astype(jnp.float32) * scale[h] * gain).astype(jnp.bfloat16)
                for h in range(PARTS)
            ],
            axis=0,
        )
        w = jnp.concatenate([short_ref[k, c, :rows] for c in range(CORES)], axis=0)
        term = jnp.dot(x, w, preferred_element_type=jnp.float32)
        total = term if total is None else total + term
    for h in range(PARTS):
        out_ref[h] = total[h * height : (h + 1) * height].astype(out_ref.dtype)


def project(x, gain, short):
    return pl.pallas_call(
        project_body,
        out_shape=pltpu.VMEM((PARTS, x.shape[2], short.shape[3]), jnp.bfloat16),
        name="project",
    )(near(x), gain, near(short))


def recur_body(
    part_ref,
    prior,
    floor_ref,
    gain_ref,
    state,
    out_ref,
    prior_ref,
    state_ref,
    read_ref,
    in_sems,
    out_sems,
):
    rows = prior_ref.shape[0]
    chunks = [slice(k, k + SLAB) for k in range(0, rows, SLAB)]
    fetches = run_copies([(prior.at[c], prior_ref.at[c]) for c in chunks], in_sems)
    stores = [
        pltpu.make_async_copy(state_ref.at[c], state.at[c], out_sems.at[k])
        for k, c in enumerate(chunks)
    ]
    pre = part_ref[0].astype(jnp.float32)
    for k in range(1, PARTS):
        pre = pre + part_ref[k].astype(jnp.float32)
    pre = pre.astype(jnp.bfloat16).astype(jnp.float32)
    width = prior_ref.shape[1]
    query = jax.nn.silu(pre[:, :width])
    floor = floor_ref[...]
    forget = floor + (1.0 - floor) * jax.nn.sigmoid(pre[:, width : 2 * width])
    value = pre[:, 2 * width : 3 * width]
    gate = jax.nn.sigmoid(pre[:, 3 * width :])
    forget_t = forget.T
    query_t = query.T
    for b in range(rows):
        if b % SLAB == 0:
            fetches[b // SLAB].wait()
        keep = forget_t[:, b : b + 1]
        fresh = keep * prior_ref[b] + (1.0 - keep) * value[b : b + 1]
        state_ref[b] = fresh
        read_ref[b : b + 1] = jnp.sum(query_t[:, b : b + 1] * fresh, axis=0, keepdims=True)
        if b % SLAB == SLAB - 1:
            stores[b // SLAB].start()
    read = read_ref[...]
    scale = lax.rsqrt(jnp.mean(read * read, axis=-1, keepdims=True) + epsilon)
    gated = (read * scale * gain_ref[...] * gate).astype(out_ref.dtype)
    out_ref[...] = jnp.broadcast_to(gated[None], out_ref.shape)
    for store in stores:
        store.wait()


def recur(part, prior, floor, gain):
    rows, width, _ = prior.shape
    anywhere = pl.BlockSpec(memory_space=pl.ANY)
    vmem = pl.BlockSpec(memory_space=pltpu.VMEM)
    return pl.pallas_call(
        recur_body,
        out_shape=(
            jax.ShapeDtypeStruct(prior.shape, jnp.float32),
            pltpu.VMEM((PARTS, rows, width), jnp.bfloat16),
        ),
        in_specs=[vmem, anywhere, vmem, vmem],
        out_specs=(anywhere, vmem),
        scratch_shapes=[
            pltpu.VMEM(prior.shape, jnp.float32),
            pltpu.VMEM(prior.shape, jnp.float32),
            pltpu.VMEM((rows, width), jnp.float32),
            pltpu.SemaphoreType.DMA((rows // SLAB,)),
            pltpu.SemaphoreType.DMA((rows // SLAB,)),
        ],
        name="recur",
    )(near(part), prior, floor, gain)


def mix_body(gated_ref, short_ref, out_ref, order_ref):
    height, width = gated_ref.shape[1:]
    rows = width // CORES
    for h in range(PARTS):
        order_ref[pl.ds(h, height, stride=PARTS)] = gated_ref[h].astype(jnp.float32)
    left = order_ref[...].astype(jnp.bfloat16)
    for k in range(CHIPS):
        right = jnp.concatenate(
            [
                short_ref[k, c, rows:, j * width : (j + 1) * width]
                for c in range(CORES)
                for j in range(4)
            ],
            axis=0,
        )
        out_ref[pl.ds(k, PARTS * height, stride=CHIPS)] = lax.dot_general(
            left, right, (((1,), (1,)), ((), ())), preferred_element_type=jnp.float32
        )


def mix_out(gated, short):
    height, width = gated.shape[1:]
    return pl.pallas_call(
        mix_body,
        out_shape=pltpu.VMEM((CHIPS * PARTS * height, width), jnp.float32),
        scratch_shapes=[pltpu.VMEM((PARTS * height, width), jnp.float32)],
        name="mix_out",
    )(near(gated), near(short))


def row_body(sums_ref, x_ref, gain_ref, out_ref, mixed_ref):
    zb = lax.axis_index("zb")
    place = lax.axis_index("y") * lax.axis_size("x") + lax.axis_index("x")
    groups, width = gain_ref.shape
    total = sums_ref[:groups]
    for k in range(1, groups):
        total = total + sums_ref[k * groups : (k + 1) * groups]
    for h in range(PARTS):
        mixed_ref[pl.ds(h, CHIPS, stride=PARTS)] = total[h * CHIPS : (h + 1) * CHIPS]
    mixed = mixed_ref[...]
    scale = lax.rsqrt(jnp.sum(mixed * mixed) / gain_ref.size + epsilon)
    stream = x_ref[:, zb].astype(jnp.float32)
    at = lax.broadcasted_iota(jnp.int32, stream.shape, 1) == place
    row = jnp.sum(jnp.where(at, stream, 0.0), axis=1)
    after = (row + mixed * scale * gain_ref[...]).astype(out_ref.dtype)
    out_ref[...] = jnp.broadcast_to(after[None], out_ref.shape)


def row_update(sums, x, gain):
    groups, width = gain.shape
    return pl.pallas_call(
        row_body,
        out_shape=pltpu.VMEM((groups, groups, width), jnp.bfloat16),
        scratch_shapes=[pltpu.VMEM((groups, width), jnp.float32)],
        name="row_update",
    )(near(sums), near(x), gain)


def mlp_body(
    row_ref,
    pre_ref,
    post_ref,
    long_ref,
    out_ref,
    own_ref,
    gain_ref,
    after_ref,
    up_ref,
    down_ref,
    sems,
):
    place = lax.axis_index("y") * lax.axis_size("x") + lax.axis_index("x")
    groups, width = pre_ref.shape
    height = row_ref.shape[0]
    units = up_ref.shape[1]
    full = groups * width
    pieces = [slice(k, k + full // PIECES) for k in range(0, full, full // PIECES)]
    copies = run_copies(
        [(long_ref.at[p, :units], up_ref.at[p]) for p in pieces]
        + [(long_ref.at[p, units:], down_ref.at[p]) for p in pieces],
        sems,
    )
    for row in range(height):
        after_ref[row * groups : (row + 1) * groups] = row_ref[row].astype(jnp.float32)
    after = [after_ref[pl.ds(f, height, stride=groups)] for f in range(groups)]
    squares = after[0] * after[0]
    for f in range(1, groups):
        squares = squares + after[f] * after[f]
    scale = lax.rsqrt(
        jnp.sum(squares, axis=-1, keepdims=True) / full + epsilon
    )
    hidden = jnp.concatenate(
        [
            (after[f] * scale * pre_ref[f : f + 1]).astype(jnp.bfloat16)
            for f in range(groups)
        ],
        axis=1,
    )
    own_ref[...] = after_ref[pl.ds(place, height, stride=groups)]
    gain_ref[...] = post_ref[pl.ds(place, 1)]
    up = None
    for k, p in enumerate(pieces):
        copies[k].wait()
        term = jnp.dot(hidden[:, p], up_ref[p], preferred_element_type=jnp.float32)
        up = term if up is None else up + term
    squared = jnp.square(jnp.maximum(up, 0.0)).astype(jnp.bfloat16)
    for k, p in enumerate(pieces):
        copies[PIECES + k].wait()
        channel = lax.dot_general(
            squared, down_ref[p], (((1,), (1,)), ((), ())), preferred_element_type=jnp.float32
        )
        for f in range(groups // PIECES):
            out_ref[k * (groups // PIECES) + f] = channel[
                :, f * width : (f + 1) * width
            ].astype(out_ref.dtype)


def mlp(after, pre, post, weights, hidden):
    rows, groups, width = after.shape
    vmem = pl.BlockSpec(memory_space=pltpu.VMEM)
    return pl.pallas_call(
        mlp_body,
        out_shape=(
            pltpu.VMEM((groups, rows, width), jnp.bfloat16),
            pltpu.VMEM((rows, width), jnp.float32),
            pltpu.VMEM((1, width), jnp.float32),
        ),
        in_specs=[vmem] * 3 + [pl.BlockSpec(memory_space=pl.ANY)],
        scratch_shapes=[
            pltpu.VMEM((rows * groups, width), jnp.float32),
            pltpu.VMEM((weights.shape[0], hidden), jnp.bfloat16),
            pltpu.VMEM((weights.shape[0], hidden), jnp.bfloat16),
            pltpu.SemaphoreType.DMA((2 * PIECES,)),
        ],
        name="mlp",
    )(near(after), pre, post, weights)


def shards(
    residual,
    prior_state,
    w_query,
    w_forget,
    w_value,
    w_outgate,
    forget_floor,
    group_gain,
    w_mix_out,
    gain_mix_pre,
    gain_mix_post,
    gain_mlp_pre,
    gain_mlp_post,
    w_up,
    w_down,
):
    batch_rows, own_cols = residual.shape
    groups = lax.axis_size(KV)
    hidden = w_up.shape[1]

    long, short, spread = pack(
        residual,
        w_query,
        w_forget,
        w_value,
        w_outgate,
        w_mix_out.T,
        w_up,
        w_down.T,
        groups * PARTS,
    )
    long = lax.all_gather(long, TP, axis=0, tiled=True)
    stream = exchange(spread, (*KV, "zb")).reshape(groups, PARTS, batch_rows, own_cols)
    short = lax.all_gather(short, ("za", "c"), axis=0).reshape(CHIPS, CORES, *short.shape)
    part = exchange(project(stream, gain_mix_pre.reshape(groups, own_cols), short), "zb")
    new_state, gated = recur(
        part, prior_state[:, 0], forget_floor[None], group_gain[None]
    )
    mixed_part = mix_out(exchange(gated, "zb"), short)
    mixed = exchange(mixed_part.reshape(groups * PARTS, CHIPS, own_cols), (*KV, "zb"))
    after_row = row_update(
        mixed.reshape(-1, own_cols), stream, gain_mix_post.reshape(groups, own_cols)
    )
    channel_part, after_own, out_gain = mlp(
        exchange(after_row, KV),
        gain_mlp_pre.reshape(groups, own_cols),
        gain_mlp_post.reshape(groups, own_cols),
        long,
        hidden,
    )
    channel = jnp.sum(exchange(channel_part, KV).astype(jnp.float32), axis=0)
    layer_out = (after_own + channel * out_gain).astype(jnp.bfloat16)
    return layer_out, new_state[:, None]


def solution(mesh):
    grid = Mesh(mesh.devices.reshape(4, 4, CHIPS, PARTS, CORES), (*KV, *TP))
    return jax.shard_map(
        shards,
        mesh=grid,
        in_specs=(
            P(TP, KV),
            P(TP, KV, None, None),
            P(TP, KV),
            P(TP, KV),
            P(TP, KV),
            P(TP, KV),
            P(KV),
            P(KV),
            P(KV, TP),
            P(),
            P(),
            P(),
            P(),
            P(TP, KV),
            P(KV, TP),
        ),
        out_specs=(P(TP, KV), P(TP, KV, None, None)),
        check_vma=False,
    )
```

```python
import jax
import jax.numpy as jnp
from jax import lax
from jax.experimental import pallas as pl
from jax.experimental.pallas import tpu as pltpu
from jax.sharding import Mesh
from jax.sharding import PartitionSpec as P

KV = ("y", "x")
TP = ("zh", "zo", "c")
NEAR = ("zo", "c")
PARTS = 4
CHIPS = 8
SLAB = 4
PIECES = 4

epsilon = 1e-06


def exchange(blocks, axes):
    return lax.all_to_all(blocks, axes, 0, 0, tiled=True)


def near(value):
    return pltpu.with_memory_space_constraint(value, pltpu.VMEM)


def run_copies(copies, sems):
    started = [
        pltpu.make_async_copy(src, dst, sems.at[k]) for k, (src, dst) in enumerate(copies)
    ]
    for copy in started:
        copy.start()
    return started


def pack_body(
    residual, wq, wf, wv, wg, mix, up, down, long_ref, short_ref, spread_ref, sems
):
    rows, cols = wq.shape
    part = mix.shape[0] // 4
    hidden = up.shape[1]
    copies = [(up, long_ref.at[:, :hidden]), (down, long_ref.at[:, hidden:])]
    for k, w in enumerate((wq, wf, wv, wg)):
        at = slice(k * cols, (k + 1) * cols)
        copies.append((w, short_ref.at[:rows, at]))
        copies.append((mix.at[k * part : (k + 1) * part], short_ref.at[rows:, at]))
    started = run_copies(copies, sems)
    spread_ref[...] = jnp.broadcast_to(residual[...][None], spread_ref.shape)
    for copy in started:
        copy.wait()


def pack(residual, wq, wf, wv, wg, mix, up, down, peers):
    rows, cols = wq.shape
    anywhere = pl.BlockSpec(memory_space=pl.ANY)
    vmem = pl.BlockSpec(memory_space=pltpu.VMEM)
    return pl.pallas_call(
        pack_body,
        out_shape=(
            jax.ShapeDtypeStruct((rows, up.shape[1] + down.shape[1]), up.dtype),
            pltpu.VMEM((rows + mix.shape[0] // 4, 4 * cols), wq.dtype),
            pltpu.VMEM((peers, *residual.shape), residual.dtype),
        ),
        in_specs=[vmem] + [anywhere] * 7,
        out_specs=(vmem,) * 3,
        scratch_shapes=[pltpu.SemaphoreType.DMA((10,))],
        name="pack",
    )(residual, wq, wf, wv, wg, mix, up, down)


def project_body(x_ref, gain_ref, short_ref, out_ref):
    zo, core = lax.axis_index("zo"), lax.axis_index("c")
    groups, _, height, width = x_ref.shape
    rows = width // 2
    squares = [None] * PARTS
    for f in range(groups):
        for h in range(PARTS):
            x = x_ref[f, h].astype(jnp.float32)
            squares[h] = x * x if f == 0 else squares[h] + x * x
    scale = [
        lax.rsqrt(jnp.sum(s, axis=-1, keepdims=True) / (groups * width) + epsilon)
        for s in squares
    ]
    lane = lax.broadcasted_iota(jnp.int32, (1, width), 1)
    here = (lane >= rows) == (core == 1)
    total = None
    for k in range(CHIPS):
        f = 2 * k + zo
        gain = gain_ref[pl.ds(f, 1)]
        x = jnp.concatenate(
            [
                jnp.where(
                    here, x_ref[f, h].astype(jnp.float32) * scale[h] * gain, 0.0
                ).astype(jnp.bfloat16)
                for h in range(PARTS)
            ],
            axis=0,
        )
        w = jnp.concatenate([short_ref[k, :rows]] * 2, axis=0)
        term = jnp.dot(x, w, preferred_element_type=jnp.float32)
        total = term if total is None else total + term
    for h in range(PARTS):
        out_ref[h] = total[h * height : (h + 1) * height].astype(out_ref.dtype)


def project(x, gain, short):
    return pl.pallas_call(
        project_body,
        out_shape=pltpu.VMEM((PARTS, x.shape[2], short.shape[2]), jnp.bfloat16),
        name="project",
    )(near(x), gain, near(short))


def recur_body(
    part_ref,
    prior,
    floor_ref,
    gain_ref,
    state,
    out_ref,
    prior_ref,
    state_ref,
    read_ref,
    in_sems,
    out_sems,
):
    rows = prior_ref.shape[0]
    chunks = [slice(k, k + SLAB) for k in range(0, rows, SLAB)]
    fetches = run_copies([(prior.at[c], prior_ref.at[c]) for c in chunks], in_sems)
    stores = [
        pltpu.make_async_copy(state_ref.at[c], state.at[c], out_sems.at[k])
        for k, c in enumerate(chunks)
    ]
    pre = part_ref[0].astype(jnp.float32)
    for k in range(1, PARTS):
        pre = pre + part_ref[k].astype(jnp.float32)
    pre = pre.astype(jnp.bfloat16).astype(jnp.float32)
    width = prior_ref.shape[1]
    query = jax.nn.silu(pre[:, :width])
    floor = floor_ref[...]
    forget = floor + (1.0 - floor) * jax.nn.sigmoid(pre[:, width : 2 * width])
    value = pre[:, 2 * width : 3 * width]
    gate = jax.nn.sigmoid(pre[:, 3 * width :])
    forget_t = forget.T
    query_t = query.T
    for b in range(rows):
        if b % SLAB == 0:
            fetches[b // SLAB].wait()
        keep = forget_t[:, b : b + 1]
        fresh = keep * prior_ref[b] + (1.0 - keep) * value[b : b + 1]
        state_ref[b] = fresh
        read_ref[b : b + 1] = jnp.sum(query_t[:, b : b + 1] * fresh, axis=0, keepdims=True)
        if b % SLAB == SLAB - 1:
            stores[b // SLAB].start()
    read = read_ref[...]
    scale = lax.rsqrt(jnp.mean(read * read, axis=-1, keepdims=True) + epsilon)
    out_ref[...] = (read * scale * gain_ref[...] * gate).astype(out_ref.dtype)
    for store in stores:
        store.wait()


def recur(part, prior, floor, gain):
    rows, width, _ = prior.shape
    anywhere = pl.BlockSpec(memory_space=pl.ANY)
    vmem = pl.BlockSpec(memory_space=pltpu.VMEM)
    return pl.pallas_call(
        recur_body,
        out_shape=(
            jax.ShapeDtypeStruct(prior.shape, jnp.float32),
            pltpu.VMEM((rows, width), jnp.bfloat16),
        ),
        in_specs=[vmem, anywhere, vmem, vmem],
        out_specs=(anywhere, vmem),
        scratch_shapes=[
            pltpu.VMEM(prior.shape, jnp.float32),
            pltpu.VMEM(prior.shape, jnp.float32),
            pltpu.VMEM((rows, width), jnp.float32),
            pltpu.SemaphoreType.DMA((rows // SLAB,)),
            pltpu.SemaphoreType.DMA((rows // SLAB,)),
        ],
        name="recur",
    )(near(part), prior, floor, gain)


def mix_body(gated_ref, short_ref, out_ref, order_ref):
    height, width = gated_ref.shape[1:]
    rows = width // 2
    for h in range(PARTS):
        order_ref[pl.ds(h, height, stride=PARTS)] = gated_ref[h].astype(jnp.float32)
    left = order_ref[...].astype(jnp.bfloat16)
    for k in range(CHIPS // 2):
        right = jnp.concatenate(
            [
                short_ref[2 * k + half, rows:, j * width : (j + 1) * width]
                for half in range(2)
                for j in range(4)
            ],
            axis=0,
        )
        out_ref[pl.ds(k, PARTS * height, stride=CHIPS // 2)] = lax.dot_general(
            left, right, (((1,), (1,)), ((), ())), preferred_element_type=jnp.float32
        )


def mix_out(gated, short):
    height, width = gated.shape[1:]
    return pl.pallas_call(
        mix_body,
        out_shape=pltpu.VMEM((CHIPS // 2 * PARTS * height, width), jnp.float32),
        scratch_shapes=[pltpu.VMEM((PARTS * height, width), jnp.float32)],
        name="mix_out",
    )(near(gated), near(short))


def row_body(sums_ref, x_ref, gain_ref, out_ref, mixed_ref):
    own = 2 * lax.axis_index("zo") + lax.axis_index("c")
    place = lax.axis_index("y") * lax.axis_size("x") + lax.axis_index("x")
    groups, width = gain_ref.shape
    pairs = CHIPS // 2
    total = sums_ref[:groups]
    for k in range(1, groups):
        total = total + sums_ref[k * groups : (k + 1) * groups]
    first = lax.broadcasted_iota(jnp.int32, (pairs, width), 1) < width // 2
    for h in range(2):
        zero = total[2 * h * pairs : (2 * h + 1) * pairs]
        one = total[(2 * h + 1) * pairs : (2 * h + 2) * pairs]
        even = jnp.where(first, zero, pltpu.roll(one, width // 2, 1))
        odd = jnp.where(first, pltpu.roll(zero, width // 2, 1), one)
        mixed_ref[pl.ds(h, pairs, stride=4)] = even
        mixed_ref[pl.ds(2 + h, pairs, stride=4)] = odd
    mixed = mixed_ref[...]
    scale = lax.rsqrt(jnp.sum(mixed * mixed) / gain_ref.size + epsilon)
    stream = x_ref[:, own].astype(jnp.float32)
    at = lax.broadcasted_iota(jnp.int32, stream.shape, 1) == place
    row = jnp.sum(jnp.where(at, stream, 0.0), axis=1)
    after = (row + mixed * scale * gain_ref[...]).astype(out_ref.dtype)
    out_ref[...] = jnp.broadcast_to(after[None], out_ref.shape)


def row_update(sums, x, gain):
    groups, width = gain.shape
    return pl.pallas_call(
        row_body,
        out_shape=pltpu.VMEM((groups, groups, width), jnp.bfloat16),
        scratch_shapes=[pltpu.VMEM((groups, width), jnp.float32)],
        name="row_update",
    )(near(sums), near(x), gain)


def mlp_body(
    row_ref,
    pre_ref,
    post_ref,
    long_ref,
    out_ref,
    own_ref,
    gain_ref,
    after_ref,
    up_ref,
    down_ref,
    sems,
):
    place = lax.axis_index("y") * lax.axis_size("x") + lax.axis_index("x")
    groups, width = pre_ref.shape
    height = row_ref.shape[0]
    units = up_ref.shape[1]
    full = groups * width
    pieces = [slice(k, k + full // PIECES) for k in range(0, full, full // PIECES)]
    copies = run_copies(
        [(long_ref.at[p, :units], up_ref.at[p]) for p in pieces]
        + [(long_ref.at[p, units:], down_ref.at[p]) for p in pieces],
        sems,
    )
    for row in range(height):
        after_ref[row * groups : (row + 1) * groups] = row_ref[row].astype(jnp.float32)
    after = [after_ref[pl.ds(f, height, stride=groups)] for f in range(groups)]
    squares = after[0] * after[0]
    for f in range(1, groups):
        squares = squares + after[f] * after[f]
    scale = lax.rsqrt(
        jnp.sum(squares, axis=-1, keepdims=True) / full + epsilon
    )
    hidden = jnp.concatenate(
        [
            (after[f] * scale * pre_ref[f : f + 1]).astype(jnp.bfloat16)
            for f in range(groups)
        ],
        axis=1,
    )
    own_ref[...] = after_ref[pl.ds(place, height, stride=groups)]
    gain_ref[...] = post_ref[pl.ds(place, 1)]
    up = None
    for k, p in enumerate(pieces):
        copies[k].wait()
        term = jnp.dot(hidden[:, p], up_ref[p], preferred_element_type=jnp.float32)
        up = term if up is None else up + term
    squared = jnp.square(jnp.maximum(up, 0.0)).astype(jnp.bfloat16)
    for k, p in enumerate(pieces):
        copies[PIECES + k].wait()
        channel = lax.dot_general(
            squared, down_ref[p], (((1,), (1,)), ((), ())), preferred_element_type=jnp.float32
        )
        for f in range(groups // PIECES):
            out_ref[k * (groups // PIECES) + f] = channel[
                :, f * width : (f + 1) * width
            ].astype(out_ref.dtype)


def mlp(after, pre, post, weights, hidden):
    rows, groups, width = after.shape
    vmem = pl.BlockSpec(memory_space=pltpu.VMEM)
    return pl.pallas_call(
        mlp_body,
        out_shape=(
            pltpu.VMEM((groups, rows, width), jnp.bfloat16),
            pltpu.VMEM((rows, width), jnp.float32),
            pltpu.VMEM((1, width), jnp.float32),
        ),
        in_specs=[vmem] * 3 + [pl.BlockSpec(memory_space=pl.ANY)],
        scratch_shapes=[
            pltpu.VMEM((rows * groups, width), jnp.float32),
            pltpu.VMEM((weights.shape[0], hidden), jnp.bfloat16),
            pltpu.VMEM((weights.shape[0], hidden), jnp.bfloat16),
            pltpu.SemaphoreType.DMA((2 * PIECES,)),
        ],
        name="mlp",
    )(near(after), pre, post, weights)


def shards(
    residual,
    prior_state,
    w_query,
    w_forget,
    w_value,
    w_outgate,
    forget_floor,
    group_gain,
    w_mix_out,
    gain_mix_pre,
    gain_mix_post,
    gain_mlp_pre,
    gain_mlp_post,
    w_up,
    w_down,
):
    batch_rows, own_cols = residual.shape
    groups = lax.axis_size(KV)
    hidden = w_up.shape[1]

    long, short, spread = pack(
        residual,
        w_query,
        w_forget,
        w_value,
        w_outgate,
        w_mix_out.T,
        w_up,
        w_down.T,
        groups * PARTS,
    )
    long = lax.all_gather(long, TP, axis=0, tiled=True)
    stream = exchange(spread, (*KV, *NEAR)).reshape(groups, PARTS, batch_rows, own_cols)
    short = lax.all_gather(short, "zh", axis=0)
    part = exchange(project(stream, gain_mix_pre.reshape(groups, own_cols), short), NEAR)
    new_state, gated = recur(
        part, prior_state[:, 0], forget_floor[None], group_gain[None]
    )
    mixed_part = mix_out(lax.all_gather(gated, NEAR, axis=0), short)
    mixed = exchange(
        mixed_part.reshape(groups * PARTS, CHIPS // 2, own_cols), (*KV, *NEAR)
    )
    after_row = row_update(
        mixed.reshape(-1, own_cols), stream, gain_mix_post.reshape(groups, own_cols)
    )
    channel_part, after_own, out_gain = mlp(
        exchange(after_row, KV),
        gain_mlp_pre.reshape(groups, own_cols),
        gain_mlp_post.reshape(groups, own_cols),
        long,
        hidden,
    )
    channel = jnp.sum(exchange(channel_part, KV).astype(jnp.float32), axis=0)
    layer_out = (after_own + channel * out_gain).astype(jnp.bfloat16)
    return layer_out, new_state[:, None]


def solution(mesh):
    grid = Mesh(mesh.devices.reshape(4, 4, CHIPS, 2, 2), (*KV, *TP))
    return jax.shard_map(
        shards,
        mesh=grid,
        in_specs=(
            P(TP, KV),
            P(TP, KV, None, None),
            P(TP, KV),
            P(TP, KV),
            P(TP, KV),
            P(TP, KV),
            P(KV),
            P(KV),
            P(KV, TP),
            P(),
            P(),
            P(),
            P(),
            P(TP, KV),
            P(KV, TP),
        ),
        out_specs=(P(TP, KV), P(TP, KV, None, None)),
        check_vma=False,
    )
```

```python
import jax
import jax.numpy as jnp
from jax import lax
from jax.experimental import pallas as pl
from jax.experimental.pallas import tpu as pltpu
from jax.sharding import Mesh
from jax.sharding import PartitionSpec as P

KV = ("y", "x")
TP = ("zh", "zo", "c")
NEAR = ("zo", "c")
PARTS = 4
CHIPS = 8
SLAB = 4
PIECES = 4

epsilon = 1e-06


def exchange(blocks, axes):
    return lax.all_to_all(blocks, axes, 0, 0, tiled=True)


def near(value):
    return pltpu.with_memory_space_constraint(value, pltpu.VMEM)


def run_copies(copies, sems):
    started = [
        pltpu.make_async_copy(src, dst, sems.at[k]) for k, (src, dst) in enumerate(copies)
    ]
    for copy in started:
        copy.start()
    return started


def pack_body(
    residual, wq, wf, wv, wg, mix, up, down, long_ref, short_ref, spread_ref, sems
):
    rows, cols = wq.shape
    part = mix.shape[0] // 4
    hidden = up.shape[1]
    copies = [(up, long_ref.at[:, :hidden]), (down, long_ref.at[:, hidden:])]
    for k, w in enumerate((wq, wf, wv, wg)):
        at = slice(k * cols, (k + 1) * cols)
        copies.append((w, short_ref.at[:rows, at]))
        copies.append((mix.at[k * part : (k + 1) * part], short_ref.at[rows:, at]))
    started = run_copies(copies, sems)
    spread_ref[...] = jnp.broadcast_to(residual[...][None], spread_ref.shape)
    for copy in started:
        copy.wait()


def pack(residual, wq, wf, wv, wg, mix, up, down, peers):
    rows, cols = wq.shape
    anywhere = pl.BlockSpec(memory_space=pl.ANY)
    vmem = pl.BlockSpec(memory_space=pltpu.VMEM)
    return pl.pallas_call(
        pack_body,
        out_shape=(
            jax.ShapeDtypeStruct((rows, up.shape[1] + down.shape[1]), up.dtype),
            pltpu.VMEM((rows + mix.shape[0] // 4, 4 * cols), wq.dtype),
            pltpu.VMEM((peers, *residual.shape), residual.dtype),
        ),
        in_specs=[vmem] + [anywhere] * 7,
        out_specs=(vmem,) * 3,
        scratch_shapes=[pltpu.SemaphoreType.DMA((10,))],
        name="pack",
    )(residual, wq, wf, wv, wg, mix, up, down)


def project_body(x_ref, gain_ref, short_ref, out_ref, mix_ref):
    zo, core = lax.axis_index("zo"), lax.axis_index("c")
    groups, _, height, width = x_ref.shape
    rows = width // 2
    squares = [None] * PARTS
    for f in range(groups):
        for h in range(PARTS):
            x = x_ref[f, h].astype(jnp.float32)
            squares[h] = x * x if f == 0 else squares[h] + x * x
    scale = [
        lax.rsqrt(jnp.sum(s, axis=-1, keepdims=True) / (groups * width) + epsilon)
        for s in squares
    ]
    lane = lax.broadcasted_iota(jnp.int32, (1, width), 1)
    here = (lane >= rows) == (core == 1)
    total = None
    for k in range(CHIPS):
        f = 2 * k + zo
        gain = gain_ref[pl.ds(f, 1)]
        x = jnp.concatenate(
            [
                jnp.where(
                    here, x_ref[f, h].astype(jnp.float32) * scale[h] * gain, 0.0
                ).astype(jnp.bfloat16)
                for h in range(PARTS)
            ],
            axis=0,
        )
        w = jnp.concatenate([short_ref[k, :rows]] * 2, axis=0)
        term = jnp.dot(x, w, preferred_element_type=jnp.float32)
        total = term if total is None else total + term
        for j in range(4):
            mix_ref[k * rows + j * (rows // 4) : k * rows + (j + 1) * (rows // 4)] = (
                short_ref[k, rows:, j * width : (j + 1) * width]
            )
    for h in range(PARTS):
        out_ref[h] = total[h * height : (h + 1) * height].astype(out_ref.dtype)


def project(x, gain, short):
    return pl.pallas_call(
        project_body,
        out_shape=(
            pltpu.VMEM((PARTS, x.shape[2], short.shape[2]), jnp.bfloat16),
            pltpu.VMEM((CHIPS * x.shape[3] // 2, x.shape[3]), jnp.bfloat16),
        ),
        name="project",
    )(near(x), gain, near(short))


def gates(pre, floor):
    width = floor.shape[1]
    forget = floor + (1.0 - floor) * jax.nn.sigmoid(pre[:, width : 2 * width])
    return forget, pre[:, 2 * width : 3 * width]


def read_body(
    part_ref, prior, floor_ref, gain_ref, out_ref, pre_ref, prior_ref, read_ref, sems
):
    rows, width, _ = prior_ref.shape
    chunks = [slice(k, k + SLAB) for k in range(0, rows, SLAB)]
    fetches = run_copies([(prior.at[c], prior_ref.at[c]) for c in chunks], sems)
    pre = part_ref[0].astype(jnp.float32)
    for k in range(1, PARTS):
        pre = pre + part_ref[k].astype(jnp.float32)
    pre = pre.astype(jnp.bfloat16).astype(jnp.float32)
    pre_ref[...] = pre
    query = jax.nn.silu(pre[:, :width])
    forget, value = gates(pre, floor_ref[...])
    gate = jax.nn.sigmoid(pre[:, 3 * width :])
    kept = (query * forget).T
    fresh = jnp.sum(query * (1.0 - forget), axis=-1, keepdims=True) * value
    for b in range(rows):
        if b % SLAB == 0:
            fetches[b // SLAB].wait()
        read_ref[b : b + 1] = jnp.sum(
            kept[:, b : b + 1] * prior_ref[b], axis=0, keepdims=True
        )
    read = read_ref[...] + fresh
    scale = lax.rsqrt(jnp.mean(read * read, axis=-1, keepdims=True) + epsilon)
    out_ref[...] = (read * scale * gain_ref[...] * gate).astype(out_ref.dtype)


def read_out(part, prior, floor, gain):
    rows, width, _ = prior.shape
    vmem = pl.BlockSpec(memory_space=pltpu.VMEM)
    return pl.pallas_call(
        read_body,
        out_shape=(
            pltpu.VMEM((rows, width), jnp.bfloat16),
            pltpu.VMEM((rows, part.shape[2]), jnp.float32),
        ),
        in_specs=[vmem, pl.BlockSpec(memory_space=pl.ANY), vmem, vmem],
        out_specs=(vmem, vmem),
        scratch_shapes=[
            pltpu.VMEM(prior.shape, jnp.float32),
            pltpu.VMEM((rows, width), jnp.float32),
            pltpu.SemaphoreType.DMA((rows // SLAB,)),
        ],
        name="read_out",
    )(near(part), prior, floor, gain)


def update_body(pre_ref, prior, floor_ref, state, prior_ref, state_ref, in_sems, out_sems):
    rows = prior_ref.shape[0]
    chunks = [slice(k, k + SLAB) for k in range(0, rows, SLAB)]
    fetches = run_copies([(prior.at[c], prior_ref.at[c]) for c in chunks], in_sems)
    stores = [
        pltpu.make_async_copy(state_ref.at[c], state.at[c], out_sems.at[k])
        for k, c in enumerate(chunks)
    ]
    forget, value = gates(pre_ref[...], floor_ref[...])
    forget = forget.T
    for b in range(rows):
        if b % SLAB == 0:
            fetches[b // SLAB].wait()
        keep = forget[:, b : b + 1]
        state_ref[b] = keep * prior_ref[b] + (1.0 - keep) * value[b : b + 1]
        if b % SLAB == SLAB - 1:
            stores[b // SLAB].start()
    for store in stores:
        store.wait()


def update(pre, prior, floor):
    rows = prior.shape[0]
    anywhere = pl.BlockSpec(memory_space=pl.ANY)
    vmem = pl.BlockSpec(memory_space=pltpu.VMEM)
    return pl.pallas_call(
        update_body,
        out_shape=jax.ShapeDtypeStruct(prior.shape, jnp.float32),
        in_specs=[vmem, anywhere, vmem],
        out_specs=anywhere,
        scratch_shapes=[
            pltpu.VMEM(prior.shape, jnp.float32),
            pltpu.VMEM(prior.shape, jnp.float32),
            pltpu.SemaphoreType.DMA((rows // SLAB,)),
            pltpu.SemaphoreType.DMA((rows // SLAB,)),
        ],
        name="update",
    )(near(pre), prior, floor)


def mix_body(gated_ref, w_ref, out_ref):
    height, width = gated_ref.shape
    rows = width // 2
    left = gated_ref[...]
    for k in range(CHIPS):
        for zo in range(2):
            right = jnp.concatenate(
                [w_ref[2 * zo + c, k * rows : (k + 1) * rows] for c in range(2)], axis=0
            )
            out_ref[pl.ds(2 * k + zo, height, stride=2 * CHIPS)] = lax.dot_general(
                left, right, (((1,), (1,)), ((), ())), preferred_element_type=jnp.float32
            )


def mix_out(gated, weights):
    height, width = gated.shape
    return pl.pallas_call(
        mix_body,
        out_shape=pltpu.VMEM((2 * CHIPS * height, width), jnp.float32),
        name="mix_out",
    )(near(gated), near(weights))


def row_body(sums_ref, x_ref, gain_ref, out_ref):
    own = 2 * lax.axis_index("zo") + lax.axis_index("c")
    place = lax.axis_index("y") * lax.axis_size("x") + lax.axis_index("x")
    mixed = sums_ref[0]
    for k in range(1, sums_ref.shape[0]):
        mixed = mixed + sums_ref[k]
    scale = lax.rsqrt(jnp.sum(mixed * mixed) / gain_ref.size + epsilon)
    stream = x_ref[:, own].astype(jnp.float32)
    at = lax.broadcasted_iota(jnp.int32, stream.shape, 1) == place
    row = jnp.sum(jnp.where(at, stream, 0.0), axis=1)
    after = (row + mixed * scale * gain_ref[...]).astype(out_ref.dtype)
    out_ref[...] = jnp.broadcast_to(after[None], out_ref.shape)


def row_update(sums, x, gain):
    groups, width = gain.shape
    return pl.pallas_call(
        row_body,
        out_shape=pltpu.VMEM((groups, groups, width), jnp.bfloat16),
        name="row_update",
    )(near(sums), near(x), gain)


def mlp_body(
    row_ref,
    pre_ref,
    post_ref,
    long_ref,
    out_ref,
    own_ref,
    gain_ref,
    after_ref,
    up_ref,
    down_ref,
    sems,
):
    place = lax.axis_index("y") * lax.axis_size("x") + lax.axis_index("x")
    groups, width = pre_ref.shape
    height = row_ref.shape[0]
    units = up_ref.shape[1]
    full = groups * width
    pieces = [slice(k, k + full // PIECES) for k in range(0, full, full // PIECES)]
    copies = run_copies(
        [(long_ref.at[p, :units], up_ref.at[p]) for p in pieces]
        + [(long_ref.at[p, units:], down_ref.at[p]) for p in pieces],
        sems,
    )
    for row in range(height):
        after_ref[row * groups : (row + 1) * groups] = row_ref[row].astype(jnp.float32)
    after = [after_ref[pl.ds(f, height, stride=groups)] for f in range(groups)]
    squares = after[0] * after[0]
    for f in range(1, groups):
        squares = squares + after[f] * after[f]
    scale = lax.rsqrt(
        jnp.sum(squares, axis=-1, keepdims=True) / full + epsilon
    )
    hidden = jnp.concatenate(
        [
            (after[f] * scale * pre_ref[f : f + 1]).astype(jnp.bfloat16)
            for f in range(groups)
        ],
        axis=1,
    )
    own_ref[...] = after_ref[pl.ds(place, height, stride=groups)]
    gain_ref[...] = post_ref[pl.ds(place, 1)]
    up = None
    for k, p in enumerate(pieces):
        copies[k].wait()
        term = jnp.dot(hidden[:, p], up_ref[p], preferred_element_type=jnp.float32)
        up = term if up is None else up + term
    squared = jnp.square(jnp.maximum(up, 0.0)).astype(jnp.bfloat16)
    for k, p in enumerate(pieces):
        copies[PIECES + k].wait()
        channel = lax.dot_general(
            squared, down_ref[p], (((1,), (1,)), ((), ())), preferred_element_type=jnp.float32
        )
        for f in range(groups // PIECES):
            out_ref[k * (groups // PIECES) + f] = channel[
                :, f * width : (f + 1) * width
            ].astype(out_ref.dtype)


def mlp(after, pre, post, weights, hidden):
    rows, groups, width = after.shape
    vmem = pl.BlockSpec(memory_space=pltpu.VMEM)
    return pl.pallas_call(
        mlp_body,
        out_shape=(
            pltpu.VMEM((groups, rows, width), jnp.bfloat16),
            pltpu.VMEM((rows, width), jnp.float32),
            pltpu.VMEM((1, width), jnp.float32),
        ),
        in_specs=[vmem] * 3 + [pl.BlockSpec(memory_space=pl.ANY)],
        scratch_shapes=[
            pltpu.VMEM((rows * groups, width), jnp.float32),
            pltpu.VMEM((weights.shape[0], hidden), jnp.bfloat16),
            pltpu.VMEM((weights.shape[0], hidden), jnp.bfloat16),
            pltpu.SemaphoreType.DMA((2 * PIECES,)),
        ],
        name="mlp",
    )(near(after), pre, post, weights)


def shards(
    residual,
    prior_state,
    w_query,
    w_forget,
    w_value,
    w_outgate,
    forget_floor,
    group_gain,
    w_mix_out,
    gain_mix_pre,
    gain_mix_post,
    gain_mlp_pre,
    gain_mlp_post,
    w_up,
    w_down,
):
    batch_rows, own_cols = residual.shape
    groups = lax.axis_size(KV)
    hidden = w_up.shape[1]

    long, short, spread = pack(
        residual,
        w_query,
        w_forget,
        w_value,
        w_outgate,
        w_mix_out.T,
        w_up,
        w_down.T,
        groups * PARTS,
    )
    long = lax.all_gather(long, TP, axis=0, tiled=True)
    stream = exchange(spread, (*KV, *NEAR)).reshape(groups, PARTS, batch_rows, own_cols)
    short = lax.all_gather(short, "zh", axis=0)
    part, mix = project(stream, gain_mix_pre.reshape(groups, own_cols), short)
    part = exchange(part, NEAR)
    prior = prior_state[:, 0]
    gated, pre = read_out(part, prior, forget_floor[None], group_gain[None])
    new_state = update(pre, prior, forget_floor[None])
    mix = lax.all_gather(mix, NEAR, axis=0)
    mixed = exchange(mix_out(gated, mix).reshape(batch_rows, groups, own_cols), KV)
    after_row = row_update(mixed, stream, gain_mix_post.reshape(groups, own_cols))
    channel_part, after_own, out_gain = mlp(
        exchange(after_row, KV),
        gain_mlp_pre.reshape(groups, own_cols),
        gain_mlp_post.reshape(groups, own_cols),
        long,
        hidden,
    )
    channel = jnp.sum(exchange(channel_part, KV).astype(jnp.float32), axis=0)
    layer_out = (after_own + channel * out_gain).astype(jnp.bfloat16)
    return layer_out, new_state[:, None]


def solution(mesh):
    grid = Mesh(mesh.devices.reshape(4, 4, CHIPS, 2, 2), (*KV, *TP))
    return jax.shard_map(
        shards,
        mesh=grid,
        in_specs=(
            P(TP, KV),
            P(TP, KV, None, None),
            P(TP, KV),
            P(TP, KV),
            P(TP, KV),
            P(TP, KV),
            P(KV),
            P(KV),
            P(KV, TP),
            P(),
            P(),
            P(),
            P(),
            P(TP, KV),
            P(KV, TP),
        ),
        out_specs=(P(TP, KV), P(TP, KV, None, None)),
        check_vma=False,
    )
```

```python
import jax
import jax.numpy as jnp
from jax import lax
from jax.experimental import pallas as pl
from jax.experimental.pallas import tpu as pltpu
from jax.sharding import Mesh
from jax.sharding import PartitionSpec as P

KV = ("y", "x")
TP = ("zh", "zo", "c")
NEAR = ("zo", "c")
PARTS = 4
CHIPS = 8
SLAB = 4
PIECES = 4

epsilon = 1e-06


def exchange(blocks, axes):
    return lax.all_to_all(blocks, axes, 0, 0, tiled=True)


def near(value):
    return pltpu.with_memory_space_constraint(value, pltpu.VMEM)


def run_copies(copies, sems):
    started = [
        pltpu.make_async_copy(src, dst, sems.at[k]) for k, (src, dst) in enumerate(copies)
    ]
    for copy in started:
        copy.start()
    return started


def pack_body(
    residual,
    wq,
    wf,
    wv,
    wg,
    mix,
    up,
    down,
    long,
    short_ref,
    spread,
    long_ref,
    spread_ref,
    sems,
    out_sems,
):
    rows, cols = wq.shape
    part = mix.shape[0] // 4
    hidden = up.shape[1]
    copies = [(up, long_ref.at[:, :hidden]), (down, long_ref.at[:, hidden:])]
    for k, w in enumerate((wq, wf, wv, wg)):
        at = slice(k * cols, (k + 1) * cols)
        copies.append((w, short_ref.at[:rows, at]))
        copies.append((mix.at[k * part : (k + 1) * part], short_ref.at[rows:, at]))
    started = run_copies(copies, sems)
    spread_ref[...] = jnp.broadcast_to(residual[...][None], spread_ref.shape)
    outs = [
        pltpu.make_async_copy(spread_ref, spread, out_sems.at[0]),
        pltpu.make_async_copy(long_ref, long, out_sems.at[1]),
    ]
    outs[0].start()
    for copy in started[:2]:
        copy.wait()
    outs[1].start()
    for copy in started[2:] + outs:
        copy.wait()


def pack(residual, wq, wf, wv, wg, mix, up, down, peers):
    rows, cols = wq.shape
    anywhere = pl.BlockSpec(memory_space=pl.ANY)
    vmem = pl.BlockSpec(memory_space=pltpu.VMEM)
    long = (rows, up.shape[1] + down.shape[1])
    spread = (peers, *residual.shape)
    return pl.pallas_call(
        pack_body,
        out_shape=(
            jax.ShapeDtypeStruct(long, up.dtype),
            pltpu.VMEM((rows + mix.shape[0] // 4, 4 * cols), wq.dtype),
            jax.ShapeDtypeStruct(spread, residual.dtype),
        ),
        in_specs=[vmem] + [anywhere] * 7,
        out_specs=(anywhere, vmem, anywhere),
        scratch_shapes=[
            pltpu.VMEM(long, up.dtype),
            pltpu.VMEM(spread, residual.dtype),
            pltpu.SemaphoreType.DMA((10,)),
            pltpu.SemaphoreType.DMA((2,)),
        ],
        name="pack",
    )(residual, wq, wf, wv, wg, mix, up, down)


def project_body(x_ref, gain_ref, short_ref, out_ref, mix_ref):
    zo, core = lax.axis_index("zo"), lax.axis_index("c")
    groups, _, height, width = x_ref.shape
    rows = width // 2
    squares = [None] * PARTS
    for f in range(groups):
        for h in range(PARTS):
            x = x_ref[f, h].astype(jnp.float32)
            squares[h] = x * x if f == 0 else squares[h] + x * x
    scale = [
        lax.rsqrt(jnp.sum(s, axis=-1, keepdims=True) / (groups * width) + epsilon)
        for s in squares
    ]
    lane = lax.broadcasted_iota(jnp.int32, (1, width), 1)
    here = (lane >= rows) == (core == 1)
    total = None
    for k in range(CHIPS):
        f = 2 * k + zo
        gain = gain_ref[pl.ds(f, 1)]
        x = jnp.concatenate(
            [
                jnp.where(
                    here, x_ref[f, h].astype(jnp.float32) * scale[h] * gain, 0.0
                ).astype(jnp.bfloat16)
                for h in range(PARTS)
            ],
            axis=0,
        )
        w = jnp.concatenate([short_ref[k, :rows]] * 2, axis=0)
        term = jnp.dot(x, w, preferred_element_type=jnp.float32)
        total = term if total is None else total + term
        for j in range(4):
            mix_ref[k * rows + j * (rows // 4) : k * rows + (j + 1) * (rows // 4)] = (
                short_ref[k, rows:, j * width : (j + 1) * width]
            )
    for h in range(PARTS):
        out_ref[h] = total[h * height : (h + 1) * height].astype(out_ref.dtype)


def project(x, gain, short):
    return pl.pallas_call(
        project_body,
        out_shape=(
            pltpu.VMEM((PARTS, x.shape[2], short.shape[2]), jnp.bfloat16),
            pltpu.VMEM((CHIPS * x.shape[3] // 2, x.shape[3]), jnp.bfloat16),
        ),
        name="project",
    )(near(x), gain, near(short))


def gates(pre, floor):
    width = floor.shape[1]
    forget = floor + (1.0 - floor) * jax.nn.sigmoid(pre[:, width : 2 * width])
    return forget, pre[:, 2 * width : 3 * width]


def read_body(
    part_ref, prior, floor_ref, gain_ref, out_ref, pre_ref, prior_ref, read_ref, sems
):
    rows, width, _ = prior_ref.shape
    chunks = [slice(k, k + SLAB) for k in range(0, rows, SLAB)]
    fetches = run_copies([(prior.at[c], prior_ref.at[c]) for c in chunks], sems)
    pre = part_ref[0].astype(jnp.float32)
    for k in range(1, PARTS):
        pre = pre + part_ref[k].astype(jnp.float32)
    pre = pre.astype(jnp.bfloat16).astype(jnp.float32)
    pre_ref[...] = pre
    query = jax.nn.silu(pre[:, :width])
    forget, value = gates(pre, floor_ref[...])
    gate = jax.nn.sigmoid(pre[:, 3 * width :])
    kept = (query * forget).T
    fresh = jnp.sum(query * (1.0 - forget), axis=-1, keepdims=True) * value
    for b in range(rows):
        if b % SLAB == 0:
            fetches[b // SLAB].wait()
        read_ref[b : b + 1] = jnp.sum(
            kept[:, b : b + 1] * prior_ref[b], axis=0, keepdims=True
        )
    read = read_ref[...] + fresh
    scale = lax.rsqrt(jnp.mean(read * read, axis=-1, keepdims=True) + epsilon)
    out_ref[...] = (read * scale * gain_ref[...] * gate).astype(out_ref.dtype)


def read_out(part, prior, floor, gain):
    rows, width, _ = prior.shape
    vmem = pl.BlockSpec(memory_space=pltpu.VMEM)
    return pl.pallas_call(
        read_body,
        out_shape=(
            pltpu.VMEM((rows, width), jnp.bfloat16),
            pltpu.VMEM((rows, part.shape[2]), jnp.float32),
        ),
        in_specs=[vmem, pl.BlockSpec(memory_space=pl.ANY), vmem, vmem],
        out_specs=(vmem, vmem),
        scratch_shapes=[
            pltpu.VMEM(prior.shape, jnp.float32),
            pltpu.VMEM((rows, width), jnp.float32),
            pltpu.SemaphoreType.DMA((rows // SLAB,)),
        ],
        name="read_out",
    )(near(part), prior, floor, gain)


def update_body(pre_ref, prior, floor_ref, state, prior_ref, state_ref, in_sems, out_sems):
    rows = prior_ref.shape[0]
    chunks = [slice(k, k + SLAB) for k in range(0, rows, SLAB)]
    fetches = run_copies([(prior.at[c], prior_ref.at[c]) for c in chunks], in_sems)
    stores = [
        pltpu.make_async_copy(state_ref.at[c], state.at[c], out_sems.at[k])
        for k, c in enumerate(chunks)
    ]
    forget, value = gates(pre_ref[...], floor_ref[...])
    forget = forget.T
    for b in range(rows):
        if b % SLAB == 0:
            fetches[b // SLAB].wait()
        keep = forget[:, b : b + 1]
        state_ref[b] = keep * prior_ref[b] + (1.0 - keep) * value[b : b + 1]
        if b % SLAB == SLAB - 1:
            stores[b // SLAB].start()
    for store in stores:
        store.wait()


def update(pre, prior, floor):
    rows = prior.shape[0]
    anywhere = pl.BlockSpec(memory_space=pl.ANY)
    vmem = pl.BlockSpec(memory_space=pltpu.VMEM)
    return pl.pallas_call(
        update_body,
        out_shape=jax.ShapeDtypeStruct(prior.shape, jnp.float32),
        in_specs=[vmem, anywhere, vmem],
        out_specs=anywhere,
        scratch_shapes=[
            pltpu.VMEM(prior.shape, jnp.float32),
            pltpu.VMEM(prior.shape, jnp.float32),
            pltpu.SemaphoreType.DMA((rows // SLAB,)),
            pltpu.SemaphoreType.DMA((rows // SLAB,)),
        ],
        name="update",
    )(near(pre), prior, floor)


def mix_body(gated_ref, w_ref, out_ref, sums_ref):
    height, width = gated_ref.shape
    rows = width // 2
    left = gated_ref[...]
    for k in range(CHIPS):
        for zo in range(2):
            right = jnp.concatenate(
                [w_ref[2 * zo + c, k * rows : (k + 1) * rows] for c in range(2)], axis=0
            )
            sums_ref[pl.ds(2 * k + zo, height, stride=2 * CHIPS)] = lax.dot_general(
                left, right, (((1,), (1,)), ((), ())), preferred_element_type=jnp.float32
            )
    for row in range(height):
        out_ref[row] = sums_ref[2 * CHIPS * row : 2 * CHIPS * (row + 1)].astype(
            out_ref.dtype
        )


def mix_out(gated, weights):
    height, width = gated.shape
    return pl.pallas_call(
        mix_body,
        out_shape=pltpu.VMEM((height, 2 * CHIPS, width), jnp.bfloat16),
        scratch_shapes=[pltpu.VMEM((2 * CHIPS * height, width), jnp.float32)],
        name="mix_out",
    )(near(gated), near(weights))


def row_body(sums_ref, x_ref, gain_ref, out_ref):
    own = 2 * lax.axis_index("zo") + lax.axis_index("c")
    place = lax.axis_index("y") * lax.axis_size("x") + lax.axis_index("x")
    mixed = sums_ref[0].astype(jnp.float32)
    for k in range(1, sums_ref.shape[0]):
        mixed = mixed + sums_ref[k].astype(jnp.float32)
    scale = lax.rsqrt(jnp.sum(mixed * mixed) / gain_ref.size + epsilon)
    stream = x_ref[:, own].astype(jnp.float32)
    at = lax.broadcasted_iota(jnp.int32, stream.shape, 1) == place
    row = jnp.sum(jnp.where(at, stream, 0.0), axis=1)
    after = (row + mixed * scale * gain_ref[...]).astype(out_ref.dtype)
    out_ref[...] = jnp.broadcast_to(after[None], out_ref.shape)


def row_update(sums, x, gain):
    groups, width = gain.shape
    return pl.pallas_call(
        row_body,
        out_shape=pltpu.VMEM((groups, groups, width), jnp.bfloat16),
        name="row_update",
    )(near(sums), near(x), gain)


def mlp_body(
    row_ref,
    pre_ref,
    post_ref,
    long_ref,
    out_ref,
    own_ref,
    gain_ref,
    after_ref,
    up_ref,
    down_ref,
    sems,
):
    place = lax.axis_index("y") * lax.axis_size("x") + lax.axis_index("x")
    groups, width = pre_ref.shape
    height = row_ref.shape[0]
    units = up_ref.shape[1]
    full = groups * width
    pieces = [slice(k, k + full // PIECES) for k in range(0, full, full // PIECES)]
    copies = run_copies(
        [(long_ref.at[p, :units], up_ref.at[p]) for p in pieces]
        + [(long_ref.at[p, units:], down_ref.at[p]) for p in pieces],
        sems,
    )
    for row in range(height):
        after_ref[row * groups : (row + 1) * groups] = row_ref[row].astype(jnp.float32)
    after = [after_ref[pl.ds(f, height, stride=groups)] for f in range(groups)]
    squares = after[0] * after[0]
    for f in range(1, groups):
        squares = squares + after[f] * after[f]
    scale = lax.rsqrt(
        jnp.sum(squares, axis=-1, keepdims=True) / full + epsilon
    )
    hidden = jnp.concatenate(
        [
            (after[f] * scale * pre_ref[f : f + 1]).astype(jnp.bfloat16)
            for f in range(groups)
        ],
        axis=1,
    )
    own_ref[...] = after_ref[pl.ds(place, height, stride=groups)]
    gain_ref[...] = post_ref[pl.ds(place, 1)]
    up = None
    for k, p in enumerate(pieces):
        copies[k].wait()
        term = jnp.dot(hidden[:, p], up_ref[p], preferred_element_type=jnp.float32)
        up = term if up is None else up + term
    squared = jnp.square(jnp.maximum(up, 0.0)).astype(jnp.bfloat16)
    for k, p in enumerate(pieces):
        copies[PIECES + k].wait()
        channel = lax.dot_general(
            squared, down_ref[p], (((1,), (1,)), ((), ())), preferred_element_type=jnp.float32
        )
        for f in range(groups // PIECES):
            out_ref[k * (groups // PIECES) + f] = channel[
                :, f * width : (f + 1) * width
            ].astype(out_ref.dtype)


def mlp(after, pre, post, weights, hidden):
    rows, groups, width = after.shape
    vmem = pl.BlockSpec(memory_space=pltpu.VMEM)
    return pl.pallas_call(
        mlp_body,
        out_shape=(
            pltpu.VMEM((groups, rows, width), jnp.bfloat16),
            pltpu.VMEM((rows, width), jnp.float32),
            pltpu.VMEM((1, width), jnp.float32),
        ),
        in_specs=[vmem] * 3 + [pl.BlockSpec(memory_space=pl.ANY)],
        scratch_shapes=[
            pltpu.VMEM((rows * groups, width), jnp.float32),
            pltpu.VMEM((weights.shape[0], hidden), jnp.bfloat16),
            pltpu.VMEM((weights.shape[0], hidden), jnp.bfloat16),
            pltpu.SemaphoreType.DMA((2 * PIECES,)),
        ],
        name="mlp",
    )(near(after), pre, post, weights)


def shards(
    residual,
    prior_state,
    w_query,
    w_forget,
    w_value,
    w_outgate,
    forget_floor,
    group_gain,
    w_mix_out,
    gain_mix_pre,
    gain_mix_post,
    gain_mlp_pre,
    gain_mlp_post,
    w_up,
    w_down,
):
    batch_rows, own_cols = residual.shape
    groups = lax.axis_size(KV)
    hidden = w_up.shape[1]

    long, short, spread = pack(
        residual,
        w_query,
        w_forget,
        w_value,
        w_outgate,
        w_mix_out.T,
        w_up,
        w_down.T,
        groups * PARTS,
    )
    long = lax.all_gather(long, TP, axis=0, tiled=True)
    stream = exchange(spread, (*KV, *NEAR)).reshape(groups, PARTS, batch_rows, own_cols)
    short = lax.all_gather(short, "zh", axis=0)
    part, mix = project(stream, gain_mix_pre.reshape(groups, own_cols), short)
    part = exchange(part, NEAR)
    prior = prior_state[:, 0]
    gated, pre = read_out(part, prior, forget_floor[None], group_gain[None])
    new_state = update(pre, prior, forget_floor[None])
    mix = lax.all_gather(mix, NEAR, axis=0)
    mixed = exchange(mix_out(gated, mix), KV)
    after_row = row_update(mixed, stream, gain_mix_post.reshape(groups, own_cols))
    channel_part, after_own, out_gain = mlp(
        exchange(after_row, KV),
        gain_mlp_pre.reshape(groups, own_cols),
        gain_mlp_post.reshape(groups, own_cols),
        long,
        hidden,
    )
    channel = jnp.sum(exchange(channel_part, KV).astype(jnp.float32), axis=0)
    layer_out = (after_own + channel * out_gain).astype(jnp.bfloat16)
    return layer_out, new_state[:, None]


def solution(mesh):
    grid = Mesh(mesh.devices.reshape(4, 4, CHIPS, 2, 2), (*KV, *TP))
    return jax.shard_map(
        shards,
        mesh=grid,
        in_specs=(
            P(TP, KV),
            P(TP, KV, None, None),
            P(TP, KV),
            P(TP, KV),
            P(TP, KV),
            P(TP, KV),
            P(KV),
            P(KV),
            P(KV, TP),
            P(),
            P(),
            P(),
            P(),
            P(TP, KV),
            P(KV, TP),
        ),
        out_specs=(P(TP, KV), P(TP, KV, None, None)),
        check_vma=False,
    )
```

```python
import jax
import jax.numpy as jnp
from jax import lax
from jax.experimental import pallas as pl
from jax.experimental.pallas import tpu as pltpu
from jax.sharding import Mesh
from jax.sharding import PartitionSpec as P

KV = ("y", "x")
TP = ("zh", "zo", "c")
NEAR = ("zo", "c")
PARTS = 4
CHIPS = 8
RINGS = [[2 * zh + (zh + g) % 2 for zh in range(CHIPS)] for g in range(2)]
SLAB = 4
PIECES = 4

epsilon = 1e-06


def exchange(blocks, axes):
    return lax.all_to_all(blocks, axes, 0, 0, tiled=True)


def near(value):
    return pltpu.with_memory_space_constraint(value, pltpu.VMEM)


def run_copies(copies, sems):
    started = [
        pltpu.make_async_copy(src, dst, sems.at[k]) for k, (src, dst) in enumerate(copies)
    ]
    for copy in started:
        copy.start()
    return started


def pack_body(
    residual,
    wq,
    wf,
    wv,
    wg,
    mix,
    up,
    down,
    long,
    short_ref,
    spread,
    long_ref,
    spread_ref,
    sems,
    out_sems,
):
    rows, cols = wq.shape
    part = mix.shape[0] // 4
    hidden = up.shape[1]
    copies = [(up, long_ref.at[:, :hidden]), (down, long_ref.at[:, hidden:])]
    for k, w in enumerate((wq, wf, wv, wg)):
        at = slice(k * cols, (k + 1) * cols)
        copies.append((w, short_ref.at[:rows, at]))
        copies.append((mix.at[k * part : (k + 1) * part], short_ref.at[rows:, at]))
    started = run_copies(copies, sems)
    spread_ref[...] = jnp.broadcast_to(residual[...][None], spread_ref.shape)
    outs = [
        pltpu.make_async_copy(spread_ref, spread, out_sems.at[0]),
        pltpu.make_async_copy(long_ref, long, out_sems.at[1]),
    ]
    outs[0].start()
    for copy in started[:2]:
        copy.wait()
    outs[1].start()
    for copy in started[2:] + outs:
        copy.wait()


def pack(residual, wq, wf, wv, wg, mix, up, down, peers):
    rows, cols = wq.shape
    anywhere = pl.BlockSpec(memory_space=pl.ANY)
    vmem = pl.BlockSpec(memory_space=pltpu.VMEM)
    long = (rows, up.shape[1] + down.shape[1])
    spread = (peers, *residual.shape)
    return pl.pallas_call(
        pack_body,
        out_shape=(
            jax.ShapeDtypeStruct(long, up.dtype),
            pltpu.VMEM((rows + mix.shape[0] // 4, 4 * cols), wq.dtype),
            jax.ShapeDtypeStruct(spread, residual.dtype),
        ),
        in_specs=[vmem] + [anywhere] * 7,
        out_specs=(anywhere, vmem, anywhere),
        scratch_shapes=[
            pltpu.VMEM(long, up.dtype),
            pltpu.VMEM(spread, residual.dtype),
            pltpu.SemaphoreType.DMA((10,)),
            pltpu.SemaphoreType.DMA((2,)),
        ],
        name="pack",
    )(residual, wq, wf, wv, wg, mix, up, down)


def project_body(x_ref, gain_ref, short_ref, out_ref):
    zo = lax.axis_index("zo")
    ring = lax.axis_index("c") + lax.axis_index("zh")
    groups, _, height, width = x_ref.shape
    rows = width // 2
    squares = [None] * PARTS
    for f in range(groups):
        for h in range(PARTS):
            x = x_ref[f, h].astype(jnp.float32)
            squares[h] = x * x if f == 0 else squares[h] + x * x
    scale = [
        lax.rsqrt(jnp.sum(s, axis=-1, keepdims=True) / (groups * width) + epsilon)
        for s in squares
    ]
    lane = lax.broadcasted_iota(jnp.int32, (1, width), 1)
    total = None
    for k in range(CHIPS):
        f = 2 * k + zo
        here = (lane >= rows) == (lax.rem(ring + k, 2) == 1)
        gain = gain_ref[pl.ds(f, 1)]
        x = jnp.concatenate(
            [
                jnp.where(
                    here, x_ref[f, h].astype(jnp.float32) * scale[h] * gain, 0.0
                ).astype(jnp.bfloat16)
                for h in range(PARTS)
            ],
            axis=0,
        )
        w = jnp.concatenate([short_ref[k, :rows]] * 2, axis=0)
        term = jnp.dot(x, w, preferred_element_type=jnp.float32)
        total = term if total is None else total + term
    for h in range(PARTS):
        out_ref[h] = total[h * height : (h + 1) * height].astype(out_ref.dtype)


def project(x, gain, short):
    return pl.pallas_call(
        project_body,
        out_shape=pltpu.VMEM((PARTS, x.shape[2], short.shape[2]), jnp.bfloat16),
        name="project",
    )(near(x), gain, near(short))


def recur_body(
    part_ref,
    prior,
    floor_ref,
    gain_ref,
    state,
    out_ref,
    prior_ref,
    state_ref,
    read_ref,
    in_sems,
    out_sems,
):
    rows = prior_ref.shape[0]
    chunks = [slice(k, k + SLAB) for k in range(0, rows, SLAB)]
    fetches = run_copies([(prior.at[c], prior_ref.at[c]) for c in chunks], in_sems)
    stores = [
        pltpu.make_async_copy(state_ref.at[c], state.at[c], out_sems.at[k])
        for k, c in enumerate(chunks)
    ]
    pre = part_ref[0].astype(jnp.float32)
    for k in range(1, PARTS):
        pre = pre + part_ref[k].astype(jnp.float32)
    pre = pre.astype(jnp.bfloat16).astype(jnp.float32)
    width = prior_ref.shape[1]
    query = jax.nn.silu(pre[:, :width])
    floor = floor_ref[...]
    forget = floor + (1.0 - floor) * jax.nn.sigmoid(pre[:, width : 2 * width])
    value = pre[:, 2 * width : 3 * width]
    gate = jax.nn.sigmoid(pre[:, 3 * width :])
    forget_t = forget.T
    query_t = query.T
    for b in range(rows):
        if b % SLAB == 0:
            fetches[b // SLAB].wait()
        keep = forget_t[:, b : b + 1]
        fresh = keep * prior_ref[b] + (1.0 - keep) * value[b : b + 1]
        state_ref[b] = fresh
        read_ref[b : b + 1] = jnp.sum(query_t[:, b : b + 1] * fresh, axis=0, keepdims=True)
        if b % SLAB == SLAB - 1:
            stores[b // SLAB].start()
    read = read_ref[...]
    scale = lax.rsqrt(jnp.mean(read * read, axis=-1, keepdims=True) + epsilon)
    out_ref[...] = (read * scale * gain_ref[...] * gate).astype(out_ref.dtype)
    for store in stores:
        store.wait()


def recur(part, prior, floor, gain):
    rows, width, _ = prior.shape
    anywhere = pl.BlockSpec(memory_space=pl.ANY)
    vmem = pl.BlockSpec(memory_space=pltpu.VMEM)
    return pl.pallas_call(
        recur_body,
        out_shape=(
            jax.ShapeDtypeStruct(prior.shape, jnp.float32),
            pltpu.VMEM((rows, width), jnp.bfloat16),
        ),
        in_specs=[vmem, anywhere, vmem, vmem],
        out_specs=(anywhere, vmem),
        scratch_shapes=[
            pltpu.VMEM(prior.shape, jnp.float32),
            pltpu.VMEM(prior.shape, jnp.float32),
            pltpu.VMEM((rows, width), jnp.float32),
            pltpu.SemaphoreType.DMA((rows // SLAB,)),
            pltpu.SemaphoreType.DMA((rows // SLAB,)),
        ],
        name="recur",
    )(near(part), prior, floor, gain)


def mix_body(gated_ref, short_ref, out_ref, order_ref):
    height, width = gated_ref.shape[1:]
    rows = width // 2
    for h in range(PARTS):
        order_ref[pl.ds(h, height, stride=PARTS)] = gated_ref[h].astype(jnp.float32)
    left = order_ref[...].astype(jnp.bfloat16)
    for k in range(CHIPS // 2):
        right = jnp.concatenate(
            [
                short_ref[2 * k + half, rows:, j * width : (j + 1) * width]
                for half in range(2)
                for j in range(4)
            ],
            axis=0,
        )
        out_ref[pl.ds(k, PARTS * height, stride=CHIPS // 2)] = lax.dot_general(
            left, right, (((1,), (1,)), ((), ())), preferred_element_type=jnp.float32
        )


def mix_out(gated, short):
    height, width = gated.shape[1:]
    return pl.pallas_call(
        mix_body,
        out_shape=pltpu.VMEM((CHIPS // 2 * PARTS * height, width), jnp.float32),
        scratch_shapes=[pltpu.VMEM((PARTS * height, width), jnp.float32)],
        name="mix_out",
    )(near(gated), near(short))


def row_body(sums_ref, x_ref, gain_ref, out_ref, mixed_ref):
    own = 2 * lax.axis_index("zo") + lax.axis_index("c")
    place = lax.axis_index("y") * lax.axis_size("x") + lax.axis_index("x")
    groups, width = gain_ref.shape
    pairs = CHIPS // 2
    total = sums_ref[:groups]
    for k in range(1, groups):
        total = total + sums_ref[k * groups : (k + 1) * groups]
    first = lax.broadcasted_iota(jnp.int32, (pairs, width), 1) < width // 2
    turned = lax.rem(lax.axis_index("zh"), 2) == 1
    for h in range(2):
        left = total[2 * h * pairs : (2 * h + 1) * pairs]
        right = total[(2 * h + 1) * pairs : (2 * h + 2) * pairs]
        zero = jnp.where(turned, right, left)
        one = pltpu.roll(jnp.where(turned, left, right), width // 2, 1)
        even = jnp.where(first, zero, one)
        odd = jnp.where(first, one, zero)
        mixed_ref[pl.ds(h, pairs, stride=4)] = even
        mixed_ref[pl.ds(2 + h, pairs, stride=4)] = odd
    mixed = mixed_ref[...]
    scale = lax.rsqrt(jnp.sum(mixed * mixed) / gain_ref.size + epsilon)
    stream = x_ref[:, own].astype(jnp.float32)
    at = lax.broadcasted_iota(jnp.int32, stream.shape, 1) == place
    row = jnp.sum(jnp.where(at, stream, 0.0), axis=1)
    after = (row + mixed * scale * gain_ref[...]).astype(out_ref.dtype)
    out_ref[...] = jnp.broadcast_to(after[None], out_ref.shape)


def row_update(sums, x, gain):
    groups, width = gain.shape
    return pl.pallas_call(
        row_body,
        out_shape=pltpu.VMEM((groups, groups, width), jnp.bfloat16),
        scratch_shapes=[pltpu.VMEM((groups, width), jnp.float32)],
        name="row_update",
    )(near(sums), near(x), gain)


def mlp_body(
    row_ref,
    pre_ref,
    post_ref,
    long_ref,
    out_ref,
    own_ref,
    gain_ref,
    after_ref,
    up_ref,
    down_ref,
    sems,
):
    place = lax.axis_index("y") * lax.axis_size("x") + lax.axis_index("x")
    groups, width = pre_ref.shape
    height = row_ref.shape[0]
    units = up_ref.shape[1]
    full = groups * width
    pieces = [slice(k, k + full // PIECES) for k in range(0, full, full // PIECES)]
    copies = run_copies(
        [(long_ref.at[p, :units], up_ref.at[p]) for p in pieces]
        + [(long_ref.at[p, units:], down_ref.at[p]) for p in pieces],
        sems,
    )
    for row in range(height):
        after_ref[row * groups : (row + 1) * groups] = row_ref[row].astype(jnp.float32)
    after = [after_ref[pl.ds(f, height, stride=groups)] for f in range(groups)]
    squares = after[0] * after[0]
    for f in range(1, groups):
        squares = squares + after[f] * after[f]
    scale = lax.rsqrt(
        jnp.sum(squares, axis=-1, keepdims=True) / full + epsilon
    )
    hidden = jnp.concatenate(
        [
            (after[f] * scale * pre_ref[f : f + 1]).astype(jnp.bfloat16)
            for f in range(groups)
        ],
        axis=1,
    )
    own_ref[...] = after_ref[pl.ds(place, height, stride=groups)]
    gain_ref[...] = post_ref[pl.ds(place, 1)]
    up = None
    for k, p in enumerate(pieces):
        copies[k].wait()
        term = jnp.dot(hidden[:, p], up_ref[p], preferred_element_type=jnp.float32)
        up = term if up is None else up + term
    squared = jnp.square(jnp.maximum(up, 0.0)).astype(jnp.bfloat16)
    for k, p in enumerate(pieces):
        copies[PIECES + k].wait()
        channel = lax.dot_general(
            squared, down_ref[p], (((1,), (1,)), ((), ())), preferred_element_type=jnp.float32
        )
        for f in range(groups // PIECES):
            out_ref[k * (groups // PIECES) + f] = channel[
                :, f * width : (f + 1) * width
            ].astype(out_ref.dtype)


def mlp(after, pre, post, weights, hidden):
    rows, groups, width = after.shape
    vmem = pl.BlockSpec(memory_space=pltpu.VMEM)
    return pl.pallas_call(
        mlp_body,
        out_shape=(
            pltpu.VMEM((groups, rows, width), jnp.bfloat16),
            pltpu.VMEM((rows, width), jnp.float32),
            pltpu.VMEM((1, width), jnp.float32),
        ),
        in_specs=[vmem] * 3 + [pl.BlockSpec(memory_space=pl.ANY)],
        scratch_shapes=[
            pltpu.VMEM((rows * groups, width), jnp.float32),
            pltpu.VMEM((weights.shape[0], hidden), jnp.bfloat16),
            pltpu.VMEM((weights.shape[0], hidden), jnp.bfloat16),
            pltpu.SemaphoreType.DMA((2 * PIECES,)),
        ],
        name="mlp",
    )(near(after), pre, post, weights)


def shards(
    residual,
    prior_state,
    w_query,
    w_forget,
    w_value,
    w_outgate,
    forget_floor,
    group_gain,
    w_mix_out,
    gain_mix_pre,
    gain_mix_post,
    gain_mlp_pre,
    gain_mlp_post,
    w_up,
    w_down,
):
    batch_rows, own_cols = residual.shape
    groups = lax.axis_size(KV)
    hidden = w_up.shape[1]

    long, short, spread = pack(
        residual,
        w_query,
        w_forget,
        w_value,
        w_outgate,
        w_mix_out.T,
        w_up,
        w_down.T,
        groups * PARTS,
    )
    long = lax.all_gather(long, TP, axis=0, tiled=True)
    stream = exchange(spread, (*KV, *NEAR)).reshape(groups, PARTS, batch_rows, own_cols)
    short = lax.all_gather(short, ("zh", "c"), axis=0, axis_index_groups=RINGS)
    part = exchange(project(stream, gain_mix_pre.reshape(groups, own_cols), short), NEAR)
    new_state, gated = recur(
        part, prior_state[:, 0], forget_floor[None], group_gain[None]
    )
    mixed_part = mix_out(lax.all_gather(gated, NEAR, axis=0), short)
    mixed = exchange(
        mixed_part.reshape(groups * PARTS, CHIPS // 2, own_cols), (*KV, *NEAR)
    )
    after_row = row_update(
        mixed.reshape(-1, own_cols), stream, gain_mix_post.reshape(groups, own_cols)
    )
    channel_part, after_own, out_gain = mlp(
        exchange(after_row, KV),
        gain_mlp_pre.reshape(groups, own_cols),
        gain_mlp_post.reshape(groups, own_cols),
        long,
        hidden,
    )
    channel = jnp.sum(exchange(channel_part, KV).astype(jnp.float32), axis=0)
    layer_out = (after_own + channel * out_gain).astype(jnp.bfloat16)
    return layer_out, new_state[:, None]


def solution(mesh):
    grid = Mesh(mesh.devices.reshape(4, 4, CHIPS, 2, 2), (*KV, *TP))
    return jax.shard_map(
        shards,
        mesh=grid,
        in_specs=(
            P(TP, KV),
            P(TP, KV, None, None),
            P(TP, KV),
            P(TP, KV),
            P(TP, KV),
            P(TP, KV),
            P(KV),
            P(KV),
            P(KV, TP),
            P(),
            P(),
            P(),
            P(),
            P(TP, KV),
            P(KV, TP),
        ),
        out_specs=(P(TP, KV), P(TP, KV, None, None)),
        check_vma=False,
    )
```

```python
import jax
import jax.numpy as jnp
from jax import lax
from jax.experimental import pallas as pl
from jax.experimental.pallas import tpu as pltpu
from jax.sharding import Mesh
from jax.sharding import PartitionSpec as P

KV = ("y", "x")
TP = ("zh", "zo", "c")
NEAR = ("zo", "c")
PARTS = 4
CHIPS = 8
RINGS = [[2 * zh + (zh + g) % 2 for zh in range(CHIPS)] for g in range(2)]
SLAB = 4
PIECES = 4

epsilon = 1e-06


def exchange(blocks, axes):
    return lax.all_to_all(blocks, axes, 0, 0, tiled=True)


def near(value):
    return pltpu.with_memory_space_constraint(value, pltpu.VMEM)


def run_copies(copies, sems):
    started = [
        pltpu.make_async_copy(src, dst, sems.at[k]) for k, (src, dst) in enumerate(copies)
    ]
    for copy in started:
        copy.start()
    return started


def pack_body(
    residual,
    wq,
    wf,
    wv,
    wg,
    mix,
    up,
    down,
    long,
    short_ref,
    spread,
    long_ref,
    spread_ref,
    sems,
    out_sems,
):
    rows, cols = wq.shape
    part = mix.shape[0] // 4
    hidden = up.shape[1]
    copies = [(up, long_ref.at[:, :hidden]), (down, long_ref.at[:, hidden:])]
    for k, w in enumerate((wq, wf, wv, wg)):
        at = slice(k * cols, (k + 1) * cols)
        copies.append((w, short_ref.at[:rows, at]))
        copies.append((mix.at[k * part : (k + 1) * part], short_ref.at[rows:, at]))
    started = run_copies(copies, sems)
    spread_ref[...] = jnp.broadcast_to(residual[...][None], spread_ref.shape)
    outs = [
        pltpu.make_async_copy(spread_ref, spread, out_sems.at[0]),
        pltpu.make_async_copy(long_ref, long, out_sems.at[1]),
    ]
    outs[0].start()
    for copy in started[:2]:
        copy.wait()
    outs[1].start()
    for copy in started[2:] + outs:
        copy.wait()


def pack(residual, wq, wf, wv, wg, mix, up, down, peers):
    rows, cols = wq.shape
    anywhere = pl.BlockSpec(memory_space=pl.ANY)
    vmem = pl.BlockSpec(memory_space=pltpu.VMEM)
    long = (rows, up.shape[1] + down.shape[1])
    spread = (peers, *residual.shape)
    return pl.pallas_call(
        pack_body,
        out_shape=(
            jax.ShapeDtypeStruct(long, up.dtype),
            pltpu.VMEM((rows + mix.shape[0] // 4, 4 * cols), wq.dtype),
            jax.ShapeDtypeStruct(spread, residual.dtype),
        ),
        in_specs=[vmem] + [anywhere] * 7,
        out_specs=(anywhere, vmem, anywhere),
        scratch_shapes=[
            pltpu.VMEM(long, up.dtype),
            pltpu.VMEM(spread, residual.dtype),
            pltpu.SemaphoreType.DMA((10,)),
            pltpu.SemaphoreType.DMA((2,)),
        ],
        name="pack",
    )(residual, wq, wf, wv, wg, mix, up, down)


def project_body(x_ref, gain_ref, short_ref, out_ref, mix_ref):
    zo = lax.axis_index("zo")
    ring = lax.axis_index("c") + lax.axis_index("zh")
    groups, _, height, width = x_ref.shape
    rows = width // 2
    squares = [None] * PARTS
    for f in range(groups):
        for h in range(PARTS):
            x = x_ref[f, h].astype(jnp.float32)
            squares[h] = x * x if f == 0 else squares[h] + x * x
    scale = [
        lax.rsqrt(jnp.sum(s, axis=-1, keepdims=True) / (groups * width) + epsilon)
        for s in squares
    ]
    lane = lax.broadcasted_iota(jnp.int32, (1, width), 1)
    total = None
    for k in range(CHIPS):
        f = 2 * k + zo
        here = (lane >= rows) == (lax.rem(ring + k, 2) == 1)
        gain = gain_ref[pl.ds(f, 1)]
        x = jnp.concatenate(
            [
                jnp.where(
                    here, x_ref[f, h].astype(jnp.float32) * scale[h] * gain, 0.0
                ).astype(jnp.bfloat16)
                for h in range(PARTS)
            ],
            axis=0,
        )
        w = jnp.concatenate([short_ref[k, :rows]] * 2, axis=0)
        term = jnp.dot(x, w, preferred_element_type=jnp.float32)
        total = term if total is None else total + term
        for j in range(4):
            mix_ref[k * rows + j * (rows // 4) : k * rows + (j + 1) * (rows // 4)] = (
                short_ref[k, rows:, j * width : (j + 1) * width]
            )
    for h in range(PARTS):
        out_ref[h] = total[h * height : (h + 1) * height].astype(out_ref.dtype)


def project(x, gain, short):
    return pl.pallas_call(
        project_body,
        out_shape=(
            pltpu.VMEM((PARTS, x.shape[2], short.shape[2]), jnp.bfloat16),
            pltpu.VMEM((CHIPS * x.shape[3] // 2, x.shape[3]), jnp.bfloat16),
        ),
        name="project",
    )(near(x), gain, near(short))


def gates(pre, floor):
    width = floor.shape[1]
    forget = floor + (1.0 - floor) * jax.nn.sigmoid(pre[:, width : 2 * width])
    return forget, pre[:, 2 * width : 3 * width]


def read_body(
    part_ref, prior, floor_ref, gain_ref, out_ref, pre_ref, prior_ref, read_ref, sems
):
    rows, width, _ = prior_ref.shape
    chunks = [slice(k, k + SLAB) for k in range(0, rows, SLAB)]
    fetches = run_copies([(prior.at[c], prior_ref.at[c]) for c in chunks], sems)
    pre = part_ref[0].astype(jnp.float32)
    for k in range(1, PARTS):
        pre = pre + part_ref[k].astype(jnp.float32)
    pre = pre.astype(jnp.bfloat16).astype(jnp.float32)
    pre_ref[...] = pre
    query = jax.nn.silu(pre[:, :width])
    forget, value = gates(pre, floor_ref[...])
    gate = jax.nn.sigmoid(pre[:, 3 * width :])
    kept = (query * forget).T
    fresh = jnp.sum(query * (1.0 - forget), axis=-1, keepdims=True) * value
    for b in range(rows):
        if b % SLAB == 0:
            fetches[b // SLAB].wait()
        read_ref[b : b + 1] = jnp.sum(
            kept[:, b : b + 1] * prior_ref[b], axis=0, keepdims=True
        )
    read = read_ref[...] + fresh
    scale = lax.rsqrt(jnp.mean(read * read, axis=-1, keepdims=True) + epsilon)
    out_ref[...] = (read * scale * gain_ref[...] * gate).astype(out_ref.dtype)


def read_out(part, prior, floor, gain):
    rows, width, _ = prior.shape
    vmem = pl.BlockSpec(memory_space=pltpu.VMEM)
    return pl.pallas_call(
        read_body,
        out_shape=(
            pltpu.VMEM((rows, width), jnp.bfloat16),
            pltpu.VMEM((rows, part.shape[2]), jnp.float32),
        ),
        in_specs=[vmem, pl.BlockSpec(memory_space=pl.ANY), vmem, vmem],
        out_specs=(vmem, vmem),
        scratch_shapes=[
            pltpu.VMEM(prior.shape, jnp.float32),
            pltpu.VMEM((rows, width), jnp.float32),
            pltpu.SemaphoreType.DMA((rows // SLAB,)),
        ],
        name="read_out",
    )(near(part), prior, floor, gain)


def update_body(pre_ref, prior, floor_ref, state, prior_ref, state_ref, in_sems, out_sems):
    rows = prior_ref.shape[0]
    chunks = [slice(k, k + SLAB) for k in range(0, rows, SLAB)]
    fetches = run_copies([(prior.at[c], prior_ref.at[c]) for c in chunks], in_sems)
    stores = [
        pltpu.make_async_copy(state_ref.at[c], state.at[c], out_sems.at[k])
        for k, c in enumerate(chunks)
    ]
    forget, value = gates(pre_ref[...], floor_ref[...])
    forget = forget.T
    for b in range(rows):
        if b % SLAB == 0:
            fetches[b // SLAB].wait()
        keep = forget[:, b : b + 1]
        state_ref[b] = keep * prior_ref[b] + (1.0 - keep) * value[b : b + 1]
        if b % SLAB == SLAB - 1:
            stores[b // SLAB].start()
    for store in stores:
        store.wait()


def update(pre, prior, floor):
    rows = prior.shape[0]
    anywhere = pl.BlockSpec(memory_space=pl.ANY)
    vmem = pl.BlockSpec(memory_space=pltpu.VMEM)
    return pl.pallas_call(
        update_body,
        out_shape=jax.ShapeDtypeStruct(prior.shape, jnp.float32),
        in_specs=[vmem, anywhere, vmem],
        out_specs=anywhere,
        scratch_shapes=[
            pltpu.VMEM(prior.shape, jnp.float32),
            pltpu.VMEM(prior.shape, jnp.float32),
            pltpu.SemaphoreType.DMA((rows // SLAB,)),
            pltpu.SemaphoreType.DMA((rows // SLAB,)),
        ],
        name="update",
    )(near(pre), prior, floor)


def mix_body(gated_ref, w_ref, out_ref, sums_ref):
    zh = lax.axis_index("zh")
    height, width = gated_ref.shape
    rows = width // 2
    left = gated_ref[...]
    for k in range(CHIPS):
        for zo in range(2):
            right = jnp.concatenate(
                [
                    w_ref[2 * zo + lax.rem(c + zh + k, 2), k * rows : (k + 1) * rows]
                    for c in range(2)
                ],
                axis=0,
            )
            sums_ref[pl.ds(2 * k + zo, height, stride=2 * CHIPS)] = lax.dot_general(
                left, right, (((1,), (1,)), ((), ())), preferred_element_type=jnp.float32
            )
    for row in range(height):
        out_ref[row] = sums_ref[2 * CHIPS * row : 2 * CHIPS * (row + 1)].astype(
            out_ref.dtype
        )


def mix_out(gated, weights):
    height, width = gated.shape
    return pl.pallas_call(
        mix_body,
        out_shape=pltpu.VMEM((height, 2 * CHIPS, width), jnp.bfloat16),
        scratch_shapes=[pltpu.VMEM((2 * CHIPS * height, width), jnp.float32)],
        name="mix_out",
    )(near(gated), near(weights))


def row_body(sums_ref, x_ref, gain_ref, out_ref):
    own = 2 * lax.axis_index("zo") + lax.axis_index("c")
    place = lax.axis_index("y") * lax.axis_size("x") + lax.axis_index("x")
    mixed = sums_ref[0].astype(jnp.float32)
    for k in range(1, sums_ref.shape[0]):
        mixed = mixed + sums_ref[k].astype(jnp.float32)
    scale = lax.rsqrt(jnp.sum(mixed * mixed) / gain_ref.size + epsilon)
    stream = x_ref[:, own].astype(jnp.float32)
    at = lax.broadcasted_iota(jnp.int32, stream.shape, 1) == place
    row = jnp.sum(jnp.where(at, stream, 0.0), axis=1)
    after = (row + mixed * scale * gain_ref[...]).astype(out_ref.dtype)
    out_ref[...] = jnp.broadcast_to(after[None], out_ref.shape)


def row_update(sums, x, gain):
    groups, width = gain.shape
    return pl.pallas_call(
        row_body,
        out_shape=pltpu.VMEM((groups, groups, width), jnp.bfloat16),
        name="row_update",
    )(near(sums), near(x), gain)


def mlp_body(
    row_ref,
    pre_ref,
    post_ref,
    long_ref,
    out_ref,
    own_ref,
    gain_ref,
    after_ref,
    up_ref,
    down_ref,
    sems,
):
    place = lax.axis_index("y") * lax.axis_size("x") + lax.axis_index("x")
    groups, width = pre_ref.shape
    height = row_ref.shape[0]
    units = up_ref.shape[1]
    full = groups * width
    pieces = [slice(k, k + full // PIECES) for k in range(0, full, full // PIECES)]
    copies = run_copies(
        [(long_ref.at[p, :units], up_ref.at[p]) for p in pieces]
        + [(long_ref.at[p, units:], down_ref.at[p]) for p in pieces],
        sems,
    )
    for row in range(height):
        after_ref[row * groups : (row + 1) * groups] = row_ref[row].astype(jnp.float32)
    after = [after_ref[pl.ds(f, height, stride=groups)] for f in range(groups)]
    squares = after[0] * after[0]
    for f in range(1, groups):
        squares = squares + after[f] * after[f]
    scale = lax.rsqrt(
        jnp.sum(squares, axis=-1, keepdims=True) / full + epsilon
    )
    hidden = jnp.concatenate(
        [
            (after[f] * scale * pre_ref[f : f + 1]).astype(jnp.bfloat16)
            for f in range(groups)
        ],
        axis=1,
    )
    own_ref[...] = after_ref[pl.ds(place, height, stride=groups)]
    gain_ref[...] = post_ref[pl.ds(place, 1)]
    up = None
    for k, p in enumerate(pieces):
        copies[k].wait()
        term = jnp.dot(hidden[:, p], up_ref[p], preferred_element_type=jnp.float32)
        up = term if up is None else up + term
    squared = jnp.square(jnp.maximum(up, 0.0)).astype(jnp.bfloat16)
    for k, p in enumerate(pieces):
        copies[PIECES + k].wait()
        channel = lax.dot_general(
            squared, down_ref[p], (((1,), (1,)), ((), ())), preferred_element_type=jnp.float32
        )
        for f in range(groups // PIECES):
            out_ref[k * (groups // PIECES) + f] = channel[
                :, f * width : (f + 1) * width
            ].astype(out_ref.dtype)


def mlp(after, pre, post, weights, hidden):
    rows, groups, width = after.shape
    vmem = pl.BlockSpec(memory_space=pltpu.VMEM)
    return pl.pallas_call(
        mlp_body,
        out_shape=(
            pltpu.VMEM((groups, rows, width), jnp.bfloat16),
            pltpu.VMEM((rows, width), jnp.float32),
            pltpu.VMEM((1, width), jnp.float32),
        ),
        in_specs=[vmem] * 3 + [pl.BlockSpec(memory_space=pl.ANY)],
        scratch_shapes=[
            pltpu.VMEM((rows * groups, width), jnp.float32),
            pltpu.VMEM((weights.shape[0], hidden), jnp.bfloat16),
            pltpu.VMEM((weights.shape[0], hidden), jnp.bfloat16),
            pltpu.SemaphoreType.DMA((2 * PIECES,)),
        ],
        name="mlp",
    )(near(after), pre, post, weights)


def shards(
    residual,
    prior_state,
    w_query,
    w_forget,
    w_value,
    w_outgate,
    forget_floor,
    group_gain,
    w_mix_out,
    gain_mix_pre,
    gain_mix_post,
    gain_mlp_pre,
    gain_mlp_post,
    w_up,
    w_down,
):
    batch_rows, own_cols = residual.shape
    groups = lax.axis_size(KV)
    hidden = w_up.shape[1]

    long, short, spread = pack(
        residual,
        w_query,
        w_forget,
        w_value,
        w_outgate,
        w_mix_out.T,
        w_up,
        w_down.T,
        groups * PARTS,
    )
    long = lax.all_gather(long, TP, axis=0, tiled=True)
    stream = exchange(spread, (*KV, *NEAR)).reshape(groups, PARTS, batch_rows, own_cols)
    short = lax.all_gather(short, ("zh", "c"), axis=0, axis_index_groups=RINGS)
    part, mix = project(stream, gain_mix_pre.reshape(groups, own_cols), short)
    part = exchange(part, NEAR)
    prior = prior_state[:, 0]
    gated, pre = read_out(part, prior, forget_floor[None], group_gain[None])
    new_state = update(pre, prior, forget_floor[None])
    mix = lax.all_gather(mix, NEAR, axis=0)
    mixed = exchange(mix_out(gated, mix), KV)
    after_row = row_update(mixed, stream, gain_mix_post.reshape(groups, own_cols))
    channel_part, after_own, out_gain = mlp(
        exchange(after_row, KV),
        gain_mlp_pre.reshape(groups, own_cols),
        gain_mlp_post.reshape(groups, own_cols),
        long,
        hidden,
    )
    channel = jnp.sum(exchange(channel_part, KV).astype(jnp.float32), axis=0)
    layer_out = (after_own + channel * out_gain).astype(jnp.bfloat16)
    return layer_out, new_state[:, None]


def solution(mesh):
    grid = Mesh(mesh.devices.reshape(4, 4, CHIPS, 2, 2), (*KV, *TP))
    return jax.shard_map(
        shards,
        mesh=grid,
        in_specs=(
            P(TP, KV),
            P(TP, KV, None, None),
            P(TP, KV),
            P(TP, KV),
            P(TP, KV),
            P(TP, KV),
            P(KV),
            P(KV),
            P(KV, TP),
            P(),
            P(),
            P(),
            P(),
            P(TP, KV),
            P(KV, TP),
        ),
        out_specs=(P(TP, KV), P(TP, KV, None, None)),
        check_vma=False,
    )
```

```python
import jax
import jax.numpy as jnp
from jax import lax
from jax.experimental import pallas as pl
from jax.experimental.pallas import tpu as pltpu
from jax.sharding import Mesh
from jax.sharding import PartitionSpec as P

KV = ("y", "x")
TP = ("zh", "zo", "c")
NEAR = ("zo", "c")
PARTS = 4
CHIPS = 8
RINGS = [[2 * zh + (zh + g) % 2 for zh in range(CHIPS)] for g in range(2)]
SLAB = 4
PIECES = 4

epsilon = 1e-06


def exchange(blocks, axes):
    return lax.all_to_all(blocks, axes, 0, 0, tiled=True)


def near(value):
    return pltpu.with_memory_space_constraint(value, pltpu.VMEM)


def run_copies(copies, sems):
    started = [
        pltpu.make_async_copy(src, dst, sems.at[k]) for k, (src, dst) in enumerate(copies)
    ]
    for copy in started:
        copy.start()
    return started


def pack_body(
    residual,
    wq,
    wf,
    wv,
    wg,
    mix,
    up,
    down,
    long,
    short_ref,
    spread,
    long_ref,
    spread_ref,
    sems,
    out_sems,
):
    rows, cols = wq.shape
    part = mix.shape[0] // 4
    hidden = up.shape[1]
    copies = [(up, long_ref.at[:, :hidden]), (down, long_ref.at[:, hidden:])]
    for k, w in enumerate((wq, wf, wv, wg)):
        at = slice(k * cols, (k + 1) * cols)
        copies.append((w, short_ref.at[:rows, at]))
        copies.append((mix.at[k * part : (k + 1) * part], short_ref.at[rows:, at]))
    started = run_copies(copies, sems)
    spread_ref[...] = jnp.broadcast_to(residual[...][None], spread_ref.shape)
    outs = [
        pltpu.make_async_copy(spread_ref, spread, out_sems.at[0]),
        pltpu.make_async_copy(long_ref, long, out_sems.at[1]),
    ]
    outs[0].start()
    for copy in started[:2]:
        copy.wait()
    outs[1].start()
    for copy in started[2:] + outs:
        copy.wait()


def pack(residual, wq, wf, wv, wg, mix, up, down, peers):
    rows, cols = wq.shape
    anywhere = pl.BlockSpec(memory_space=pl.ANY)
    vmem = pl.BlockSpec(memory_space=pltpu.VMEM)
    long = (rows, up.shape[1] + down.shape[1])
    spread = (peers, *residual.shape)
    return pl.pallas_call(
        pack_body,
        out_shape=(
            jax.ShapeDtypeStruct(long, up.dtype),
            pltpu.VMEM((rows + mix.shape[0] // 4, 4 * cols), wq.dtype),
            jax.ShapeDtypeStruct(spread, residual.dtype),
        ),
        in_specs=[vmem] + [anywhere] * 7,
        out_specs=(anywhere, vmem, anywhere),
        scratch_shapes=[
            pltpu.VMEM(long, up.dtype),
            pltpu.VMEM(spread, residual.dtype),
            pltpu.SemaphoreType.DMA((10,)),
            pltpu.SemaphoreType.DMA((2,)),
        ],
        name="pack",
    )(residual, wq, wf, wv, wg, mix, up, down)


def project_body(x_ref, gain_ref, short_ref, out_ref, mix_ref):
    zo = lax.axis_index("zo")
    ring = lax.axis_index("c") + lax.axis_index("zh")
    groups, _, height, width = x_ref.shape
    rows = width // 2
    squares = [None] * PARTS
    for f in range(groups):
        for h in range(PARTS):
            x = x_ref[f, h].astype(jnp.float32)
            squares[h] = x * x if f == 0 else squares[h] + x * x
    scale = [
        lax.rsqrt(jnp.sum(s, axis=-1, keepdims=True) / (groups * width) + epsilon)
        for s in squares
    ]
    lane = lax.broadcasted_iota(jnp.int32, (1, width), 1)
    total = None
    for k in range(CHIPS):
        f = 2 * k + zo
        here = (lane >= rows) == (lax.rem(ring + k, 2) == 1)
        gain = gain_ref[pl.ds(f, 1)]
        x = jnp.concatenate(
            [
                jnp.where(
                    here, x_ref[f, h].astype(jnp.float32) * scale[h] * gain, 0.0
                ).astype(jnp.bfloat16)
                for h in range(PARTS)
            ],
            axis=0,
        )
        w = jnp.concatenate([short_ref[k, :rows]] * 2, axis=0)
        term = jnp.dot(x, w, preferred_element_type=jnp.float32)
        total = term if total is None else total + term
        for j in range(4):
            mix_ref[k * rows + j * (rows // 4) : k * rows + (j + 1) * (rows // 4)] = (
                short_ref[k, rows:, j * width : (j + 1) * width]
            )
    for h in range(PARTS):
        out_ref[h] = total[h * height : (h + 1) * height].astype(out_ref.dtype)


def project(x, gain, short):
    return pl.pallas_call(
        project_body,
        out_shape=(
            pltpu.VMEM((PARTS, x.shape[2], short.shape[2]), jnp.bfloat16),
            pltpu.VMEM((CHIPS * x.shape[3] // 2, x.shape[3]), jnp.bfloat16),
        ),
        name="project",
    )(near(x), gain, near(short))


def gates(pre, floor):
    width = floor.shape[1]
    forget = floor + (1.0 - floor) * jax.nn.sigmoid(pre[:, width : 2 * width])
    return forget, pre[:, 2 * width : 3 * width]


def read_body(
    part_ref, prior, floor_ref, gain_ref, out_ref, pre_ref, prior_ref, read_ref, sems
):
    rows, width, _ = prior_ref.shape
    chunks = [slice(k, k + SLAB) for k in range(0, rows, SLAB)]
    fetches = run_copies([(prior.at[c], prior_ref.at[c]) for c in chunks], sems)
    pre = part_ref[0].astype(jnp.float32)
    for k in range(1, PARTS):
        pre = pre + part_ref[k].astype(jnp.float32)
    pre = pre.astype(jnp.bfloat16).astype(jnp.float32)
    pre_ref[...] = pre
    query = jax.nn.silu(pre[:, :width])
    forget, value = gates(pre, floor_ref[...])
    gate = jax.nn.sigmoid(pre[:, 3 * width :])
    kept = (query * forget).T
    fresh = jnp.sum(query * (1.0 - forget), axis=-1, keepdims=True) * value
    for b in range(rows):
        if b % SLAB == 0:
            fetches[b // SLAB].wait()
        read_ref[b : b + 1] = jnp.sum(
            kept[:, b : b + 1] * prior_ref[b], axis=0, keepdims=True
        )
    read = read_ref[...] + fresh
    scale = lax.rsqrt(jnp.mean(read * read, axis=-1, keepdims=True) + epsilon)
    out_ref[...] = (read * scale * gain_ref[...] * gate).astype(out_ref.dtype)


def read_out(part, prior, floor, gain):
    rows, width, _ = prior.shape
    vmem = pl.BlockSpec(memory_space=pltpu.VMEM)
    return pl.pallas_call(
        read_body,
        out_shape=(
            pltpu.VMEM((rows, width), jnp.bfloat16),
            pltpu.VMEM((rows, part.shape[2]), jnp.float32),
        ),
        in_specs=[vmem, pl.BlockSpec(memory_space=pl.ANY), vmem, vmem],
        out_specs=(vmem, vmem),
        scratch_shapes=[
            pltpu.VMEM(prior.shape, jnp.float32),
            pltpu.VMEM((rows, width), jnp.float32),
            pltpu.SemaphoreType.DMA((rows // SLAB,)),
        ],
        name="read_out",
    )(near(part), prior, floor, gain)


def update_body(pre_ref, prior, floor_ref, state, prior_ref, state_ref, in_sems, out_sems):
    rows = prior_ref.shape[0]
    chunks = [slice(k, k + SLAB) for k in range(0, rows, SLAB)]
    fetches = run_copies([(prior.at[c], prior_ref.at[c]) for c in chunks], in_sems)
    stores = [
        pltpu.make_async_copy(state_ref.at[c], state.at[c], out_sems.at[k])
        for k, c in enumerate(chunks)
    ]
    forget, value = gates(pre_ref[...], floor_ref[...])
    forget = forget.T
    for b in range(rows):
        if b % SLAB == 0:
            fetches[b // SLAB].wait()
        keep = forget[:, b : b + 1]
        state_ref[b] = keep * prior_ref[b] + (1.0 - keep) * value[b : b + 1]
        if b % SLAB == SLAB - 1:
            stores[b // SLAB].start()
    for store in stores:
        store.wait()


def update(pre, prior, floor):
    rows = prior.shape[0]
    anywhere = pl.BlockSpec(memory_space=pl.ANY)
    vmem = pl.BlockSpec(memory_space=pltpu.VMEM)
    return pl.pallas_call(
        update_body,
        out_shape=jax.ShapeDtypeStruct(prior.shape, jnp.float32),
        in_specs=[vmem, anywhere, vmem],
        out_specs=anywhere,
        scratch_shapes=[
            pltpu.VMEM(prior.shape, jnp.float32),
            pltpu.VMEM(prior.shape, jnp.float32),
            pltpu.SemaphoreType.DMA((rows // SLAB,)),
            pltpu.SemaphoreType.DMA((rows // SLAB,)),
        ],
        name="update",
    )(near(pre), prior, floor)


def mix_body(gated_ref, w_ref, out_ref, sums_ref):
    zh = lax.axis_index("zh")
    height, width = gated_ref.shape
    rows = width // 2
    left = gated_ref[...]
    for k in range(CHIPS):
        for zo in range(2):
            right = jnp.concatenate(
                [
                    w_ref[2 * zo + lax.rem(c + zh + k, 2), k * rows : (k + 1) * rows]
                    for c in range(2)
                ],
                axis=0,
            )
            sums_ref[pl.ds(2 * k + zo, height, stride=2 * CHIPS)] = lax.dot_general(
                left, right, (((1,), (1,)), ((), ())), preferred_element_type=jnp.float32
            )
    for row in range(height):
        out_ref[row] = sums_ref[2 * CHIPS * row : 2 * CHIPS * (row + 1)].astype(
            out_ref.dtype
        )


def mix_out(gated, weights):
    height, width = gated.shape
    return pl.pallas_call(
        mix_body,
        out_shape=pltpu.VMEM((height, 2 * CHIPS, width), jnp.bfloat16),
        scratch_shapes=[pltpu.VMEM((2 * CHIPS * height, width), jnp.float32)],
        name="mix_out",
    )(near(gated), near(weights))


def row_body(sums_ref, x_ref, gain_ref, out_ref):
    own = 2 * lax.axis_index("zo") + lax.axis_index("c")
    place = lax.axis_index("y") * lax.axis_size("x") + lax.axis_index("x")
    mixed = sums_ref[0].astype(jnp.float32)
    for k in range(1, sums_ref.shape[0]):
        mixed = mixed + sums_ref[k].astype(jnp.float32)
    scale = lax.rsqrt(jnp.sum(mixed * mixed) / gain_ref.size + epsilon)
    stream = x_ref[:, own].astype(jnp.float32)
    at = lax.broadcasted_iota(jnp.int32, stream.shape, 1) == place
    row = jnp.sum(jnp.where(at, stream, 0.0), axis=1)
    after = (row + mixed * scale * gain_ref[...]).astype(out_ref.dtype)
    out_ref[...] = jnp.broadcast_to(after[None], out_ref.shape)


def row_update(sums, x, gain):
    groups, width = gain.shape
    return pl.pallas_call(
        row_body,
        out_shape=pltpu.VMEM((groups, groups, width), jnp.bfloat16),
        name="row_update",
    )(near(sums), near(x), gain)


def mlp_body(
    row_ref,
    pre_ref,
    post_ref,
    long_ref,
    out,
    own_ref,
    gain_ref,
    after_ref,
    up_ref,
    down_ref,
    out_ref,
    up_sems,
    down_sems,
    out_sems,
):
    place = lax.axis_index("y") * lax.axis_size("x") + lax.axis_index("x")
    groups, width = pre_ref.shape
    height = row_ref.shape[0]
    units = up_ref.shape[1]
    full = groups * width
    pieces = [slice(k, k + full // PIECES) for k in range(0, full, full // PIECES)]
    ups = run_copies([(long_ref.at[p, :units], up_ref.at[p]) for p in pieces], up_sems)
    for row in range(height):
        after_ref[row * groups : (row + 1) * groups] = row_ref[row].astype(jnp.float32)
    after = [after_ref[pl.ds(f, height, stride=groups)] for f in range(groups)]
    squares = after[0] * after[0]
    for f in range(1, groups):
        squares = squares + after[f] * after[f]
    scale = lax.rsqrt(
        jnp.sum(squares, axis=-1, keepdims=True) / full + epsilon
    )
    hidden = jnp.concatenate(
        [
            (after[f] * scale * pre_ref[f : f + 1]).astype(jnp.bfloat16)
            for f in range(groups)
        ],
        axis=1,
    )
    own_ref[...] = after_ref[pl.ds(place, height, stride=groups)]
    gain_ref[...] = post_ref[pl.ds(place, 1)]
    up = None
    for k, p in enumerate(pieces):
        ups[k].wait()
        if k == 0:
            downs = run_copies(
                [(long_ref.at[q, units:], down_ref.at[q]) for q in pieces], down_sems
            )
        term = jnp.dot(hidden[:, p], up_ref[p], preferred_element_type=jnp.float32)
        up = term if up is None else up + term
    squared = jnp.square(jnp.maximum(up, 0.0)).astype(jnp.bfloat16)
    some = groups // PIECES
    outs = [
        pltpu.make_async_copy(
            out_ref.at[k * some : (k + 1) * some],
            out.at[k * some : (k + 1) * some],
            out_sems.at[k],
        )
        for k in range(PIECES)
    ]
    for k, p in enumerate(pieces):
        downs[k].wait()
        channel = lax.dot_general(
            squared, down_ref[p], (((1,), (1,)), ((), ())), preferred_element_type=jnp.float32
        )
        for f in range(some):
            out_ref[k * some + f] = channel[:, f * width : (f + 1) * width].astype(
                out_ref.dtype
            )
        outs[k].start()
    for copy in outs:
        copy.wait()


def mlp(after, pre, post, weights, hidden):
    rows, groups, width = after.shape
    vmem = pl.BlockSpec(memory_space=pltpu.VMEM)
    return pl.pallas_call(
        mlp_body,
        out_shape=(
            jax.ShapeDtypeStruct((groups, rows, width), jnp.bfloat16),
            pltpu.VMEM((rows, width), jnp.float32),
            pltpu.VMEM((1, width), jnp.float32),
        ),
        out_specs=(pl.BlockSpec(memory_space=pl.ANY), vmem, vmem),
        in_specs=[vmem] * 3 + [pl.BlockSpec(memory_space=pl.ANY)],
        scratch_shapes=[
            pltpu.VMEM((rows * groups, width), jnp.float32),
            pltpu.VMEM((weights.shape[0], hidden), jnp.bfloat16),
            pltpu.VMEM((weights.shape[0], hidden), jnp.bfloat16),
            pltpu.VMEM((groups, rows, width), jnp.bfloat16),
            pltpu.SemaphoreType.DMA((PIECES,)),
            pltpu.SemaphoreType.DMA((PIECES,)),
            pltpu.SemaphoreType.DMA((PIECES,)),
        ],
        name="mlp",
    )(near(after), pre, post, weights)


def shards(
    residual,
    prior_state,
    w_query,
    w_forget,
    w_value,
    w_outgate,
    forget_floor,
    group_gain,
    w_mix_out,
    gain_mix_pre,
    gain_mix_post,
    gain_mlp_pre,
    gain_mlp_post,
    w_up,
    w_down,
):
    batch_rows, own_cols = residual.shape
    groups = lax.axis_size(KV)
    hidden = w_up.shape[1]

    long, short, spread = pack(
        residual,
        w_query,
        w_forget,
        w_value,
        w_outgate,
        w_mix_out.T,
        w_up,
        w_down.T,
        groups * PARTS,
    )
    long = lax.all_gather(long, TP, axis=0, tiled=True)
    stream = exchange(spread, (*KV, *NEAR)).reshape(groups, PARTS, batch_rows, own_cols)
    short = lax.all_gather(short, ("zh", "c"), axis=0, axis_index_groups=RINGS)
    part, mix = project(stream, gain_mix_pre.reshape(groups, own_cols), short)
    part = exchange(part, NEAR)
    prior = prior_state[:, 0]
    gated, pre = read_out(part, prior, forget_floor[None], group_gain[None])
    new_state = update(pre, prior, forget_floor[None])
    mix = lax.all_gather(mix, NEAR, axis=0)
    mixed = exchange(mix_out(gated, mix), KV)
    after_row = row_update(mixed, stream, gain_mix_post.reshape(groups, own_cols))
    channel_part, after_own, out_gain = mlp(
        exchange(after_row, KV),
        gain_mlp_pre.reshape(groups, own_cols),
        gain_mlp_post.reshape(groups, own_cols),
        long,
        hidden,
    )
    channel = jnp.sum(exchange(channel_part, KV).astype(jnp.float32), axis=0)
    layer_out = (after_own + channel * out_gain).astype(jnp.bfloat16)
    return layer_out, new_state[:, None]


def solution(mesh):
    grid = Mesh(mesh.devices.reshape(4, 4, CHIPS, 2, 2), (*KV, *TP))
    return jax.shard_map(
        shards,
        mesh=grid,
        in_specs=(
            P(TP, KV),
            P(TP, KV, None, None),
            P(TP, KV),
            P(TP, KV),
            P(TP, KV),
            P(TP, KV),
            P(KV),
            P(KV),
            P(KV, TP),
            P(),
            P(),
            P(),
            P(),
            P(TP, KV),
            P(KV, TP),
        ),
        out_specs=(P(TP, KV), P(TP, KV, None, None)),
        check_vma=False,
    )
```

```python
import jax
import jax.numpy as jnp
from jax import lax
from jax.experimental import pallas as pl
from jax.experimental.pallas import tpu as pltpu
from jax.sharding import Mesh
from jax.sharding import PartitionSpec as P

KV = ("y", "x")
TP = ("zh", "zo", "c")
NEAR = ("zo", "c")
PARTS = 4
CHIPS = 8
RINGS = [[2 * zh + (zh + g) % 2 for zh in range(CHIPS)] for g in range(2)]
SLAB = 8
PIECES = 2

epsilon = 1e-06


def exchange(blocks, axes):
    return lax.all_to_all(blocks, axes, 0, 0, tiled=True)


def near(value):
    return pltpu.with_memory_space_constraint(value, pltpu.VMEM)


def run_copies(copies, sems):
    started = [
        pltpu.make_async_copy(src, dst, sems.at[k]) for k, (src, dst) in enumerate(copies)
    ]
    for copy in started:
        copy.start()
    return started


def pack_body(
    residual,
    wq,
    wf,
    wv,
    wg,
    mix,
    up,
    down,
    long,
    short_ref,
    spread,
    long_ref,
    spread_ref,
    sems,
    out_sems,
):
    rows, cols = wq.shape
    part = mix.shape[0] // 4
    hidden = up.shape[1]
    copies = [(up, long_ref.at[:, :hidden]), (down, long_ref.at[:, hidden:])]
    for k, w in enumerate((wq, wf, wv, wg)):
        at = slice(k * cols, (k + 1) * cols)
        copies.append((w, short_ref.at[:rows, at]))
        copies.append((mix.at[k * part : (k + 1) * part], short_ref.at[rows:, at]))
    started = run_copies(copies, sems)
    spread_ref[...] = jnp.broadcast_to(residual[...][None], spread_ref.shape)
    outs = [
        pltpu.make_async_copy(spread_ref, spread, out_sems.at[0]),
        pltpu.make_async_copy(long_ref, long, out_sems.at[1]),
    ]
    outs[0].start()
    for copy in started[:2]:
        copy.wait()
    outs[1].start()
    for copy in started[2:] + outs:
        copy.wait()


def pack(residual, wq, wf, wv, wg, mix, up, down, peers):
    rows, cols = wq.shape
    anywhere = pl.BlockSpec(memory_space=pl.ANY)
    vmem = pl.BlockSpec(memory_space=pltpu.VMEM)
    long = (rows, up.shape[1] + down.shape[1])
    spread = (peers, *residual.shape)
    return pl.pallas_call(
        pack_body,
        out_shape=(
            jax.ShapeDtypeStruct(long, up.dtype),
            pltpu.VMEM((rows + mix.shape[0] // 4, 4 * cols), wq.dtype),
            jax.ShapeDtypeStruct(spread, residual.dtype),
        ),
        in_specs=[vmem] + [anywhere] * 7,
        out_specs=(anywhere, vmem, anywhere),
        scratch_shapes=[
            pltpu.VMEM(long, up.dtype),
            pltpu.VMEM(spread, residual.dtype),
            pltpu.SemaphoreType.DMA((10,)),
            pltpu.SemaphoreType.DMA((2,)),
        ],
        name="pack",
    )(residual, wq, wf, wv, wg, mix, up, down)


def project_body(x_ref, gain_ref, short_ref, out, mix_ref, out_ref, sem):
    zo = lax.axis_index("zo")
    ring = lax.axis_index("c") + lax.axis_index("zh")
    groups, _, height, width = x_ref.shape
    rows = width // 2
    squares = [None] * PARTS
    for f in range(groups):
        for h in range(PARTS):
            x = x_ref[f, h].astype(jnp.float32)
            squares[h] = x * x if f == 0 else squares[h] + x * x
    scale = [
        lax.rsqrt(jnp.sum(s, axis=-1, keepdims=True) / (groups * width) + epsilon)
        for s in squares
    ]
    lane = lax.broadcasted_iota(jnp.int32, (1, width), 1)
    total = None
    for k in range(CHIPS):
        f = 2 * k + zo
        here = (lane >= rows) == (lax.rem(ring + k, 2) == 1)
        gain = gain_ref[pl.ds(f, 1)]
        x = jnp.concatenate(
            [
                jnp.where(
                    here, x_ref[f, h].astype(jnp.float32) * scale[h] * gain, 0.0
                ).astype(jnp.bfloat16)
                for h in range(PARTS)
            ],
            axis=0,
        )
        w = jnp.concatenate([short_ref[k, :rows]] * 2, axis=0)
        term = jnp.dot(x, w, preferred_element_type=jnp.float32)
        total = term if total is None else total + term
    for h in range(PARTS):
        out_ref[h] = total[h * height : (h + 1) * height].astype(out_ref.dtype)
    send = pltpu.make_async_copy(out_ref, out, sem)
    send.start()
    for k in range(CHIPS):
        for j in range(4):
            mix_ref[k * rows + j * (rows // 4) : k * rows + (j + 1) * (rows // 4)] = (
                short_ref[k, rows:, j * width : (j + 1) * width]
            )
    send.wait()


def project(x, gain, short):
    vmem = pl.BlockSpec(memory_space=pltpu.VMEM)
    part = (PARTS, x.shape[2], short.shape[2])
    return pl.pallas_call(
        project_body,
        out_shape=(
            jax.ShapeDtypeStruct(part, jnp.bfloat16),
            pltpu.VMEM((CHIPS * x.shape[3] // 2, x.shape[3]), jnp.bfloat16),
        ),
        in_specs=[vmem] * 3,
        out_specs=(pl.BlockSpec(memory_space=pl.ANY), vmem),
        scratch_shapes=[pltpu.VMEM(part, jnp.bfloat16), pltpu.SemaphoreType.DMA(())],
        name="project",
    )(near(x), gain, near(short))


def gates(pre, floor):
    width = floor.shape[1]
    forget = floor + (1.0 - floor) * jax.nn.sigmoid(pre[:, width : 2 * width])
    return forget, pre[:, 2 * width : 3 * width]


def read_body(
    part_ref, prior, floor_ref, gain_ref, out_ref, pre_ref, prior_ref, read_ref, sems
):
    rows, width, _ = prior_ref.shape
    chunks = [slice(k, k + SLAB) for k in range(0, rows, SLAB)]
    fetches = run_copies([(prior.at[c], prior_ref.at[c]) for c in chunks], sems)
    pre = part_ref[0].astype(jnp.float32)
    for k in range(1, PARTS):
        pre = pre + part_ref[k].astype(jnp.float32)
    pre = pre.astype(jnp.bfloat16).astype(jnp.float32)
    pre_ref[...] = pre
    query = jax.nn.silu(pre[:, :width])
    forget, value = gates(pre, floor_ref[...])
    gate = jax.nn.sigmoid(pre[:, 3 * width :])
    kept = (query * forget).T
    fresh = jnp.sum(query * (1.0 - forget), axis=-1, keepdims=True) * value
    for b in range(rows):
        if b % SLAB == 0:
            fetches[b // SLAB].wait()
        read_ref[b : b + 1] = jnp.sum(
            kept[:, b : b + 1] * prior_ref[b], axis=0, keepdims=True
        )
    read = read_ref[...] + fresh
    scale = lax.rsqrt(jnp.mean(read * read, axis=-1, keepdims=True) + epsilon)
    out_ref[...] = (read * scale * gain_ref[...] * gate).astype(out_ref.dtype)


def read_out(part, prior, floor, gain):
    rows, width, _ = prior.shape
    vmem = pl.BlockSpec(memory_space=pltpu.VMEM)
    return pl.pallas_call(
        read_body,
        out_shape=(
            pltpu.VMEM((rows, width), jnp.bfloat16),
            pltpu.VMEM((rows, part.shape[2]), jnp.float32),
        ),
        in_specs=[vmem, pl.BlockSpec(memory_space=pl.ANY), vmem, vmem],
        out_specs=(vmem, vmem),
        scratch_shapes=[
            pltpu.VMEM(prior.shape, jnp.float32),
            pltpu.VMEM((rows, width), jnp.float32),
            pltpu.SemaphoreType.DMA((rows // SLAB,)),
        ],
        name="read_out",
    )(near(part), prior, floor, gain)


def update_body(pre_ref, prior, floor_ref, state, prior_ref, state_ref, in_sems, out_sems):
    rows = prior_ref.shape[0]
    chunks = [slice(k, k + SLAB) for k in range(0, rows, SLAB)]
    fetches = run_copies([(prior.at[c], prior_ref.at[c]) for c in chunks], in_sems)
    stores = [
        pltpu.make_async_copy(state_ref.at[c], state.at[c], out_sems.at[k])
        for k, c in enumerate(chunks)
    ]
    forget, value = gates(pre_ref[...], floor_ref[...])
    forget = forget.T
    for b in range(rows):
        if b % SLAB == 0:
            fetches[b // SLAB].wait()
        keep = forget[:, b : b + 1]
        state_ref[b] = keep * prior_ref[b] + (1.0 - keep) * value[b : b + 1]
        if b % SLAB == SLAB - 1:
            stores[b // SLAB].start()
    for store in stores:
        store.wait()


def update(pre, prior, floor):
    rows = prior.shape[0]
    anywhere = pl.BlockSpec(memory_space=pl.ANY)
    vmem = pl.BlockSpec(memory_space=pltpu.VMEM)
    return pl.pallas_call(
        update_body,
        out_shape=jax.ShapeDtypeStruct(prior.shape, jnp.float32),
        in_specs=[vmem, anywhere, vmem],
        out_specs=anywhere,
        scratch_shapes=[
            pltpu.VMEM(prior.shape, jnp.float32),
            pltpu.VMEM(prior.shape, jnp.float32),
            pltpu.SemaphoreType.DMA((rows // SLAB,)),
            pltpu.SemaphoreType.DMA((rows // SLAB,)),
        ],
        name="update",
    )(near(pre), prior, floor)


def mix_body(gated_ref, w_ref, out_ref, sums_ref):
    zh = lax.axis_index("zh")
    height, width = gated_ref.shape
    rows = width // 2
    left = gated_ref[...]
    for k in range(CHIPS):
        for zo in range(2):
            right = jnp.concatenate(
                [
                    w_ref[2 * zo + lax.rem(c + zh + k, 2), k * rows : (k + 1) * rows]
                    for c in range(2)
                ],
                axis=0,
            )
            sums_ref[pl.ds(2 * k + zo, height, stride=2 * CHIPS)] = lax.dot_general(
                left, right, (((1,), (1,)), ((), ())), preferred_element_type=jnp.float32
            )
    for row in range(height):
        out_ref[row] = sums_ref[2 * CHIPS * row : 2 * CHIPS * (row + 1)].astype(
            out_ref.dtype
        )


def mix_out(gated, weights):
    height, width = gated.shape
    return pl.pallas_call(
        mix_body,
        out_shape=pltpu.VMEM((height, 2 * CHIPS, width), jnp.bfloat16),
        scratch_shapes=[pltpu.VMEM((2 * CHIPS * height, width), jnp.float32)],
        name="mix_out",
    )(near(gated), near(weights))


def row_body(sums_ref, x_ref, gain_ref, out_ref):
    own = 2 * lax.axis_index("zo") + lax.axis_index("c")
    place = lax.axis_index("y") * lax.axis_size("x") + lax.axis_index("x")
    mixed = sums_ref[0].astype(jnp.float32)
    for k in range(1, sums_ref.shape[0]):
        mixed = mixed + sums_ref[k].astype(jnp.float32)
    scale = lax.rsqrt(jnp.sum(mixed * mixed) / gain_ref.size + epsilon)
    stream = x_ref[:, own].astype(jnp.float32)
    at = lax.broadcasted_iota(jnp.int32, stream.shape, 1) == place
    row = jnp.sum(jnp.where(at, stream, 0.0), axis=1)
    after = (row + mixed * scale * gain_ref[...]).astype(out_ref.dtype)
    out_ref[...] = jnp.broadcast_to(after[None], out_ref.shape)


def row_update(sums, x, gain):
    groups, width = gain.shape
    return pl.pallas_call(
        row_body,
        out_shape=pltpu.VMEM((groups, groups, width), jnp.bfloat16),
        name="row_update",
    )(near(sums), near(x), gain)


def mlp_body(
    row_ref,
    pre_ref,
    post_ref,
    long_ref,
    out_ref,
    own_ref,
    gain_ref,
    after_ref,
    up_ref,
    down_ref,
    sems,
):
    place = lax.axis_index("y") * lax.axis_size("x") + lax.axis_index("x")
    groups, width = pre_ref.shape
    height = row_ref.shape[0]
    units = up_ref.shape[1]
    full = groups * width
    pieces = [slice(k, k + full // PIECES) for k in range(0, full, full // PIECES)]
    copies = run_copies(
        [(long_ref.at[p, :units], up_ref.at[p]) for p in pieces]
        + [(long_ref.at[p, units:], down_ref.at[p]) for p in pieces],
        sems,
    )
    for row in range(height):
        after_ref[row * groups : (row + 1) * groups] = row_ref[row].astype(jnp.float32)
    after = [after_ref[pl.ds(f, height, stride=groups)] for f in range(groups)]
    squares = after[0] * after[0]
    for f in range(1, groups):
        squares = squares + after[f] * after[f]
    scale = lax.rsqrt(
        jnp.sum(squares, axis=-1, keepdims=True) / full + epsilon
    )
    hidden = jnp.concatenate(
        [
            (after[f] * scale * pre_ref[f : f + 1]).astype(jnp.bfloat16)
            for f in range(groups)
        ],
        axis=1,
    )
    own_ref[...] = after_ref[pl.ds(place, height, stride=groups)]
    gain_ref[...] = post_ref[pl.ds(place, 1)]
    up = None
    for k, p in enumerate(pieces):
        copies[k].wait()
        term = jnp.dot(hidden[:, p], up_ref[p], preferred_element_type=jnp.float32)
        up = term if up is None else up + term
    squared = jnp.square(jnp.maximum(up, 0.0)).astype(jnp.bfloat16)
    for k, p in enumerate(pieces):
        copies[PIECES + k].wait()
        channel = lax.dot_general(
            squared, down_ref[p], (((1,), (1,)), ((), ())), preferred_element_type=jnp.float32
        )
        for f in range(groups // PIECES):
            out_ref[k * (groups // PIECES) + f] = channel[
                :, f * width : (f + 1) * width
            ].astype(out_ref.dtype)


def mlp(after, pre, post, weights, hidden):
    rows, groups, width = after.shape
    vmem = pl.BlockSpec(memory_space=pltpu.VMEM)
    return pl.pallas_call(
        mlp_body,
        out_shape=(
            pltpu.VMEM((groups, rows, width), jnp.bfloat16),
            pltpu.VMEM((rows, width), jnp.float32),
            pltpu.VMEM((1, width), jnp.float32),
        ),
        in_specs=[vmem] * 3 + [pl.BlockSpec(memory_space=pl.ANY)],
        scratch_shapes=[
            pltpu.VMEM((rows * groups, width), jnp.float32),
            pltpu.VMEM((weights.shape[0], hidden), jnp.bfloat16),
            pltpu.VMEM((weights.shape[0], hidden), jnp.bfloat16),
            pltpu.SemaphoreType.DMA((2 * PIECES,)),
        ],
        name="mlp",
    )(near(after), pre, post, weights)


def shards(
    residual,
    prior_state,
    w_query,
    w_forget,
    w_value,
    w_outgate,
    forget_floor,
    group_gain,
    w_mix_out,
    gain_mix_pre,
    gain_mix_post,
    gain_mlp_pre,
    gain_mlp_post,
    w_up,
    w_down,
):
    batch_rows, own_cols = residual.shape
    groups = lax.axis_size(KV)
    hidden = w_up.shape[1]

    long, short, spread = pack(
        residual,
        w_query,
        w_forget,
        w_value,
        w_outgate,
        w_mix_out.T,
        w_up,
        w_down.T,
        groups * PARTS,
    )
    long = lax.all_gather(long, TP, axis=0, tiled=True)
    stream = exchange(spread, (*KV, *NEAR)).reshape(groups, PARTS, batch_rows, own_cols)
    short = lax.all_gather(short, ("zh", "c"), axis=0, axis_index_groups=RINGS)
    part, mix = project(stream, gain_mix_pre.reshape(groups, own_cols), short)
    part = exchange(part, NEAR)
    prior = prior_state[:, 0]
    gated, pre = read_out(part, prior, forget_floor[None], group_gain[None])
    new_state = update(pre, prior, forget_floor[None])
    mix = lax.all_gather(mix, NEAR, axis=0)
    mixed = exchange(mix_out(gated, mix), KV)
    after_row = row_update(mixed, stream, gain_mix_post.reshape(groups, own_cols))
    channel_part, after_own, out_gain = mlp(
        exchange(after_row, KV),
        gain_mlp_pre.reshape(groups, own_cols),
        gain_mlp_post.reshape(groups, own_cols),
        long,
        hidden,
    )
    channel = jnp.sum(exchange(channel_part, KV).astype(jnp.float32), axis=0)
    layer_out = (after_own + channel * out_gain).astype(jnp.bfloat16)
    return layer_out, new_state[:, None]


def solution(mesh):
    grid = Mesh(mesh.devices.reshape(4, 4, CHIPS, 2, 2), (*KV, *TP))
    return jax.shard_map(
        shards,
        mesh=grid,
        in_specs=(
            P(TP, KV),
            P(TP, KV, None, None),
            P(TP, KV),
            P(TP, KV),
            P(TP, KV),
            P(TP, KV),
            P(KV),
            P(KV),
            P(KV, TP),
            P(),
            P(),
            P(),
            P(),
            P(TP, KV),
            P(KV, TP),
        ),
        out_specs=(P(TP, KV), P(TP, KV, None, None)),
        check_vma=False,
    )
```

```python
import jax
import jax.numpy as jnp
from jax import lax
from jax.experimental import pallas as pl
from jax.experimental.pallas import tpu as pltpu
from jax.sharding import Mesh
from jax.sharding import PartitionSpec as P

KV = ("y", "x")
TP = ("zh", "zo", "c")
NEAR = ("zo", "c")
PARTS = 4
CHIPS = 8
RINGS = [[2 * zh + (zh + g) % 2 for zh in range(CHIPS)] for g in range(2)]
SLAB = 8
PIECES = 2

epsilon = 1e-06


def exchange(blocks, axes):
    return lax.all_to_all(blocks, axes, 0, 0, tiled=True)


def near(value):
    return pltpu.with_memory_space_constraint(value, pltpu.VMEM)


def run_copies(copies, sems):
    started = [
        pltpu.make_async_copy(src, dst, sems.at[k]) for k, (src, dst) in enumerate(copies)
    ]
    for copy in started:
        copy.start()
    return started


def pack_body(
    residual,
    wq,
    wf,
    wv,
    wg,
    mix,
    up,
    down,
    long,
    short_ref,
    spread,
    long_ref,
    spread_ref,
    sems,
    out_sems,
):
    rows, cols = wq.shape
    part = mix.shape[0] // 4
    hidden = up.shape[1]
    copies = [(up, long_ref.at[:, :hidden]), (down, long_ref.at[:, hidden:])]
    for k, w in enumerate((wq, wf, wv, wg)):
        at = slice(k * cols, (k + 1) * cols)
        copies.append((w, short_ref.at[:rows, at]))
        copies.append((mix.at[k * part : (k + 1) * part], short_ref.at[rows:, at]))
    started = run_copies(copies, sems)
    spread_ref[...] = jnp.broadcast_to(residual[...][None], spread_ref.shape)
    outs = [
        pltpu.make_async_copy(spread_ref, spread, out_sems.at[0]),
        pltpu.make_async_copy(long_ref, long, out_sems.at[1]),
    ]
    outs[0].start()
    for copy in started[:2]:
        copy.wait()
    outs[1].start()
    for copy in started[2:] + outs:
        copy.wait()


def pack(residual, wq, wf, wv, wg, mix, up, down, peers):
    rows, cols = wq.shape
    anywhere = pl.BlockSpec(memory_space=pl.ANY)
    vmem = pl.BlockSpec(memory_space=pltpu.VMEM)
    long = (rows, up.shape[1] + down.shape[1])
    spread = (peers, *residual.shape)
    return pl.pallas_call(
        pack_body,
        out_shape=(
            jax.ShapeDtypeStruct(long, up.dtype),
            pltpu.VMEM((rows + mix.shape[0] // 4, 4 * cols), wq.dtype),
            jax.ShapeDtypeStruct(spread, residual.dtype),
        ),
        in_specs=[vmem] + [anywhere] * 7,
        out_specs=(anywhere, vmem, anywhere),
        scratch_shapes=[
            pltpu.VMEM(long, up.dtype),
            pltpu.VMEM(spread, residual.dtype),
            pltpu.SemaphoreType.DMA((10,)),
            pltpu.SemaphoreType.DMA((2,)),
        ],
        name="pack",
    )(residual, wq, wf, wv, wg, mix, up, down)


def project_body(x_ref, gain_ref, short_ref, out, mix_ref, out_ref, sem):
    zo = lax.axis_index("zo")
    ring = lax.axis_index("c") + lax.axis_index("zh")
    groups, _, height, width = x_ref.shape
    rows = width // 2
    squares = [None] * PARTS
    for f in range(groups):
        for h in range(PARTS):
            x = x_ref[f, h].astype(jnp.float32)
            squares[h] = x * x if f == 0 else squares[h] + x * x
    scale = [
        lax.rsqrt(jnp.sum(s, axis=-1, keepdims=True) / (groups * width) + epsilon)
        for s in squares
    ]
    lane = lax.broadcasted_iota(jnp.int32, (1, width), 1)
    total = None
    for k in range(CHIPS):
        f = 2 * k + zo
        here = (lane >= rows) == (lax.rem(ring + k, 2) == 1)
        gain = gain_ref[pl.ds(f, 1)]
        x = jnp.concatenate(
            [
                jnp.where(
                    here, x_ref[f, h].astype(jnp.float32) * scale[h] * gain, 0.0
                ).astype(jnp.bfloat16)
                for h in range(PARTS)
            ],
            axis=0,
        )
        w = jnp.concatenate([short_ref[k, :rows]] * 2, axis=0)
        term = jnp.dot(x, w, preferred_element_type=jnp.float32)
        total = term if total is None else total + term
    for h in range(PARTS):
        out_ref[h] = total[h * height : (h + 1) * height].astype(out_ref.dtype)
    send = pltpu.make_async_copy(out_ref, out, sem)
    send.start()
    for k in range(CHIPS):
        for j in range(4):
            mix_ref[k * rows + j * (rows // 4) : k * rows + (j + 1) * (rows // 4)] = (
                short_ref[k, rows:, j * width : (j + 1) * width]
            )
    send.wait()


def project(x, gain, short):
    vmem = pl.BlockSpec(memory_space=pltpu.VMEM)
    part = (PARTS, x.shape[2], short.shape[2])
    return pl.pallas_call(
        project_body,
        out_shape=(
            jax.ShapeDtypeStruct(part, jnp.bfloat16),
            pltpu.VMEM((CHIPS * x.shape[3] // 2, x.shape[3]), jnp.bfloat16),
        ),
        in_specs=[vmem] * 3,
        out_specs=(pl.BlockSpec(memory_space=pl.ANY), vmem),
        scratch_shapes=[pltpu.VMEM(part, jnp.bfloat16), pltpu.SemaphoreType.DMA(())],
        name="project",
    )(near(x), gain, near(short))


def gates(pre, floor):
    width = floor.shape[1]
    forget = floor + (1.0 - floor) * jax.nn.sigmoid(pre[:, width : 2 * width])
    return forget, pre[:, 2 * width : 3 * width]


def read_body(
    part_ref, prior, floor_ref, gain_ref, out_ref, pre_ref, prior_ref, read_ref, sems
):
    rows, width, _ = prior_ref.shape
    chunks = [slice(k, k + SLAB) for k in range(0, rows, SLAB)]
    fetches = run_copies([(prior.at[c], prior_ref.at[c]) for c in chunks], sems)
    pre = part_ref[0].astype(jnp.float32)
    for k in range(1, PARTS):
        pre = pre + part_ref[k].astype(jnp.float32)
    pre = pre.astype(jnp.bfloat16).astype(jnp.float32)
    pre_ref[...] = pre
    query = jax.nn.silu(pre[:, :width])
    forget, value = gates(pre, floor_ref[...])
    gate = jax.nn.sigmoid(pre[:, 3 * width :])
    kept = (query * forget).T
    fresh = jnp.sum(query * (1.0 - forget), axis=-1, keepdims=True) * value
    for b in range(rows):
        if b % SLAB == 0:
            fetches[b // SLAB].wait()
        read_ref[b : b + 1] = jnp.sum(
            kept[:, b : b + 1] * prior_ref[b], axis=0, keepdims=True
        )
    read = read_ref[...] + fresh
    scale = lax.rsqrt(jnp.mean(read * read, axis=-1, keepdims=True) + epsilon)
    out_ref[...] = (read * scale * gain_ref[...] * gate).astype(out_ref.dtype)


def read_out(part, prior, floor, gain):
    rows, width, _ = prior.shape
    vmem = pl.BlockSpec(memory_space=pltpu.VMEM)
    return pl.pallas_call(
        read_body,
        out_shape=(
            pltpu.VMEM((rows, width), jnp.bfloat16),
            pltpu.VMEM((rows, part.shape[2]), jnp.float32),
        ),
        in_specs=[vmem, pl.BlockSpec(memory_space=pl.ANY), vmem, vmem],
        out_specs=(vmem, vmem),
        scratch_shapes=[
            pltpu.VMEM(prior.shape, jnp.float32),
            pltpu.VMEM((rows, width), jnp.float32),
            pltpu.SemaphoreType.DMA((rows // SLAB,)),
        ],
        name="read_out",
    )(near(part), prior, floor, gain)


def update_body(pre_ref, prior, floor_ref, state, prior_ref, state_ref, in_sems, out_sems):
    rows = prior_ref.shape[0]
    chunks = [slice(k, k + SLAB) for k in range(0, rows, SLAB)]
    fetches = run_copies([(prior.at[c], prior_ref.at[c]) for c in chunks], in_sems)
    stores = [
        pltpu.make_async_copy(state_ref.at[c], state.at[c], out_sems.at[k])
        for k, c in enumerate(chunks)
    ]
    forget, value = gates(pre_ref[...], floor_ref[...])
    forget = forget.T
    for b in range(rows):
        if b % SLAB == 0:
            fetches[b // SLAB].wait()
        keep = forget[:, b : b + 1]
        state_ref[b] = keep * prior_ref[b] + (1.0 - keep) * value[b : b + 1]
        if b % SLAB == SLAB - 1:
            stores[b // SLAB].start()
    for store in stores:
        store.wait()


def update(pre, prior, floor):
    rows = prior.shape[0]
    anywhere = pl.BlockSpec(memory_space=pl.ANY)
    vmem = pl.BlockSpec(memory_space=pltpu.VMEM)
    return pl.pallas_call(
        update_body,
        out_shape=jax.ShapeDtypeStruct(prior.shape, jnp.float32),
        in_specs=[vmem, anywhere, vmem],
        out_specs=anywhere,
        scratch_shapes=[
            pltpu.VMEM(prior.shape, jnp.float32),
            pltpu.VMEM(prior.shape, jnp.float32),
            pltpu.SemaphoreType.DMA((rows // SLAB,)),
            pltpu.SemaphoreType.DMA((rows // SLAB,)),
        ],
        name="update",
    )(near(pre), prior, floor)


def mix_body(gated_ref, w_ref, out_ref, order_ref):
    height, width = gated_ref.shape[1:]
    pairs = CHIPS // 2
    for c in range(2):
        order_ref[pl.ds(c, height, stride=2)] = gated_ref[c].astype(jnp.float32)
    left = order_ref[...].astype(jnp.bfloat16)
    for zo in range(2):
        for k in range(pairs):
            out_ref[pl.ds(zo * pairs + k, 2 * height, stride=CHIPS)] = lax.dot_general(
                left,
                w_ref[zo, k * width : (k + 1) * width],
                (((1,), (1,)), ((), ())),
                preferred_element_type=jnp.float32,
            )


def mix_out(gated, weights):
    height, width = gated.shape[1:]
    return pl.pallas_call(
        mix_body,
        out_shape=pltpu.VMEM((2 * CHIPS * height, width), jnp.float32),
        scratch_shapes=[pltpu.VMEM((2 * height, width), jnp.float32)],
        name="mix_out",
    )(near(gated), near(weights))


def row_body(sums_ref, x_ref, gain_ref, out_ref, mixed_ref):
    own = 2 * lax.axis_index("zo") + lax.axis_index("c")
    place = lax.axis_index("y") * lax.axis_size("x") + lax.axis_index("x")
    groups, width = gain_ref.shape
    pairs = CHIPS // 2
    total = sums_ref[:groups]
    for k in range(1, groups):
        total = total + sums_ref[k * groups : (k + 1) * groups]
    first = lax.broadcasted_iota(jnp.int32, (pairs, width), 1) < width // 2
    turned = lax.rem(lax.axis_index("zh"), 2) == 1
    for h in range(2):
        left = total[h * pairs : (h + 1) * pairs]
        right = total[(2 + h) * pairs : (3 + h) * pairs]
        zero = jnp.where(turned, right, left)
        one = pltpu.roll(jnp.where(turned, left, right), width // 2, 1)
        even = jnp.where(first, zero, one)
        odd = jnp.where(first, one, zero)
        mixed_ref[pl.ds(h, pairs, stride=4)] = even
        mixed_ref[pl.ds(2 + h, pairs, stride=4)] = odd
    mixed = mixed_ref[...]
    scale = lax.rsqrt(jnp.sum(mixed * mixed) / gain_ref.size + epsilon)
    stream = x_ref[:, own].astype(jnp.float32)
    at = lax.broadcasted_iota(jnp.int32, stream.shape, 1) == place
    row = jnp.sum(jnp.where(at, stream, 0.0), axis=1)
    after = (row + mixed * scale * gain_ref[...]).astype(out_ref.dtype)
    out_ref[...] = jnp.broadcast_to(after[None], out_ref.shape)


def row_update(sums, x, gain):
    groups, width = gain.shape
    return pl.pallas_call(
        row_body,
        out_shape=pltpu.VMEM((groups, groups, width), jnp.bfloat16),
        scratch_shapes=[pltpu.VMEM((groups, width), jnp.float32)],
        name="row_update",
    )(near(sums), near(x), gain)


def mlp_body(
    row_ref,
    pre_ref,
    post_ref,
    long_ref,
    out_ref,
    own_ref,
    gain_ref,
    after_ref,
    up_ref,
    down_ref,
    sems,
):
    place = lax.axis_index("y") * lax.axis_size("x") + lax.axis_index("x")
    groups, width = pre_ref.shape
    height = row_ref.shape[0]
    units = up_ref.shape[1]
    full = groups * width
    pieces = [slice(k, k + full // PIECES) for k in range(0, full, full // PIECES)]
    copies = run_copies(
        [(long_ref.at[p, :units], up_ref.at[p]) for p in pieces]
        + [(long_ref.at[p, units:], down_ref.at[p]) for p in pieces],
        sems,
    )
    for row in range(height):
        after_ref[row * groups : (row + 1) * groups] = row_ref[row].astype(jnp.float32)
    after = [after_ref[pl.ds(f, height, stride=groups)] for f in range(groups)]
    squares = after[0] * after[0]
    for f in range(1, groups):
        squares = squares + after[f] * after[f]
    scale = lax.rsqrt(
        jnp.sum(squares, axis=-1, keepdims=True) / full + epsilon
    )
    hidden = jnp.concatenate(
        [
            (after[f] * scale * pre_ref[f : f + 1]).astype(jnp.bfloat16)
            for f in range(groups)
        ],
        axis=1,
    )
    own_ref[...] = after_ref[pl.ds(place, height, stride=groups)]
    gain_ref[...] = post_ref[pl.ds(place, 1)]
    up = None
    for k, p in enumerate(pieces):
        copies[k].wait()
        term = jnp.dot(hidden[:, p], up_ref[p], preferred_element_type=jnp.float32)
        up = term if up is None else up + term
    squared = jnp.square(jnp.maximum(up, 0.0)).astype(jnp.bfloat16)
    for k, p in enumerate(pieces):
        copies[PIECES + k].wait()
        channel = lax.dot_general(
            squared, down_ref[p], (((1,), (1,)), ((), ())), preferred_element_type=jnp.float32
        )
        for f in range(groups // PIECES):
            out_ref[k * (groups // PIECES) + f] = channel[
                :, f * width : (f + 1) * width
            ].astype(out_ref.dtype)


def mlp(after, pre, post, weights, hidden):
    rows, groups, width = after.shape
    vmem = pl.BlockSpec(memory_space=pltpu.VMEM)
    return pl.pallas_call(
        mlp_body,
        out_shape=(
            pltpu.VMEM((groups, rows, width), jnp.bfloat16),
            pltpu.VMEM((rows, width), jnp.float32),
            pltpu.VMEM((1, width), jnp.float32),
        ),
        in_specs=[vmem] * 3 + [pl.BlockSpec(memory_space=pl.ANY)],
        scratch_shapes=[
            pltpu.VMEM((rows * groups, width), jnp.float32),
            pltpu.VMEM((weights.shape[0], hidden), jnp.bfloat16),
            pltpu.VMEM((weights.shape[0], hidden), jnp.bfloat16),
            pltpu.SemaphoreType.DMA((2 * PIECES,)),
        ],
        name="mlp",
    )(near(after), pre, post, weights)


def shards(
    residual,
    prior_state,
    w_query,
    w_forget,
    w_value,
    w_outgate,
    forget_floor,
    group_gain,
    w_mix_out,
    gain_mix_pre,
    gain_mix_post,
    gain_mlp_pre,
    gain_mlp_post,
    w_up,
    w_down,
):
    batch_rows, own_cols = residual.shape
    groups = lax.axis_size(KV)
    hidden = w_up.shape[1]

    long, short, spread = pack(
        residual,
        w_query,
        w_forget,
        w_value,
        w_outgate,
        w_mix_out.T,
        w_up,
        w_down.T,
        groups * PARTS,
    )
    long = lax.all_gather(long, TP, axis=0, tiled=True)
    stream = exchange(spread, (*KV, *NEAR)).reshape(groups, PARTS, batch_rows, own_cols)
    short = lax.all_gather(short, ("zh", "c"), axis=0, axis_index_groups=RINGS)
    part, mix = project(stream, gain_mix_pre.reshape(groups, own_cols), short)
    part = exchange(part, NEAR)
    prior = prior_state[:, 0]
    gated, pre = read_out(part, prior, forget_floor[None], group_gain[None])
    new_state = update(pre, prior, forget_floor[None])
    mix = lax.all_gather(mix, "zo", axis=0)
    gated = lax.all_gather(gated, "c", axis=0)
    mixed = mix_out(gated, mix).reshape(2 * groups, CHIPS, own_cols)
    mixed = exchange(mixed, (*KV, "c")).reshape(-1, own_cols)
    after_row = row_update(mixed, stream, gain_mix_post.reshape(groups, own_cols))
    channel_part, after_own, out_gain = mlp(
        exchange(after_row, KV),
        gain_mlp_pre.reshape(groups, own_cols),
        gain_mlp_post.reshape(groups, own_cols),
        long,
        hidden,
    )
    channel = jnp.sum(exchange(channel_part, KV).astype(jnp.float32), axis=0)
    layer_out = (after_own + channel * out_gain).astype(jnp.bfloat16)
    return layer_out, new_state[:, None]


def solution(mesh):
    grid = Mesh(mesh.devices.reshape(4, 4, CHIPS, 2, 2), (*KV, *TP))
    return jax.shard_map(
        shards,
        mesh=grid,
        in_specs=(
            P(TP, KV),
            P(TP, KV, None, None),
            P(TP, KV),
            P(TP, KV),
            P(TP, KV),
            P(TP, KV),
            P(KV),
            P(KV),
            P(KV, TP),
            P(),
            P(),
            P(),
            P(),
            P(TP, KV),
            P(KV, TP),
        ),
        out_specs=(P(TP, KV), P(TP, KV, None, None)),
        check_vma=False,
    )
```

```python
import jax
import jax.numpy as jnp
from jax import lax
from jax.experimental import pallas as pl
from jax.experimental.pallas import tpu as pltpu
from jax.sharding import Mesh
from jax.sharding import PartitionSpec as P

KV = ("y", "x")
TP = ("zh", "zo", "c")
NEAR = ("zo", "c")
PARTS = 4
CHIPS = 8
RINGS = [[2 * zh + (zh + g) % 2 for zh in range(CHIPS)] for g in range(2)]
SLAB = 8
PIECES = 2

epsilon = 1e-06


def exchange(blocks, axes):
    return lax.all_to_all(blocks, axes, 0, 0, tiled=True)


def near(value):
    return pltpu.with_memory_space_constraint(value, pltpu.VMEM)


def run_copies(copies, sems):
    started = [
        pltpu.make_async_copy(src, dst, sems.at[k]) for k, (src, dst) in enumerate(copies)
    ]
    for copy in started:
        copy.start()
    return started


def pack_body(
    residual,
    wq,
    wf,
    wv,
    wg,
    mix,
    up,
    down,
    long,
    short_ref,
    spread,
    long_ref,
    spread_ref,
    sems,
    out_sems,
):
    rows, cols = wq.shape
    part = mix.shape[0] // 4
    hidden = up.shape[1]
    copies = [(up, long_ref.at[:, :hidden]), (down, long_ref.at[:, hidden:])]
    for k, w in enumerate((wq, wf, wv, wg)):
        at = slice(k * cols, (k + 1) * cols)
        copies.append((w, short_ref.at[:rows, at]))
        copies.append((mix.at[k * part : (k + 1) * part], short_ref.at[rows:, at]))
    started = run_copies(copies, sems)
    spread_ref[...] = jnp.broadcast_to(residual[...][None], spread_ref.shape)
    outs = [
        pltpu.make_async_copy(spread_ref, spread, out_sems.at[0]),
        pltpu.make_async_copy(long_ref, long, out_sems.at[1]),
    ]
    outs[0].start()
    for copy in started[:2]:
        copy.wait()
    outs[1].start()
    for copy in started[2:] + outs:
        copy.wait()


def pack(residual, wq, wf, wv, wg, mix, up, down, peers):
    rows, cols = wq.shape
    anywhere = pl.BlockSpec(memory_space=pl.ANY)
    vmem = pl.BlockSpec(memory_space=pltpu.VMEM)
    long = (rows, up.shape[1] + down.shape[1])
    spread = (peers, *residual.shape)
    return pl.pallas_call(
        pack_body,
        out_shape=(
            jax.ShapeDtypeStruct(long, up.dtype),
            pltpu.VMEM((rows + mix.shape[0] // 4, 4 * cols), wq.dtype),
            jax.ShapeDtypeStruct(spread, residual.dtype),
        ),
        in_specs=[vmem] + [anywhere] * 7,
        out_specs=(anywhere, vmem, anywhere),
        scratch_shapes=[
            pltpu.VMEM(long, up.dtype),
            pltpu.VMEM(spread, residual.dtype),
            pltpu.SemaphoreType.DMA((10,)),
            pltpu.SemaphoreType.DMA((2,)),
        ],
        name="pack",
    )(residual, wq, wf, wv, wg, mix, up, down)


def project_body(x_ref, gain_ref, short_ref, out, mix_ref, out_ref, sem):
    zo = lax.axis_index("zo")
    ring = lax.axis_index("c") + lax.axis_index("zh")
    groups, _, height, width = x_ref.shape
    rows = width // 2
    squares = [None] * PARTS
    for f in range(groups):
        for h in range(PARTS):
            x = x_ref[f, h].astype(jnp.float32)
            squares[h] = x * x if f == 0 else squares[h] + x * x
    scale = [
        lax.rsqrt(jnp.sum(s, axis=-1, keepdims=True) / (groups * width) + epsilon)
        for s in squares
    ]
    lane = lax.broadcasted_iota(jnp.int32, (1, width), 1)
    total = None
    for k in range(CHIPS):
        f = 2 * k + zo
        here = (lane >= rows) == (lax.rem(ring + k, 2) == 1)
        gain = gain_ref[pl.ds(f, 1)]
        x = jnp.concatenate(
            [
                jnp.where(
                    here, x_ref[f, h].astype(jnp.float32) * scale[h] * gain, 0.0
                ).astype(jnp.bfloat16)
                for h in range(PARTS)
            ],
            axis=0,
        )
        w = jnp.concatenate([short_ref[k, :rows]] * 2, axis=0)
        term = jnp.dot(x, w, preferred_element_type=jnp.float32)
        total = term if total is None else total + term
    for h in range(PARTS):
        out_ref[h] = total[h * height : (h + 1) * height].astype(out_ref.dtype)
    send = pltpu.make_async_copy(out_ref, out, sem)
    send.start()
    for k in range(CHIPS):
        for j in range(4):
            mix_ref[k * rows + j * (rows // 4) : k * rows + (j + 1) * (rows // 4)] = (
                short_ref[k, rows:, j * width : (j + 1) * width]
            )
    send.wait()


def project(x, gain, short):
    vmem = pl.BlockSpec(memory_space=pltpu.VMEM)
    part = (PARTS, x.shape[2], short.shape[2])
    return pl.pallas_call(
        project_body,
        out_shape=(
            jax.ShapeDtypeStruct(part, jnp.bfloat16),
            pltpu.VMEM((CHIPS * x.shape[3] // 2, x.shape[3]), jnp.bfloat16),
        ),
        in_specs=[vmem] * 3,
        out_specs=(pl.BlockSpec(memory_space=pl.ANY), vmem),
        scratch_shapes=[pltpu.VMEM(part, jnp.bfloat16), pltpu.SemaphoreType.DMA(())],
        name="project",
    )(near(x), gain, near(short))


def gates(pre, floor):
    width = floor.shape[1]
    forget = floor + (1.0 - floor) * jax.nn.sigmoid(pre[:, width : 2 * width])
    return forget, pre[:, 2 * width : 3 * width]


def read_body(
    part_ref, prior, floor_ref, gain_ref, out_ref, pre_ref, prior_ref, read_ref, sems
):
    rows, width, _ = prior_ref.shape
    chunks = [slice(k, k + SLAB) for k in range(0, rows, SLAB)]
    fetches = run_copies([(prior.at[c], prior_ref.at[c]) for c in chunks], sems)
    pre = part_ref[0].astype(jnp.float32)
    for k in range(1, PARTS):
        pre = pre + part_ref[k].astype(jnp.float32)
    pre = pre.astype(jnp.bfloat16).astype(jnp.float32)
    pre_ref[...] = pre
    query = jax.nn.silu(pre[:, :width])
    forget, value = gates(pre, floor_ref[...])
    gate = jax.nn.sigmoid(pre[:, 3 * width :])
    kept = (query * forget).T
    fresh = jnp.sum(query * (1.0 - forget), axis=-1, keepdims=True) * value
    for b in range(rows):
        if b % SLAB == 0:
            fetches[b // SLAB].wait()
        read_ref[b : b + 1] = jnp.sum(
            kept[:, b : b + 1] * prior_ref[b], axis=0, keepdims=True
        )
    read = read_ref[...] + fresh
    scale = lax.rsqrt(jnp.mean(read * read, axis=-1, keepdims=True) + epsilon)
    out_ref[...] = (read * scale * gain_ref[...] * gate).astype(out_ref.dtype)


def read_out(part, prior, floor, gain):
    rows, width, _ = prior.shape
    vmem = pl.BlockSpec(memory_space=pltpu.VMEM)
    return pl.pallas_call(
        read_body,
        out_shape=(
            pltpu.VMEM((rows, width), jnp.bfloat16),
            pltpu.VMEM((rows, part.shape[2]), jnp.float32),
        ),
        in_specs=[vmem, pl.BlockSpec(memory_space=pl.ANY), vmem, vmem],
        out_specs=(vmem, vmem),
        scratch_shapes=[
            pltpu.VMEM(prior.shape, jnp.float32),
            pltpu.VMEM((rows, width), jnp.float32),
            pltpu.SemaphoreType.DMA((rows // SLAB,)),
        ],
        name="read_out",
    )(near(part), prior, floor, gain)


def update_body(pre_ref, prior, floor_ref, state, prior_ref, state_ref, in_sems, out_sems):
    rows = prior_ref.shape[0]
    chunks = [slice(k, k + SLAB) for k in range(0, rows, SLAB)]
    fetches = run_copies([(prior.at[c], prior_ref.at[c]) for c in chunks], in_sems)
    stores = [
        pltpu.make_async_copy(state_ref.at[c], state.at[c], out_sems.at[k])
        for k, c in enumerate(chunks)
    ]
    forget, value = gates(pre_ref[...], floor_ref[...])
    forget = forget.T
    for b in range(rows):
        if b % SLAB == 0:
            fetches[b // SLAB].wait()
        keep = forget[:, b : b + 1]
        state_ref[b] = keep * prior_ref[b] + (1.0 - keep) * value[b : b + 1]
        if b % SLAB == SLAB - 1:
            stores[b // SLAB].start()
    for store in stores:
        store.wait()


def update(pre, prior, floor):
    rows = prior.shape[0]
    anywhere = pl.BlockSpec(memory_space=pl.ANY)
    vmem = pl.BlockSpec(memory_space=pltpu.VMEM)
    return pl.pallas_call(
        update_body,
        out_shape=jax.ShapeDtypeStruct(prior.shape, jnp.float32),
        in_specs=[vmem, anywhere, vmem],
        out_specs=anywhere,
        scratch_shapes=[
            pltpu.VMEM(prior.shape, jnp.float32),
            pltpu.VMEM(prior.shape, jnp.float32),
            pltpu.SemaphoreType.DMA((rows // SLAB,)),
            pltpu.SemaphoreType.DMA((rows // SLAB,)),
        ],
        name="update",
    )(near(pre), prior, floor)


def mix_body(gated_ref, w_ref, out_ref, sums_ref):
    zh = lax.axis_index("zh")
    height, width = gated_ref.shape
    rows = width // 2
    left = gated_ref[...]
    for k in range(CHIPS):
        for zo in range(2):
            right = jnp.concatenate(
                [
                    w_ref[2 * zo + lax.rem(c + zh + k, 2), k * rows : (k + 1) * rows]
                    for c in range(2)
                ],
                axis=0,
            )
            sums_ref[pl.ds(2 * k + zo, height, stride=2 * CHIPS)] = lax.dot_general(
                left, right, (((1,), (1,)), ((), ())), preferred_element_type=jnp.float32
            )
    for row in range(height):
        out_ref[row] = sums_ref[2 * CHIPS * row : 2 * CHIPS * (row + 1)].astype(
            out_ref.dtype
        )


def mix_out(gated, weights):
    height, width = gated.shape
    return pl.pallas_call(
        mix_body,
        out_shape=pltpu.VMEM((height, 2 * CHIPS, width), jnp.bfloat16),
        scratch_shapes=[pltpu.VMEM((2 * CHIPS * height, width), jnp.float32)],
        name="mix_out",
    )(near(gated), near(weights))


def row_body(sums_ref, x_ref, gain_ref, out_ref):
    own = 2 * lax.axis_index("zo") + lax.axis_index("c")
    place = lax.axis_index("y") * lax.axis_size("x") + lax.axis_index("x")
    mixed = sums_ref[0].astype(jnp.float32)
    for k in range(1, sums_ref.shape[0]):
        mixed = mixed + sums_ref[k].astype(jnp.float32)
    scale = lax.rsqrt(jnp.sum(mixed * mixed) / gain_ref.size + epsilon)
    stream = x_ref[:, own].astype(jnp.float32)
    at = lax.broadcasted_iota(jnp.int32, stream.shape, 1) == place
    row = jnp.sum(jnp.where(at, stream, 0.0), axis=1)
    after = (row + mixed * scale * gain_ref[...]).astype(out_ref.dtype)
    out_ref[...] = jnp.broadcast_to(after[None], out_ref.shape)


def row_update(sums, x, gain):
    groups, width = gain.shape
    return pl.pallas_call(
        row_body,
        out_shape=pltpu.VMEM((groups, groups, width), jnp.bfloat16),
        name="row_update",
    )(near(sums), near(x), gain)


def mlp_body(
    row_ref,
    pre_ref,
    post_ref,
    long_ref,
    out_ref,
    own_ref,
    gain_ref,
    after_ref,
    up_ref,
    down_ref,
    sems,
):
    place = lax.axis_index("y") * lax.axis_size("x") + lax.axis_index("x")
    groups, width = pre_ref.shape
    height = row_ref.shape[0]
    units = up_ref.shape[1]
    full = groups * width
    pieces = [slice(k, k + full // PIECES) for k in range(0, full, full // PIECES)]
    copies = run_copies(
        [(long_ref.at[p, :units], up_ref.at[p]) for p in pieces]
        + [(long_ref.at[p, units:], down_ref.at[p]) for p in pieces],
        sems,
    )
    for row in range(height):
        after_ref[row * groups : (row + 1) * groups] = row_ref[row].astype(jnp.float32)
    after = [after_ref[pl.ds(f, height, stride=groups)] for f in range(groups)]
    squares = after[0] * after[0]
    for f in range(1, groups):
        squares = squares + after[f] * after[f]
    scale = lax.rsqrt(
        jnp.sum(squares, axis=-1, keepdims=True) / full + epsilon
    )
    hidden = jnp.concatenate(
        [
            (after[f] * scale * pre_ref[f : f + 1]).astype(jnp.bfloat16)
            for f in range(groups)
        ],
        axis=1,
    )
    own_ref[...] = after_ref[pl.ds(place, height, stride=groups)]
    gain_ref[...] = post_ref[pl.ds(place, 1)]
    up = None
    for k, p in enumerate(pieces):
        copies[k].wait()
        term = jnp.dot(hidden[:, p], up_ref[p], preferred_element_type=jnp.float32)
        up = term if up is None else up + term
    squared = jnp.square(jnp.maximum(up, 0.0)).astype(jnp.bfloat16)
    for k, p in enumerate(pieces):
        copies[PIECES + k].wait()
        channel = lax.dot_general(
            squared, down_ref[p], (((1,), (1,)), ((), ())), preferred_element_type=jnp.float32
        )
        for f in range(groups // PIECES):
            out_ref[k * (groups // PIECES) + f] = channel[
                :, f * width : (f + 1) * width
            ].astype(out_ref.dtype)


def mlp(after, pre, post, weights, hidden):
    rows, groups, width = after.shape
    vmem = pl.BlockSpec(memory_space=pltpu.VMEM)
    return pl.pallas_call(
        mlp_body,
        out_shape=(
            pltpu.VMEM((groups, rows, width), jnp.bfloat16),
            pltpu.VMEM((rows, width), jnp.float32),
            pltpu.VMEM((1, width), jnp.float32),
        ),
        in_specs=[vmem] * 3 + [pl.BlockSpec(memory_space=pl.ANY)],
        scratch_shapes=[
            pltpu.VMEM((rows * groups, width), jnp.float32),
            pltpu.VMEM((weights.shape[0], hidden), jnp.bfloat16),
            pltpu.VMEM((weights.shape[0], hidden), jnp.bfloat16),
            pltpu.SemaphoreType.DMA((2 * PIECES,)),
        ],
        name="mlp",
    )(near(after), pre, post, weights)


def shards(
    residual,
    prior_state,
    w_query,
    w_forget,
    w_value,
    w_outgate,
    forget_floor,
    group_gain,
    w_mix_out,
    gain_mix_pre,
    gain_mix_post,
    gain_mlp_pre,
    gain_mlp_post,
    w_up,
    w_down,
):
    batch_rows, own_cols = residual.shape
    groups = lax.axis_size(KV)
    hidden = w_up.shape[1]

    long, short, spread = pack(
        residual,
        w_query,
        w_forget,
        w_value,
        w_outgate,
        w_mix_out.T,
        w_up,
        w_down.T,
        groups * PARTS,
    )
    long = lax.all_gather(long, TP, axis=0, tiled=True)
    stream = exchange(spread, (*KV, *NEAR)).reshape(groups, PARTS, batch_rows, own_cols)
    short = lax.all_gather(short, ("zh", "c"), axis=0, axis_index_groups=RINGS)
    part, mix = project(stream, gain_mix_pre.reshape(groups, own_cols), short)
    part = exchange(part, NEAR)
    prior = prior_state[:, 0]
    gated, pre = read_out(part, prior, forget_floor[None], group_gain[None])
    new_state = update(pre, prior, forget_floor[None])
    mix = lax.all_gather(mix, NEAR, axis=0)
    mixed = exchange(mix_out(gated, mix), KV)
    after_row = row_update(mixed, stream, gain_mix_post.reshape(groups, own_cols))
    after_row, new_state = lax.optimization_barrier((after_row, new_state))
    channel_part, after_own, out_gain = mlp(
        exchange(after_row, KV),
        gain_mlp_pre.reshape(groups, own_cols),
        gain_mlp_post.reshape(groups, own_cols),
        long,
        hidden,
    )
    channel = jnp.sum(exchange(channel_part, KV).astype(jnp.float32), axis=0)
    layer_out = (after_own + channel * out_gain).astype(jnp.bfloat16)
    return layer_out, new_state[:, None]


def solution(mesh):
    grid = Mesh(mesh.devices.reshape(4, 4, CHIPS, 2, 2), (*KV, *TP))
    return jax.shard_map(
        shards,
        mesh=grid,
        in_specs=(
            P(TP, KV),
            P(TP, KV, None, None),
            P(TP, KV),
            P(TP, KV),
            P(TP, KV),
            P(TP, KV),
            P(KV),
            P(KV),
            P(KV, TP),
            P(),
            P(),
            P(),
            P(),
            P(TP, KV),
            P(KV, TP),
        ),
        out_specs=(P(TP, KV), P(TP, KV, None, None)),
        check_vma=False,
    )
```
